256 devices in a mesh: sp: 32 (over z, x), tp: 8 (over y, core).
Axes of the slice: x: 4, y: 4, z: 8, core: 2. Of those that a mesh axis runs over, the one named last changes fastest.
Arguments:
- tokens: bfloat16 [8192, 1024], P(('sp', 'tp')), may hold values from -6 to 6
- doc_ids: int32 [8192], P('sp'), may hold values from 0 to 31, never falling along the last dimension, each value on 1 to 4608 neighbouring positions
- down_query: bfloat16 [1024, 256], P('sp'), may hold values from -0.1875 to 0.1875
- down_key: bfloat16 [1024, 256], P('sp'), may hold values from -0.1875 to 0.1875
- down_rotary: bfloat16 [1024, 32], P('sp'), may hold values from -0.1875 to 0.1875
- query_gain: float32 [256], replicated, may hold values from 0.1 to 1.9
- key_gain: float32 [256], replicated, may hold values from 0.1 to 1.9
- up_query: bfloat16 [256, 1536], P('sp', 'tp'), may hold values from -0.375 to 0.375
- up_key: bfloat16 [256, 1024], P('sp', 'tp'), may hold values from -0.375 to 0.375
- up_value: bfloat16 [256, 1024], P('sp', 'tp'), may hold values from -0.375 to 0.375
- output_weight: bfloat16 [1024, 1024], P('tp', 'sp'), may hold values from -0.1875 to 0.1875
- out_gain: float32 [1024], replicated, may hold values from 0.1 to 1.9
Outputs:
- mixed: bfloat16 [8192, 1024], P(('sp', 'tp'))
- log_sums: float32 [8192, 16], P('sp', 'tp')
The draws below stay inside these ranges and needn't reach their ends.
Inputs may be any that keep to these rules, and one draw needn't show every extreme that they name: doc_ids never fall along the sequence and run from 0 to at most the number of devices along sp minus one; each document has 1 to 4608 positions, and one document has exactly that many.
All inputs are finite; a program needn't handle non-finite values.
Results may differ from the reference program's by a relative error of at most 0.02.
Values may be sent and summed in bfloat16 or wider, within the bound.
No kernel may reach another device: no remote copies, remote signals or barrier semaphores. Data moves between devices by JAX's collectives and lax.ppermute only.
A program may use at most 64 MiB of HBM per device.

```python
import math
import jax
import jax.numpy as jnp
import numpy as np
from jax import lax

D = 1024
HEADS = 16
Q_RANK = 256
KV_RANK = 256
NOPE = 64
ROPE = 32
VDIM = 64
TOK_DEV = 256
TOKENS = 8192
N_SP = 32


def block_scale(key, extent, pieces, least, high):
    def one(position, shards_of):
        draws = jax.random.uniform(jax.random.fold_in(jax.random.fold_in(key, 6), position), (shards_of,), jnp.float32, least / len(pieces), high / len(pieces))
        return jnp.repeat(jnp.exp(draws), extent[position] // shards_of).reshape((-1,) + (1,) * (len(extent) - position - 1))

    level = one(*pieces[0])
    for cut in pieces[1:]:
        level = level * one(*cut)
    return level


def profile(number_of, total, bound, skew):
    portions = [(1 << 20) // math.isqrt(standing ** skew) + 1 for standing in range(2, number_of + 1)]
    rest, given = total - bound - (number_of - 1), [1] * (number_of - 1)
    while rest > 0:
        movable = [i for i in range(number_of - 1) if given[i] < bound]
        pool, budget = sum([portions[i] for i in movable]), rest
        for i in movable:
            more = min(bound - given[i], max(1, budget * portions[i] // pool), rest)
            given[i] = given[i] + more
            rest = rest - more
    return np.array([bound] + given)


def uneven_parts(key, count, total, bound, lean):
    if count == 2:
        one = jax.random.randint(key, (), max(1, total - bound), min(bound, total - 1) + 1)
        return jnp.stack([one, total - one])
    lengths = jnp.asarray(profile(count, total, bound, lean), jnp.int32)
    twos = (count - 1) // 2
    source_of, sink = lengths[1:1 + 2 * twos:2], lengths[2:2 + 2 * twos:2]
    room = jnp.minimum(source_of - 1, bound - sink)
    moved = jax.random.randint(jax.random.fold_in(key, 1), (twos,), 0, 1 << 20) % (room + 1)
    lengths = lengths.at[1:1 + 2 * twos:2].set(source_of - moved).at[2:2 + 2 * twos:2].set(sink + moved)
    return lengths[jax.random.permutation(jax.random.fold_in(key, 2), count)]


def normal_values(own_key, shape, width, bound, split=(), kind=jnp.bfloat16):
    values = width * jax.random.normal(own_key, shape, jnp.float32)
    if split:
        values = values * block_scale(own_key, shape, split, -0.22, 0.18)
    return jnp.clip(values, -bound, bound).astype(kind)


def setup_inputs(seed: int = 0) -> dict:
    seeds = jax.random.split(jax.random.key(seed), 13)
    return {
        "tokens": normal_values(seeds[0], (TOKENS, D), 1.0, 6.0, ((0, 256),)),
        "doc_ids": jnp.searchsorted(jnp.cumsum(uneven_parts(seeds[1], N_SP, TOKENS, TOK_DEV * N_SP // 2 + 2 * TOK_DEV, 2)), jnp.arange(TOKENS), side="right").astype(jnp.int32),
        "down_query": normal_values(seeds[2], (D, Q_RANK), D ** -0.5, 0.1875, ((0, 32),)),
        "down_key": normal_values(seeds[3], (D, KV_RANK), D ** -0.5, 0.1875, ((0, 32),)),
        "down_rotary": normal_values(seeds[4], (D, ROPE), D ** -0.5, 0.1875, ((0, 32),)),
        "query_gain": jnp.clip(1.0 + 0.18 * jax.random.normal(seeds[5], (Q_RANK,), jnp.float32), 0.1, 1.9),
        "key_gain": jnp.clip(1.0 + 0.18 * jax.random.normal(seeds[6], (KV_RANK,), jnp.float32), 0.1, 1.9),
        "up_query": normal_values(seeds[7], (Q_RANK, HEADS * (NOPE + ROPE)), Q_RANK ** -0.5, 0.375, ((0, 32), (1, 8))),
        "up_key": normal_values(seeds[8], (KV_RANK, HEADS * NOPE), KV_RANK ** -0.5, 0.375, ((0, 32), (1, 8))),
        "up_value": normal_values(seeds[9], (KV_RANK, HEADS * VDIM), KV_RANK ** -0.5, 0.375, ((0, 32), (1, 8))),
        "output_weight": normal_values(seeds[10], (HEADS * VDIM, D), (HEADS * VDIM) ** -0.5, 0.1875, ((0, 8), (1, 32))),
        "out_gain": jnp.clip(1.0 + 0.18 * jax.random.normal(seeds[11], (D,), jnp.float32), 0.1, 1.9),
    }


NEG_BIG = -1e+30
THETA = 10000.0
EPS = 1e-06

def settle(quantity):
    return lax.optimization_barrier(quantity.astype(jnp.bfloat16))

def rms_gain(summed, gain_vector):
    widened = settle(summed).astype(jnp.float32)
    scaled = widened * lax.rsqrt(lax.optimization_barrier(jnp.mean(widened * widened, axis=-1, keepdims=True)) + EPS)
    return (scaled * gain_vector).astype(jnp.bfloat16)

def rotate(vectors, positions):
    half_width = vectors.shape[-1] // 2
    inverse = THETA ** (-jnp.arange(half_width, dtype=jnp.float32) / half_width)
    angles = positions.astype(jnp.float32)[:, None] * inverse[None, :]
    angles = angles.reshape((vectors.shape[0],) + (1,) * (vectors.ndim - 2) + (half_width,))
    cosine_part = jnp.cos(angles)
    sine_part = jnp.sin(angles)
    widened = vectors.astype(jnp.float32)
    front_half = widened[..., :half_width]
    back_half = widened[..., half_width:]
    return jnp.concatenate([front_half * cosine_part - back_half * sine_part, back_half * cosine_part + front_half * sine_part], axis=-1).astype(jnp.bfloat16)

def reference(tokens, doc_ids, down_query, down_key, down_rotary, query_gain, key_gain, up_query, up_key, up_value, output_weight, out_gain):
    highest = lax.Precision.HIGHEST
    positions = jnp.arange(TOKENS, dtype=jnp.int32)
    query_latent = rms_gain(jnp.dot(tokens, down_query, preferred_element_type=jnp.float32), query_gain)
    key_latent = rms_gain(jnp.dot(tokens, down_key, preferred_element_type=jnp.float32), key_gain)
    key_turned = rotate(settle(jnp.dot(tokens, down_rotary, preferred_element_type=jnp.float32)), positions)
    queries = settle(jnp.dot(query_latent, up_query, preferred_element_type=jnp.float32))
    queries = queries.reshape(TOKENS, HEADS, NOPE + ROPE)
    query_plain = queries[..., :NOPE]
    query_turned = rotate(queries[..., NOPE:], positions)
    key_plain = settle(jnp.dot(key_latent, up_key, preferred_element_type=jnp.float32)).reshape(TOKENS, HEADS, NOPE)
    values = settle(jnp.dot(key_latent, up_value, preferred_element_type=jnp.float32)).reshape(TOKENS, HEADS, VDIM)
    score_scale = 1.0 / math.sqrt(NOPE + ROPE)
    plain_wide = key_plain.astype(jnp.float32)
    turned_wide = key_turned.astype(jnp.float32)
    values_wide = values.astype(jnp.float32)

    def one_block(block_parts):
        plain_block, turned_block, docs_block = block_parts
        scores = jnp.einsum('qhd,khd->hqk', plain_block.astype(jnp.float32), plain_wide, precision=highest)
        scores = scores + jnp.einsum('qhr,kr->hqk', turned_block.astype(jnp.float32), turned_wide, precision=highest)
        scores = scores * score_scale
        same_doc = (docs_block[:, None] == doc_ids[None, :])[None]
        top_score = lax.optimization_barrier(jnp.max(jnp.where(same_doc, scores, NEG_BIG), axis=-1, keepdims=True))
        weights = jnp.where(same_doc, jnp.exp(scores - top_score), 0.0)
        weight_sum = lax.optimization_barrier(jnp.sum(weights, axis=-1))
        mixed_rows = jnp.einsum('hqk,khv->qhv', settle(weights).astype(jnp.float32), values_wide, precision=highest)
        mixed_rows = mixed_rows / weight_sum.T[:, :, None]
        return (mixed_rows, (top_score[..., 0] + jnp.log(weight_sum)).T)
    blocks = (query_plain.reshape(N_SP, TOK_DEV, HEADS, NOPE), query_turned.reshape(N_SP, TOK_DEV, HEADS, ROPE), doc_ids.reshape(N_SP, TOK_DEV))
    mixed_rows, log_sums = lax.map(one_block, blocks)
    attended = mixed_rows.reshape(TOKENS, HEADS * VDIM).astype(jnp.bfloat16)
    log_sums = log_sums.reshape(TOKENS, HEADS)
    projected = jnp.dot(attended, output_weight, preferred_element_type=jnp.float32)
    return (rms_gain(projected, out_gain), log_sums)
```

```python
import math

import jax
import jax.numpy as jnp
import numpy as np
from jax import lax
from jax.experimental import pallas as pl
from jax.experimental.pallas import tpu as pltpu
from jax.sharding import Mesh
from jax.sharding import PartitionSpec as P

NOPE = 64
ROPE = 32
VDIM = 64
NZ, NX, NY, NC = 8, 4, 4, 2
NS = NZ * NX
AXES = ("z", "x", "y", "c")
SP = ("z", "x")
TP = ("y", "c")
NEG_BIG = -1e30
FLOOR = -1e20
THETA = 10000.0
EPS = 1e-06
LN2 = math.log(2.0)
SCALE2 = 1.0 / math.sqrt(NOPE + ROPE) / LN2
BF = jnp.bfloat16
F32 = jnp.float32


VMEM = pltpu.VMEM
SMEM_SPEC = pl.BlockSpec(memory_space=pltpu.SMEM)
VMEM_SPEC = pl.BlockSpec(memory_space=pltpu.VMEM)
ANY_SPEC = pl.BlockSpec(memory_space=pl.ANY)


def call(body, outs, n_smem, n_in, scratch=(), any_from=None, cost=None):
    specs = [SMEM_SPEC] * n_smem
    for i in range(n_in):
        specs.append(ANY_SPEC if any_from is not None and i >= any_from else VMEM_SPEC)
    single = not isinstance(outs, tuple)
    return pl.pallas_call(
        body,
        out_shape=outs,
        in_specs=specs,
        out_specs=VMEM_SPEC if single else tuple(VMEM_SPEC for _ in outs),
        scratch_shapes=list(scratch),
        compiler_params=pltpu.CompilerParams(vmem_limit_bytes=50 * 1024 * 1024),
        cost_estimate=cost,
        name=body.__name__,
    )


def lanes(shape):
    return lax.broadcasted_iota(jnp.int32, shape, len(shape) - 1)


def column(row):
    return jnp.transpose(jnp.broadcast_to(row, (128, 128)))


def project(where, t0, t1, t2, t3, gathered, cos_ref, sin_ref, q_ref, k_ref, tok):
    y = where[2]
    for j, part in enumerate((t0, t1, t2, t3)):
        at = lax.rem(y - j + NY, NY)
        tok[pl.ds(pl.multiple_of(at * 32, 32), 32), :] = part[...]
    rows = tok[...]
    weights = gathered[:, 0:32, :].reshape(NS * 32, 128)
    both = jnp.dot(rows, weights, preferred_element_type=F32)
    turned = jnp.transpose(both).astype(BF)
    q_ref[...] = turned[0:64, :]
    k_ref[0:64, :] = turned[64:128, :]
    group = lanes((8, 128)) // 32
    pieces = []
    for z in range(NZ):
        piece = gathered[4 * z, 64:72, :].astype(F32)
        for g in range(1, 4):
            piece = jnp.where(group == g, gathered[4 * z + g, 64:72, :].astype(F32), piece)
        pieces.append(piece)
    rope = jnp.concatenate(pieces, axis=1)
    rope = jnp.concatenate([rope, jnp.zeros_like(rope)], axis=0).astype(BF)
    raw = lax.dot_general(rope, rows, (((1,), (1,)), ((), ())), preferred_element_type=F32)
    raw = raw[0:8, :].astype(BF).astype(F32)
    rotated = raw * cos_ref[...] + pltpu.roll(raw, 4, 0) * sin_ref[...]
    k_ref[64:72, :] = rotated.astype(BF)


def make_queries(q_in, up_own, up_other, gain, cos_ref, low_ref, high_ref, out):
    blocks = []
    for y in range(NY):
        blocks.append(
            jnp.concatenate([q_in[2 * y].astype(F32), q_in[2 * y + 1].astype(F32)], axis=1)
        )
    total = blocks[0] * blocks[0]
    for b in blocks[1:]:
        total = total + b * b
    mean = jnp.sum(total, axis=0, keepdims=True) * (1.0 / 256.0)
    inverse = lax.rsqrt(mean + EPS)
    gains = jnp.concatenate([column(gain[0:1, :]), column(gain[1:2, :])], axis=0)
    gains = jnp.concatenate([gains, gains], axis=1)
    latent = jnp.concatenate(blocks, axis=0) * inverse * gains
    latent = jnp.transpose(latent).astype(BF)
    lane = lanes((256, 128))
    for p, up in enumerate((up_own, up_other)):
        wide = up[...].astype(F32)
        plain_w = wide[:, 0:8, :].reshape(256, 128).astype(BF)
        rope_w = wide[:, 24:32, :].reshape(256, 128).astype(BF)
        plain = jnp.dot(latent, plain_w, preferred_element_type=F32) * SCALE2
        raw = jnp.dot(latent, rope_w, preferred_element_type=F32) * SCALE2
        rope = (
            raw * cos_ref[...]
            + pltpu.roll(raw, 124, 1) * low_ref[...]
            + pltpu.roll(raw, 4, 1) * high_ref[...]
        )
        for i in range(2):
            own = slice(256 * i, 256 * (i + 1))
            out[p, own, 0:128] = jnp.where(lane // 64 == i, plain, 0.0).astype(BF)
            out[p, own, 128:256] = jnp.where(lane // 32 == i, rope, 0.0).astype(BF)


def attend(
    where, q_ref, up_own, up_other, gain, key_docs, query_docs, b0, b1, b2, b3,
    keep_ref, send_ref, ml_ref, kb, s_buf, v_buf, mx, total, acc, uk, uv, gains, docs_col, sems,
):
    x0, y0, c, low, high = where[1], where[2], where[3], where[4], where[5]
    copies = [
        pltpu.make_async_copy(part, kb.at[j], sems.at[j]) for j, part in enumerate((b0, b1, b2, b3))
    ]
    for copy in copies:
        copy.start()
    for p, up in enumerate((up_own, up_other)):
        wide = up[...].astype(F32)
        own = slice(128 * p, 128 * (p + 1))
        uk[own, :] = jnp.transpose(wide[:, 8:16, :].reshape(256, 128)).astype(BF)
        uv[own, :] = jnp.transpose(wide[:, 16:24, :].reshape(256, 128)).astype(BF)
    for i in range(2):
        gains[128 * i : 128 * (i + 1), :] = column(gain[i : i + 1, :])
        docs_col[128 * i : 128 * (i + 1), :] = column(query_docs[i : i + 1, :])
    mx[...] = jnp.full(mx.shape, NEG_BIG, F32)
    total[...] = jnp.zeros(total.shape, F32)
    acc[...] = jnp.zeros(acc.shape, F32)
    for copy in copies:
        copy.wait()
    first = low // 2
    last = high // 2 + 1

    def scores(tile, carry):
        z = tile // 2
        latents, ropes = [], []
        for half in range(2):
            x = 2 * lax.rem(tile, 2) + half
            jx = lax.rem(x0 - x + NX, NX)
            parts, turned = [], []
            for y in range(NY):
                jy = lax.rem(y0 - y + NY, NY)
                third = jnp.where(c == 0, jy, jx)
                second = jnp.where(c == 0, jx, jy)
                slab = kb[third, second, z].astype(F32)
                parts.append(slab[0:64, :])
                turned.append(slab[64:72, :])
            squares = parts[0] * parts[0]
            for part in parts[1:]:
                squares = squares + part * part
            mean = jnp.sum(squares, axis=0, keepdims=True) * (1.0 / 256.0)
            inverse = lax.rsqrt(mean + EPS)
            latent = jnp.concatenate(parts, axis=0) * inverse * gains[...]
            latents.append(latent.astype(BF))
            ropes.append(jnp.concatenate(turned, axis=0).astype(BF))
        latent = jnp.concatenate(latents, axis=1)
        rope = jnp.concatenate(ropes, axis=1)
        keys = jnp.dot(uk[...], latent, preferred_element_type=F32).astype(BF)
        values = jnp.dot(uv[...], latent, preferred_element_type=F32)
        v_buf[tile] = jnp.transpose(values).astype(BF)
        blank = jnp.zeros((64, 256), BF)
        same = []
        for half in range(2):
            docs_row = key_docs[pl.ds(2 * tile + half, 1), :]
            same.append(docs_col[...] == docs_row)
        for p in range(2):
            stack = jnp.concatenate([keys[128 * p : 128 * (p + 1), :], rope, rope, blank], axis=0)
            for i in range(2):
                own = slice(256 * i, 256 * (i + 1))
                got = jnp.dot(q_ref[p, own, :], stack, preferred_element_type=F32)
                lhs = jnp.where(same[0], got[:, 0:128], NEG_BIG)
                rhs = jnp.where(same[1], got[:, 128:256], NEG_BIG)
                s_buf[tile, 2 * p + i, :, 0:128] = lhs
                s_buf[tile, 2 * p + i, :, 128:256] = rhs
                mx[2 * p + i] = jnp.maximum(mx[2 * p + i], jnp.maximum(lhs, rhs))
        return carry

    lax.fori_loop(first, last, scores, 0)
    tops = []
    for h in range(4):
        top = jnp.max(mx[h], axis=1, keepdims=True)
        top = jnp.maximum(top, FLOOR)
        mx[h] = jnp.broadcast_to(top, (256, 128))
        tops.append(top)

    def weigh(tile, carry):
        v = v_buf[tile]
        lane = lanes((256, 256)) // 64
        result = acc[...]
        for h in range(4):
            top = mx[h]
            lhs = jnp.exp2(s_buf[tile, h, :, 0:128] - top)
            rhs = jnp.exp2(s_buf[tile, h, :, 128:256] - top)
            total[h] = total[h] + lhs + rhs
            weights = jnp.concatenate([lhs.astype(BF), rhs.astype(BF)], axis=1)
            own = jnp.where(lane == h, v, jnp.zeros_like(v))
            result = result + jnp.dot(weights, own, preferred_element_type=F32)
        acc[...] = result
        return carry

    lax.fori_loop(first, last, weigh, 0)
    lane = lanes((256, 128))
    packed = jnp.zeros((256, 128), F32)
    for h in range(4):
        packed = jnp.where(lane == h, tops[h], packed)
        packed = jnp.where(lane == 4 + h, jnp.sum(total[h], axis=1, keepdims=True), packed)
    ml_ref[...] = packed
    keep_ref[...] = acc[pl.ds(pl.multiple_of(c * 128, 128), 128), :]
    send_ref[...] = acc[pl.ds(pl.multiple_of((1 - c) * 128, 128), 128), :].astype(BF)


def combine(where, keep, got, ml_own, ml_got, w_own, w_other, part_ref, lse_ref, f_own, f_got):
    c = where[3]
    own = ml_own[...]
    other = ml_got[...]
    for h in range(4):
        k = (h + 2) % 4
        m0, l0 = own[:, h : h + 1], own[:, 4 + h : 5 + h]
        m1, l1 = other[:, k : k + 1], other[:, 4 + k : 5 + k]
        top = jnp.maximum(m0, m1)
        e0 = jnp.exp2(m0 - top)
        e1 = jnp.exp2(m1 - top)
        weight_sum = l0 * e0 + l1 * e1
        if h < 2:
            lse = (top + jnp.log2(weight_sum)) * LN2
            for half in range(2):
                for y in range(NY):
                    lse_ref[64 * y + 32 * half : 64 * y + 32 * half + 32, h : h + 1] = lse[
                        128 * half + 32 * y : 128 * half + 32 * y + 32, :
                    ]
        f_own[h] = jnp.broadcast_to(e0 / weight_sum, (256, 128))
        f_got[h] = jnp.broadcast_to(e1 / weight_sum, (256, 128))
    rows = pl.ds(pl.multiple_of(c * 128, 128), 128)
    lane = lanes((128, 128)) // 64
    result = jnp.zeros((128, 1024), F32)
    for p, w in enumerate((w_own, w_other)):
        a = jnp.where(lane == 0, f_own[2 * p, rows, :], f_own[2 * p + 1, rows, :])
        b = jnp.where(lane == 0, f_got[2 * p, rows, :], f_got[2 * p + 1, rows, :])
        mine = keep[:, 128 * p : 128 * (p + 1)]
        theirs = got[:, 128 * (1 - p) : 128 * (2 - p)].astype(F32)
        attended = (mine * a + theirs * b).astype(BF)
        result = result + lax.dot_general(
            attended, w[...].reshape(1024, 128), (((1,), (1,)), ((), ())),
            preferred_element_type=F32,
        )
    part_ref[...] = result.astype(BF).reshape(NY, 32, 1024)


def finish(parts, gain, out):
    summed = parts[0].astype(F32)
    for y in range(1, NY):
        summed = summed + parts[y].astype(F32)
    wide = summed.astype(BF).astype(F32)
    mean = jnp.mean(wide * wide, axis=1, keepdims=True)
    out[...] = (wide * lax.rsqrt(mean + EPS) * gain[...]).astype(BF)


def spread(value, axes, count):
    return lax.all_to_all(jnp.broadcast_to(value[None], (count,) + value.shape), axes, 0, 0)


def flat(z, x, y, c):
    return ((z * NX + x) * NY + y) * NC + c


def shift_pairs(stage, j):
    pairs = []
    for z in range(NZ):
        for x in range(NX):
            for y in range(NY):
                for c in range(NC):
                    along_x = (c == 0) == (stage == 2)
                    to = flat(z, (x + j) % NX, y, c) if along_x else flat(z, x, (y + j) % NY, c)
                    pairs.append((flat(z, x, y, c), to))
    return pairs


def after(value, *others):
    return lax.optimization_barrier((value,) + others)[0]


def local(
    tokens, doc_ids, down_query, down_key, down_rotary, query_gain, key_gain,
    up_query, up_key, up_value, output_weight, out_gain,
):
    z = lax.axis_index("z")
    x = lax.axis_index("x")
    y = lax.axis_index("y")
    c = lax.axis_index("c")
    sp = z * NX + x
    here = jnp.stack([z, x, y, c]).astype(jnp.int32)
    swap = [(0, 1), (1, 0)]

    shifted = [
        lax.ppermute(tokens, "y", [(i, (i + j) % NY) for i in range(NY)]) for j in range(1, NY)
    ]

    down = jnp.concatenate(
        [
            lax.dynamic_slice_in_dim(down_query, 64 * y, 64, 1),
            lax.dynamic_slice_in_dim(down_key, 64 * y, 64, 1),
        ],
        axis=1,
    )
    rotary = lax.dynamic_index_in_dim(down_rotary.reshape(32, 2, 4, 4), y, 2, keepdims=False)
    rotary = jnp.tile(rotary.reshape(32, 8).T, (1, 4))
    heads = up_query.reshape(8, 2, NOPE + ROPE)
    plain = heads[:, :, :NOPE].reshape(8, 128)
    turning = heads[:, :, NOPE:].reshape(8, 2, 2, 4, 4).transpose(0, 1, 3, 2, 4).reshape(8, 64)
    docs = doc_ids.astype(BF).reshape(8, 32)
    mixed_rows = jnp.concatenate([turning, docs, jnp.zeros((8, 32), BF)], axis=1)
    message = jnp.concatenate([down, plain, up_key, up_value, mixed_rows, rotary], axis=0)
    gathered = spread(message, SP, NS)

    f32_base = (sp * 256).astype(F32)
    key_tok = lax.broadcasted_iota(jnp.int32, (8, 128), 1)
    key_row = lax.broadcasted_iota(jnp.int32, (8, 128), 0)
    key_pos = f32_base + (64 * (key_tok // 32) + 32 * c + key_tok % 32).astype(F32)
    key_freq = THETA ** (-(4 * y + key_row % 4).astype(F32) / 16)
    key_angle = key_pos * key_freq
    key_cos = jnp.cos(key_angle)
    key_sin = jnp.sin(key_angle) * jnp.where(key_row < 4, -1.0, 1.0)
    tok = lax.broadcasted_iota(jnp.int32, (256, 128), 0)
    lane = lax.broadcasted_iota(jnp.int32, (256, 128), 1)
    pos = f32_base + (64 * ((tok % 128) // 32) + 32 * (tok // 128) + tok % 32).astype(F32)
    freq = THETA ** (-(4 * ((lane % 32) // 8) + lane % 4).astype(F32) / 16)
    angle = pos * freq
    used = lane < 64
    is_low = (lane // 4) % 2 == 0
    cos = jnp.where(used, jnp.cos(angle), 0.0)
    sine = jnp.sin(angle)
    low_sin = jnp.where(used & is_low, -sine, 0.0)
    high_sin = jnp.where(used & ~is_low, sine, 0.0)

    q_part, k_part = call(
        project,
        (jax.ShapeDtypeStruct((64, 128), BF), jax.ShapeDtypeStruct((72, 128), BF)),
        1, 7, scratch=[VMEM((128, 1024), BF)],
    )(here, tokens, *shifted, gathered, key_cos, key_sin)

    stage1 = spread(k_part, "z", NZ)
    stage2 = [stage1] + [lax.ppermute(stage1, AXES, shift_pairs(2, j)) for j in range(1, 4)]
    held = jnp.stack(stage2)
    stage3 = [held] + [lax.ppermute(held, AXES, shift_pairs(3, j)) for j in range(1, 4)]

    up_own = gathered[:, 32:64, :]
    up_other = lax.ppermute(up_own, "c", swap)
    q_all = spread(after(q_part, stage1), TP, NY * NC)
    queries = call(
        make_queries, jax.ShapeDtypeStruct((2, 512, 256), BF), 0, 7
    )(q_all, up_own, up_other, query_gain.reshape(2, 128), cos, low_sin, high_sin)

    out_own = spread(after(output_weight.T, q_all), SP, NS)
    out_other = lax.ppermute(out_own, "c", swap)

    all_docs = gathered[:, 56:64, 64:96].astype(F32)
    key_docs = lax.dynamic_index_in_dim(
        all_docs.reshape(NS, 4, 2, 32), c, 2, keepdims=False
    ).reshape(NS, 128)
    query_docs = doc_ids.astype(F32).reshape(4, 2, 32).transpose(1, 0, 2).reshape(2, 128)
    own_first = doc_ids[0].astype(F32)
    own_last = doc_ids[255].astype(F32)
    low = jnp.sum((all_docs[:, 7, 31] < own_first).astype(jnp.int32))
    high = NS - 1 - jnp.sum((all_docs[:, 0, 0] > own_last).astype(jnp.int32))
    where = jnp.stack([z, x, y, c, low, high]).astype(jnp.int32)

    keep, send, ml = call(
        attend,
        (
            jax.ShapeDtypeStruct((128, 256), F32),
            jax.ShapeDtypeStruct((128, 256), BF),
            jax.ShapeDtypeStruct((256, 128), F32),
        ),
        1, 10, any_from=6,
        scratch=[
            VMEM((4, 4, NZ, 72, 128), BF),
            VMEM((16, 4, 256, 256), F32),
            VMEM((16, 256, 256), BF),
            VMEM((4, 256, 128), F32),
            VMEM((4, 256, 128), F32),
            VMEM((256, 256), F32),
            VMEM((256, 256), BF),
            VMEM((256, 256), BF),
            VMEM((256, 128), F32),
            VMEM((256, 128), F32),
            pltpu.SemaphoreType.DMA((4,)),
        ],
    )(where, queries, up_own, up_other, key_gain.reshape(2, 128), key_docs, query_docs, *stage3)

    got = lax.ppermute(send, "c", swap)
    ml_got = lax.ppermute(ml, "c", swap)
    part, log_sums = call(
        combine,
        (jax.ShapeDtypeStruct((NY, 32, 1024), BF), jax.ShapeDtypeStruct((256, 2), F32)),
        1, 6, scratch=[VMEM((4, 256, 128), F32), VMEM((4, 256, 128), F32)],
    )(here, keep, got, ml, ml_got, out_own, out_other)
    parts = lax.all_to_all(part, "y", 0, 0)
    mixed = call(finish, jax.ShapeDtypeStruct((32, 1024), BF), 0, 2)(
        parts, out_gain.reshape(1, 1024)
    )
    return mixed, log_sums


def solution(mesh):
    finer = Mesh(mesh.devices.reshape(NZ, NX, NY, NC), AXES)
    return jax.shard_map(
        local,
        mesh=finer,
        in_specs=(
            P(AXES, None), P(SP), P(SP, None), P(SP, None), P(SP, None), P(), P(),
            P(SP, TP), P(SP, TP), P(SP, TP), P(TP, SP), P(),
        ),
        out_specs=(P(AXES, None), P(SP, TP)),
        check_vma=False,
    )
```

```python
import math

import jax
import jax.numpy as jnp
from jax import lax
from jax.experimental import pallas as pl
from jax.experimental.pallas import tpu as pltpu
from jax.sharding import Mesh
from jax.sharding import PartitionSpec as P


NOPE = 64
ROPE = 32
NZ, NX, NY, NC = 8, 4, 4, 2
NS = NZ * NX
AXES = ("z", "x", "y", "c")
SP = ("z", "x")
TP = ("y", "c")
NEG_BIG = -1e30
FLOOR = -1e20
THETA = 10000.0
EPS = 1e-06
LN2 = math.log(2.0)
SCALE2 = 1.0 / math.sqrt(NOPE + ROPE) / LN2
BF = jnp.bfloat16
F32 = jnp.float32


VMEM = pltpu.VMEM
SMEM_SPEC = pl.BlockSpec(memory_space=pltpu.SMEM)
VMEM_SPEC = pl.BlockSpec(memory_space=pltpu.VMEM)
ANY_SPEC = pl.BlockSpec(memory_space=pl.ANY)


def call(body, outs, n_smem, n_in, scratch=(), any_from=None, cost=None):
    specs = [SMEM_SPEC] * n_smem
    for i in range(n_in):
        specs.append(ANY_SPEC if any_from is not None and i >= any_from else VMEM_SPEC)
    single = not isinstance(outs, tuple)
    return pl.pallas_call(
        body,
        out_shape=outs,
        in_specs=specs,
        out_specs=VMEM_SPEC if single else tuple(VMEM_SPEC for _ in outs),
        scratch_shapes=list(scratch),
        compiler_params=pltpu.CompilerParams(vmem_limit_bytes=50 * 1024 * 1024),
        cost_estimate=cost,
    )


def lanes(shape):
    return lax.broadcasted_iota(jnp.int32, shape, len(shape) - 1)


def column(row):
    return jnp.transpose(jnp.broadcast_to(row, (128, 128)))


def pack(where, dq, dk, dr, out, flipped):
    y = where[2]

    def chosen(ref):
        block = ref[:, 0:64]
        for k in range(1, NY):
            block = jnp.where(y == k, ref[:, 64 * k : 64 * (k + 1)], block)
        return block

    block = jnp.concatenate([chosen(dq), chosen(dk)], axis=1)
    rope = dr[...].astype(F32)
    rope = jnp.concatenate([rope, jnp.zeros((32, 96), F32)], axis=1)
    flipped[...] = jnp.transpose(jnp.concatenate([rope] * 4, axis=0))
    turned = jnp.concatenate([flipped[pl.ds(4 * y, 4), :], flipped[pl.ds(16 + 4 * y, 4), :]], axis=0)
    turned = turned.astype(BF)
    for s in range(NS):
        out[s, 0:32, :] = block
        out[s, 32:40, :] = turned


def project(where, t0, t1, t2, t3, gathered, cos_ref, sin_ref, q_ref, k_ref, tok):
    y = where[2]
    for j, part in enumerate((t0, t1, t2, t3)):
        at = lax.rem(y - j + NY, NY)
        tok[pl.ds(pl.multiple_of(at * 32, 32), 32), :] = part[...]
    rows = tok[...]
    weights = gathered[:, 0:32, :].reshape(NS * 32, 128)
    both = jnp.dot(rows, weights, preferred_element_type=F32)
    turned = jnp.transpose(both).astype(BF)
    for t in range(NY * NC):
        q_ref[t] = turned[0:64, :]
    for t in range(NZ):
        k_ref[t, 0:64, :] = turned[64:128, :]
    group = lanes((8, 128)) // 32
    pieces = []
    for z in range(NZ):
        piece = gathered[4 * z, 32:40, :].astype(F32)
        for g in range(1, 4):
            piece = jnp.where(group == g, gathered[4 * z + g, 32:40, :].astype(F32), piece)
        pieces.append(piece)
    rope = jnp.concatenate(pieces, axis=1)
    rope = jnp.concatenate([rope, jnp.zeros_like(rope)], axis=0).astype(BF)
    raw = lax.dot_general(rope, rows, (((1,), (1,)), ((), ())), preferred_element_type=F32)
    raw = raw[0:8, :].astype(BF).astype(F32)
    rotated = raw * cos_ref[...] + pltpu.roll(raw, 4, 0) * sin_ref[...]
    rotated = rotated.astype(BF)
    for t in range(NZ):
        k_ref[t, 64:72, :] = rotated


def make_queries(q_in, up_own, up_other, gain, cos_ref, low_ref, high_ref, out):
    blocks = []
    for y in range(NY):
        blocks.append(
            jnp.concatenate([q_in[2 * y].astype(F32), q_in[2 * y + 1].astype(F32)], axis=1)
        )
    total = blocks[0] * blocks[0]
    for b in blocks[1:]:
        total = total + b * b
    mean = jnp.sum(total, axis=0, keepdims=True) * (1.0 / 256.0)
    inverse = lax.rsqrt(mean + EPS)
    gains = jnp.concatenate([column(gain[0:1, :]), column(gain[1:2, :])], axis=0)
    gains = jnp.concatenate([gains, gains], axis=1)
    latent = jnp.concatenate(blocks, axis=0) * inverse * gains
    latent = jnp.transpose(latent).astype(BF)
    lane = lanes((256, 128))
    for p, up in enumerate((up_own, up_other)):
        wide = up[...].astype(F32)
        plain_w = wide[:, 0:8, :].reshape(256, 128).astype(BF)
        rope_w = wide[:, 24:32, :].reshape(256, 128).astype(BF)
        plain = jnp.dot(latent, plain_w, preferred_element_type=F32) * SCALE2
        raw = jnp.dot(latent, rope_w, preferred_element_type=F32) * SCALE2
        rope = (
            raw * cos_ref[...]
            + pltpu.roll(raw, 124, 1) * low_ref[...]
            + pltpu.roll(raw, 4, 1) * high_ref[...]
        )
        for i in range(2):
            own = slice(256 * i, 256 * (i + 1))
            out[p, own, 0:128] = jnp.where(lane // 64 == i, plain, 0.0).astype(BF)
            out[p, own, 128:256] = jnp.where(lane // 32 == i, rope, 0.0).astype(BF)


def attend(
    where, q_ref, up_own, up_other, gain, key_docs, query_docs, b0, b1, b2, b3,
    keep_ref, send_ref, ml_ref, kb, s_buf, v_buf, mx, total, acc, uk, uv, gains, docs_col, sems,
):
    x0, y0, c, low, high = where[1], where[2], where[3], where[4], where[5]
    copies = [
        pltpu.make_async_copy(part, kb.at[j], sems.at[j]) for j, part in enumerate((b0, b1, b2, b3))
    ]
    for copy in copies:
        copy.start()
    for p, up in enumerate((up_own, up_other)):
        wide = up[...].astype(F32)
        own = slice(128 * p, 128 * (p + 1))
        uk[own, :] = jnp.transpose(wide[:, 8:16, :].reshape(256, 128)).astype(BF)
        uv[own, :] = jnp.transpose(wide[:, 16:24, :].reshape(256, 128)).astype(BF)
    for i in range(2):
        gains[128 * i : 128 * (i + 1), :] = column(gain[i : i + 1, :])
        docs_col[128 * i : 128 * (i + 1), :] = column(query_docs[i : i + 1, :])
    mx[...] = jnp.full(mx.shape, NEG_BIG, F32)
    total[...] = jnp.zeros(total.shape, F32)
    acc[...] = jnp.zeros(acc.shape, F32)
    for copy in copies:
        copy.wait()
    first = low // 2
    last = high // 2 + 1

    def scores(tile, carry):
        z = tile // 2
        latents, ropes = [], []
        for half in range(2):
            x = 2 * lax.rem(tile, 2) + half
            jx = lax.rem(x0 - x + NX, NX)
            parts, turned = [], []
            for y in range(NY):
                jy = lax.rem(y0 - y + NY, NY)
                third = jnp.where(c == 0, jy, jx)
                second = jnp.where(c == 0, jx, jy)
                slab = kb[third, second, z].astype(F32)
                parts.append(slab[0:64, :])
                turned.append(slab[64:72, :])
            squares = parts[0] * parts[0]
            for part in parts[1:]:
                squares = squares + part * part
            mean = jnp.sum(squares, axis=0, keepdims=True) * (1.0 / 256.0)
            inverse = lax.rsqrt(mean + EPS)
            latent = jnp.concatenate(parts, axis=0) * inverse * gains[...]
            latents.append(latent.astype(BF))
            ropes.append(jnp.concatenate(turned, axis=0).astype(BF))
        latent = jnp.concatenate(latents, axis=1)
        rope = jnp.concatenate(ropes, axis=1)
        keys = jnp.dot(uk[...], latent, preferred_element_type=F32).astype(BF)
        values = jnp.dot(uv[...], latent, preferred_element_type=F32)
        v_buf[tile] = jnp.transpose(values).astype(BF)
        blank = jnp.zeros((64, 256), BF)
        same = []
        for half in range(2):
            docs_row = key_docs[pl.ds(2 * tile + half, 1), :]
            same.append(docs_col[...] == docs_row)
        for p in range(2):
            stack = jnp.concatenate([keys[128 * p : 128 * (p + 1), :], rope, rope, blank], axis=0)
            for i in range(2):
                own = slice(256 * i, 256 * (i + 1))
                got = jnp.dot(q_ref[p, own, :], stack, preferred_element_type=F32)
                lhs = jnp.where(same[0], got[:, 0:128], NEG_BIG)
                rhs = jnp.where(same[1], got[:, 128:256], NEG_BIG)
                s_buf[tile, 2 * p + i, :, 0:128] = lhs
                s_buf[tile, 2 * p + i, :, 128:256] = rhs
                mx[2 * p + i] = jnp.maximum(mx[2 * p + i], jnp.maximum(lhs, rhs))
        return carry

    lax.fori_loop(first, last, scores, 0)
    tops = []
    for h in range(4):
        top = jnp.max(mx[h], axis=1, keepdims=True)
        top = jnp.maximum(top, FLOOR)
        mx[h] = jnp.broadcast_to(top, (256, 128))
        tops.append(top)

    def weigh(tile, carry):
        v = v_buf[tile]
        lane = lanes((256, 256)) // 64
        result = acc[...]
        for h in range(4):
            top = mx[h]
            lhs = jnp.exp2(s_buf[tile, h, :, 0:128] - top)
            rhs = jnp.exp2(s_buf[tile, h, :, 128:256] - top)
            total[h] = total[h] + lhs + rhs
            weights = jnp.concatenate([lhs.astype(BF), rhs.astype(BF)], axis=1)
            own = jnp.where(lane == h, v, jnp.zeros_like(v))
            result = result + jnp.dot(weights, own, preferred_element_type=F32)
        acc[...] = result
        return carry

    lax.fori_loop(first, last, weigh, 0)
    lane = lanes((256, 128))
    packed = jnp.zeros((256, 128), F32)
    for h in range(4):
        packed = jnp.where(lane == h, tops[h], packed)
        packed = jnp.where(lane == 4 + h, jnp.sum(total[h], axis=1, keepdims=True), packed)
    ml_ref[...] = packed
    keep_ref[...] = acc[pl.ds(pl.multiple_of(c * 128, 128), 128), :]
    send_ref[...] = acc[pl.ds(pl.multiple_of((1 - c) * 128, 128), 128), :].astype(BF)


def combine(where, keep, got, ml_own, ml_got, w_own, w_other, part_ref, lse_ref, f_own, f_got):
    c = where[3]
    own = ml_own[...]
    other = ml_got[...]
    for h in range(4):
        k = (h + 2) % 4
        m0, l0 = own[:, h : h + 1], own[:, 4 + h : 5 + h]
        m1, l1 = other[:, k : k + 1], other[:, 4 + k : 5 + k]
        top = jnp.maximum(m0, m1)
        e0 = jnp.exp2(m0 - top)
        e1 = jnp.exp2(m1 - top)
        weight_sum = l0 * e0 + l1 * e1
        if h < 2:
            lse = (top + jnp.log2(weight_sum)) * LN2
            for half in range(2):
                for y in range(NY):
                    lse_ref[64 * y + 32 * half : 64 * y + 32 * half + 32, h : h + 1] = lse[
                        128 * half + 32 * y : 128 * half + 32 * y + 32, :
                    ]
        f_own[h] = jnp.broadcast_to(e0 / weight_sum, (256, 128))
        f_got[h] = jnp.broadcast_to(e1 / weight_sum, (256, 128))
    rows = pl.ds(pl.multiple_of(c * 128, 128), 128)
    lane = lanes((128, 128)) // 64
    result = jnp.zeros((128, 1024), F32)
    for p, w in enumerate((w_own, w_other)):
        a = jnp.where(lane == 0, f_own[2 * p, rows, :], f_own[2 * p + 1, rows, :])
        b = jnp.where(lane == 0, f_got[2 * p, rows, :], f_got[2 * p + 1, rows, :])
        mine = keep[:, 128 * p : 128 * (p + 1)]
        theirs = got[:, 128 * (1 - p) : 128 * (2 - p)].astype(F32)
        attended = (mine * a + theirs * b).astype(BF)
        result = result + lax.dot_general(
            attended, w[:, 32:64, :].reshape(1024, 128), (((1,), (1,)), ((), ())),
            preferred_element_type=F32,
        )
    part_ref[...] = result.astype(BF).reshape(NY, 32, 1024)


def finish(parts, gain, out):
    summed = parts[0].astype(F32)
    for y in range(1, NY):
        summed = summed + parts[y].astype(F32)
    wide = summed.astype(BF).astype(F32)
    mean = jnp.mean(wide * wide, axis=1, keepdims=True)
    out[...] = (wide * lax.rsqrt(mean + EPS) * gain[...]).astype(BF)


def flat(z, x, y, c):
    return ((z * NX + x) * NY + y) * NC + c


def shift_pairs(stage, j):
    pairs = []
    for z in range(NZ):
        for x in range(NX):
            for y in range(NY):
                for c in range(NC):
                    along_x = (c == 0) == (stage == 2)
                    to = flat(z, (x + j) % NX, y, c) if along_x else flat(z, x, (y + j) % NY, c)
                    pairs.append((flat(z, x, y, c), to))
    return pairs


def layer(
    tokens, doc_ids, down_query, down_key, down_rotary, query_gain, key_gain,
    up_query, up_key, up_value, output_weight, out_gain,
):
    z = lax.axis_index("z")
    x = lax.axis_index("x")
    y = lax.axis_index("y")
    c = lax.axis_index("c")
    sp = z * NX + x
    here = jnp.stack([z, x, y, c]).astype(jnp.int32)
    swap = [(0, 1), (1, 0)]

    message = call(
        pack, jax.ShapeDtypeStruct((NS, 40, 128), BF), 1, 3, scratch=[VMEM((128, 128), F32)]
    )(here, down_query, down_key, down_rotary)
    gathered = lax.all_to_all(message, SP, 0, 0)

    shifted = [
        lax.ppermute(tokens, "y", [(i, (i + j) % NY) for i in range(NY)]) for j in range(1, NY)
    ]

    heads = up_query.reshape(8, 2, NOPE + ROPE)
    plain = heads[:, :, :NOPE].reshape(8, 128)
    turning = heads[:, :, NOPE:].reshape(8, 2, 2, 4, 4).transpose(0, 1, 3, 2, 4).reshape(8, 64)
    docs = doc_ids.astype(BF).reshape(8, 32)
    mixed_rows = jnp.concatenate([turning, docs, jnp.zeros((8, 32), BF)], axis=1)
    later = jnp.concatenate([plain, up_key, up_value, mixed_rows, output_weight.T], axis=0)
    later = jnp.broadcast_to(later[None], (NS, 64, 128))

    f32_base = (sp * 256).astype(F32)
    key_tok = lax.broadcasted_iota(jnp.int32, (8, 128), 1)
    key_row = lax.broadcasted_iota(jnp.int32, (8, 128), 0)
    key_pos = f32_base + (64 * (key_tok // 32) + 32 * c + key_tok % 32).astype(F32)
    key_freq = THETA ** (-(4 * y + key_row % 4).astype(F32) / 16)
    key_angle = key_pos * key_freq
    key_cos = jnp.cos(key_angle)
    key_sin = jnp.sin(key_angle) * jnp.where(key_row < 4, -1.0, 1.0)
    tok = lax.broadcasted_iota(jnp.int32, (256, 128), 0)
    lane = lax.broadcasted_iota(jnp.int32, (256, 128), 1)
    pos = f32_base + (64 * ((tok % 128) // 32) + 32 * (tok // 128) + tok % 32).astype(F32)
    freq = THETA ** (-(4 * ((lane % 32) // 8) + lane % 4).astype(F32) / 16)
    angle = pos * freq
    used = lane < 64
    is_low = (lane // 4) % 2 == 0
    cos = jnp.where(used, jnp.cos(angle), 0.0)
    sine = jnp.sin(angle)
    low_sin = jnp.where(used & is_low, -sine, 0.0)
    high_sin = jnp.where(used & ~is_low, sine, 0.0)

    q_part, k_part = call(
        project,
        (jax.ShapeDtypeStruct((NY * NC, 64, 128), BF), jax.ShapeDtypeStruct((NZ, 72, 128), BF)),
        1, 7, scratch=[VMEM((128, 1024), BF)],
    )(here, tokens, *shifted, gathered, key_cos, key_sin)

    stage1 = lax.all_to_all(k_part, "z", 0, 0)
    stage2 = [lax.ppermute(stage1, AXES, shift_pairs(2, j)) for j in range(1, 4)]
    held = jnp.stack([stage1] + stage2)
    stage3 = [lax.ppermute(held, AXES, shift_pairs(3, j)) for j in range(1, 4)]

    up_own = lax.all_to_all(later, SP, 0, 0)
    up_other = lax.ppermute(up_own, "c", swap)
    q_all = lax.all_to_all(q_part, TP, 0, 0)
    queries = call(
        make_queries, jax.ShapeDtypeStruct((2, 512, 256), BF), 0, 7
    )(q_all, up_own, up_other, query_gain.reshape(2, 128), cos, low_sin, high_sin)

    all_docs = up_own[:, 24:32, 64:96].astype(F32)
    key_docs = lax.dynamic_index_in_dim(
        all_docs.reshape(NS, 4, 2, 32), c, 2, keepdims=False
    ).reshape(NS, 128)
    query_docs = doc_ids.astype(F32).reshape(4, 2, 32).transpose(1, 0, 2).reshape(2, 128)
    own_first = doc_ids[0].astype(F32)
    own_last = doc_ids[255].astype(F32)
    low = jnp.sum((all_docs[:, 7, 31] < own_first).astype(jnp.int32))
    high = NS - 1 - jnp.sum((all_docs[:, 0, 0] > own_last).astype(jnp.int32))
    where = jnp.stack([z, x, y, c, low, high]).astype(jnp.int32)

    keep, send, ml = call(
        attend,
        (
            jax.ShapeDtypeStruct((128, 256), F32),
            jax.ShapeDtypeStruct((128, 256), BF),
            jax.ShapeDtypeStruct((256, 128), F32),
        ),
        1, 10, any_from=6,
        scratch=[
            VMEM((4, 4, NZ, 72, 128), BF),
            VMEM((16, 4, 256, 256), F32),
            VMEM((16, 256, 256), BF),
            VMEM((4, 256, 128), F32),
            VMEM((4, 256, 128), F32),
            VMEM((256, 256), F32),
            VMEM((256, 256), BF),
            VMEM((256, 256), BF),
            VMEM((256, 128), F32),
            VMEM((256, 128), F32),
            pltpu.SemaphoreType.DMA((4,)),
        ],
    )(where, queries, up_own, up_other, key_gain.reshape(2, 128), key_docs, query_docs, held, *stage3)

    got = lax.ppermute(send, "c", swap)
    ml_got = lax.ppermute(ml, "c", swap)
    part, log_sums = call(
        combine,
        (jax.ShapeDtypeStruct((NY, 32, 1024), BF), jax.ShapeDtypeStruct((256, 2), F32)),
        1, 6, scratch=[VMEM((4, 256, 128), F32), VMEM((4, 256, 128), F32)],
    )(here, keep, got, ml, ml_got, up_own, up_other)
    parts = lax.all_to_all(part, "y", 0, 0)
    mixed = call(finish, jax.ShapeDtypeStruct((32, 1024), BF), 0, 2)(
        parts, out_gain.reshape(1, 1024)
    )
    return mixed, log_sums


def solution(mesh):
    finer = Mesh(mesh.devices.reshape(NZ, NX, NY, NC), AXES)
    return jax.shard_map(
        layer,
        mesh=finer,
        in_specs=(
            P(AXES, None), P(SP), P(SP, None), P(SP, None), P(SP, None), P(), P(),
            P(SP, TP), P(SP, TP), P(SP, TP), P(TP, SP), P(),
        ),
        out_specs=(P(AXES, None), P(SP, TP)),
        check_vma=False,
    )
```

```python
import math

import jax
import jax.numpy as jnp
from jax import lax
from jax.experimental import pallas as pl
from jax.experimental.pallas import tpu as pltpu
from jax.sharding import Mesh
from jax.sharding import PartitionSpec as P


NOPE = 64
ROPE = 32
NZ, NX, NY, NC = 8, 4, 4, 2
NS = NZ * NX
AXES = ("z", "x", "y", "c")
SP = ("z", "x")
TP = ("y", "c")
NEG_BIG = -1e30
FLOOR = -1e20
THETA = 10000.0
EPS = 1e-06
LN2 = math.log(2.0)
SCALE2 = 1.0 / math.sqrt(NOPE + ROPE) / LN2
BF = jnp.bfloat16
F32 = jnp.float32


VMEM = pltpu.VMEM
SMEM_SPEC = pl.BlockSpec(memory_space=pltpu.SMEM)
VMEM_SPEC = pl.BlockSpec(memory_space=pltpu.VMEM)
ANY_SPEC = pl.BlockSpec(memory_space=pl.ANY)


def call(body, outs, n_smem, n_in, scratch=(), any_from=None, cost=None):
    specs = [SMEM_SPEC] * n_smem
    for i in range(n_in):
        specs.append(ANY_SPEC if any_from is not None and i >= any_from else VMEM_SPEC)
    single = not isinstance(outs, tuple)
    return pl.pallas_call(
        body,
        out_shape=outs,
        in_specs=specs,
        out_specs=VMEM_SPEC if single else tuple(VMEM_SPEC for _ in outs),
        scratch_shapes=list(scratch),
        compiler_params=pltpu.CompilerParams(vmem_limit_bytes=50 * 1024 * 1024),
        cost_estimate=cost,
    )


def lanes(shape):
    return lax.broadcasted_iota(jnp.int32, shape, len(shape) - 1)


def column(row):
    return jnp.transpose(jnp.broadcast_to(row, (128, 128)))


def pack(where, dq, dk, dr, out, flipped):
    y = where[2]

    def chosen(ref):
        block = ref[:, 0:64]
        for k in range(1, NY):
            block = jnp.where(y == k, ref[:, 64 * k : 64 * (k + 1)], block)
        return block

    block = jnp.concatenate([chosen(dq), chosen(dk)], axis=1)
    rope = dr[...].astype(F32)
    rope = jnp.concatenate([rope, jnp.zeros((32, 96), F32)], axis=1)
    flipped[...] = jnp.transpose(jnp.concatenate([rope] * 4, axis=0))
    turned = jnp.concatenate([flipped[pl.ds(4 * y, 4), :], flipped[pl.ds(16 + 4 * y, 4), :]], axis=0)
    turned = turned.astype(BF)
    for s in range(NS):
        out[s, 0:32, :] = block
        out[s, 32:40, :] = turned


def project(where, t0, t1, t2, t3, gathered, cos_ref, sin_ref, q_ref, k_ref, tok):
    y = where[2]
    for j, part in enumerate((t0, t1, t2, t3)):
        at = lax.rem(y - j + NY, NY)
        tok[pl.ds(pl.multiple_of(at * 32, 32), 32), :] = part[...]
    rows = tok[...]
    weights = gathered[:, 0:32, :].reshape(NS * 32, 128)
    both = jnp.dot(rows, weights, preferred_element_type=F32)
    turned = jnp.transpose(both).astype(BF)
    q_ref[...] = turned[0:64, :]
    for t in range(NZ):
        k_ref[t, 0:64, :] = turned[64:128, :]
    group = lanes((8, 128)) // 32
    pieces = []
    for z in range(NZ):
        piece = gathered[4 * z, 32:40, :].astype(F32)
        for g in range(1, 4):
            piece = jnp.where(group == g, gathered[4 * z + g, 32:40, :].astype(F32), piece)
        pieces.append(piece)
    rope = jnp.concatenate(pieces, axis=1)
    rope = jnp.concatenate([rope, jnp.zeros_like(rope)], axis=0).astype(BF)
    raw = lax.dot_general(rope, rows, (((1,), (1,)), ((), ())), preferred_element_type=F32)
    raw = raw[0:8, :].astype(BF).astype(F32)
    rotated = raw * cos_ref[...] + pltpu.roll(raw, 4, 0) * sin_ref[...]
    rotated = rotated.astype(BF)
    for t in range(NZ):
        k_ref[t, 64:72, :] = rotated


def make_queries(
    where, q0, q1, q2, q3, up_own, up_other, gain, cos_ref, low_ref, high_ref, out, latents
):
    y, c = where[2], where[3]
    for j, part in enumerate((q0, q1, q2, q3)):
        own, other = part[0].astype(F32), part[1].astype(F32)
        rows = pl.ds(pl.multiple_of(lax.rem(y - j + NY, NY) * 64, 64), 64)
        latents[rows, 0:128] = jnp.where(c == 0, own, other)
        latents[rows, 128:256] = jnp.where(c == 0, other, own)
    raw = latents[...]
    mean = jnp.sum(raw * raw, axis=0, keepdims=True) * (1.0 / 256.0)
    inverse = lax.rsqrt(mean + EPS)
    gains = jnp.concatenate([column(gain[0:1, :]), column(gain[1:2, :])], axis=0)
    gains = jnp.concatenate([gains, gains], axis=1)
    latent = raw * inverse * gains
    latent = jnp.transpose(latent).astype(BF)
    lane = lanes((256, 128))
    for p, up in enumerate((up_own, up_other)):
        wide = up[...].astype(F32)
        plain_w = wide[:, 0:8, :].reshape(256, 128).astype(BF)
        rope_w = wide[:, 24:32, :].reshape(256, 128).astype(BF)
        plain = jnp.dot(latent, plain_w, preferred_element_type=F32) * SCALE2
        raw = jnp.dot(latent, rope_w, preferred_element_type=F32) * SCALE2
        rope = (
            raw * cos_ref[...]
            + pltpu.roll(raw, 124, 1) * low_ref[...]
            + pltpu.roll(raw, 4, 1) * high_ref[...]
        )
        for i in range(2):
            own = slice(256 * i, 256 * (i + 1))
            out[p, own, 0:128] = jnp.where(lane // 64 == i, plain, 0.0).astype(BF)
            out[p, own, 128:256] = jnp.where(lane // 32 == i, rope, 0.0).astype(BF)


def attend(
    where, q_ref, up_own, up_other, gain, key_docs, query_docs, b0, b1, b2, b3,
    keep_ref, send_ref, ml_ref, kb, s_buf, v_buf, mx, total, acc, uk, uv, gains, docs_col, sems,
):
    x0, y0, c, low, high = where[1], where[2], where[3], where[4], where[5]
    copies = [
        pltpu.make_async_copy(part, kb.at[j], sems.at[j]) for j, part in enumerate((b0, b1, b2, b3))
    ]
    for copy in copies:
        copy.start()
    for p, up in enumerate((up_own, up_other)):
        wide = up[...].astype(F32)
        own = slice(128 * p, 128 * (p + 1))
        uk[own, :] = jnp.transpose(wide[:, 8:16, :].reshape(256, 128)).astype(BF)
        uv[own, :] = jnp.transpose(wide[:, 16:24, :].reshape(256, 128)).astype(BF)
    for i in range(2):
        gains[128 * i : 128 * (i + 1), :] = column(gain[i : i + 1, :])
        docs_col[128 * i : 128 * (i + 1), :] = column(query_docs[i : i + 1, :])
    mx[...] = jnp.full(mx.shape, NEG_BIG, F32)
    total[...] = jnp.zeros(total.shape, F32)
    acc[...] = jnp.zeros(acc.shape, F32)
    for copy in copies:
        copy.wait()
    first = low // 2
    last = high // 2 + 1

    def scores(tile, carry):
        z = tile // 2
        latents, ropes = [], []
        for half in range(2):
            x = 2 * lax.rem(tile, 2) + half
            jx = lax.rem(x0 - x + NX, NX)
            parts, turned = [], []
            for y in range(NY):
                jy = lax.rem(y0 - y + NY, NY)
                third = jnp.where(c == 0, jy, jx)
                second = jnp.where(c == 0, jx, jy)
                slab = kb[third, second, z].astype(F32)
                parts.append(slab[0:64, :])
                turned.append(slab[64:72, :])
            squares = parts[0] * parts[0]
            for part in parts[1:]:
                squares = squares + part * part
            mean = jnp.sum(squares, axis=0, keepdims=True) * (1.0 / 256.0)
            inverse = lax.rsqrt(mean + EPS)
            latent = jnp.concatenate(parts, axis=0) * inverse * gains[...]
            latents.append(latent.astype(BF))
            ropes.append(jnp.concatenate(turned, axis=0).astype(BF))
        latent = jnp.concatenate(latents, axis=1)
        rope = jnp.concatenate(ropes, axis=1)
        keys = jnp.dot(uk[...], latent, preferred_element_type=F32).astype(BF)
        values = jnp.dot(uv[...], latent, preferred_element_type=F32)
        v_buf[tile] = jnp.transpose(values).astype(BF)
        blank = jnp.zeros((64, 256), BF)
        same = []
        for half in range(2):
            docs_row = key_docs[pl.ds(2 * tile + half, 1), :]
            same.append(docs_col[...] == docs_row)
        for p in range(2):
            stack = jnp.concatenate([keys[128 * p : 128 * (p + 1), :], rope, rope, blank], axis=0)
            for i in range(2):
                own = slice(256 * i, 256 * (i + 1))
                got = jnp.dot(q_ref[p, own, :], stack, preferred_element_type=F32)
                lhs = jnp.where(same[0], got[:, 0:128], NEG_BIG)
                rhs = jnp.where(same[1], got[:, 128:256], NEG_BIG)
                s_buf[tile, 2 * p + i, :, 0:128] = lhs
                s_buf[tile, 2 * p + i, :, 128:256] = rhs
                mx[2 * p + i] = jnp.maximum(mx[2 * p + i], jnp.maximum(lhs, rhs))
        return carry

    lax.fori_loop(first, last, scores, 0)
    tops = []
    for h in range(4):
        top = jnp.max(mx[h], axis=1, keepdims=True)
        top = jnp.maximum(top, FLOOR)
        mx[h] = jnp.broadcast_to(top, (256, 128))
        tops.append(top)

    def weigh(tile, carry):
        v = v_buf[tile]
        lane = lanes((256, 256)) // 64
        result = acc[...]
        for h in range(4):
            top = mx[h]
            lhs = jnp.exp2(s_buf[tile, h, :, 0:128] - top)
            rhs = jnp.exp2(s_buf[tile, h, :, 128:256] - top)
            total[h] = total[h] + lhs + rhs
            weights = jnp.concatenate([lhs.astype(BF), rhs.astype(BF)], axis=1)
            own = jnp.where(lane == h, v, jnp.zeros_like(v))
            result = result + jnp.dot(weights, own, preferred_element_type=F32)
        acc[...] = result
        return carry

    lax.fori_loop(first, last, weigh, 0)
    lane = lanes((256, 128))
    packed = jnp.zeros((256, 128), F32)
    for h in range(4):
        packed = jnp.where(lane == h, tops[h], packed)
        packed = jnp.where(lane == 4 + h, jnp.sum(total[h], axis=1, keepdims=True), packed)
    ml_ref[...] = packed
    keep_ref[...] = acc[pl.ds(pl.multiple_of(c * 128, 128), 128), :]
    send_ref[...] = acc[pl.ds(pl.multiple_of((1 - c) * 128, 128), 128), :].astype(BF)


def combine(where, keep, got, ml_own, ml_got, w_own, w_other, part_ref, lse_ref, f_own, f_got, scratch):
    c = where[3]
    own = ml_own[...]
    other = ml_got[...]
    for h in range(4):
        k = (h + 2) % 4
        m0, l0 = own[:, h : h + 1], own[:, 4 + h : 5 + h]
        m1, l1 = other[:, k : k + 1], other[:, 4 + k : 5 + k]
        top = jnp.maximum(m0, m1)
        e0 = jnp.exp2(m0 - top)
        e1 = jnp.exp2(m1 - top)
        weight_sum = l0 * e0 + l1 * e1
        if h < 2:
            lse = (top + jnp.log2(weight_sum)) * LN2
            for half in range(2):
                for y in range(NY):
                    lse_ref[64 * y + 32 * half : 64 * y + 32 * half + 32, h : h + 1] = lse[
                        128 * half + 32 * y : 128 * half + 32 * y + 32, :
                    ]
        f_own[h] = jnp.broadcast_to(e0 / weight_sum, (256, 128))
        f_got[h] = jnp.broadcast_to(e1 / weight_sum, (256, 128))
    rows = pl.ds(pl.multiple_of(c * 128, 128), 128)
    lane = lanes((128, 128)) // 64
    result = jnp.zeros((128, 1024), F32)
    for p, w in enumerate((w_own, w_other)):
        a = jnp.where(lane == 0, f_own[2 * p, rows, :], f_own[2 * p + 1, rows, :])
        b = jnp.where(lane == 0, f_got[2 * p, rows, :], f_got[2 * p + 1, rows, :])
        mine = keep[:, 128 * p : 128 * (p + 1)]
        theirs = got[:, 128 * (1 - p) : 128 * (2 - p)].astype(F32)
        attended = (mine * a + theirs * b).astype(BF)
        result = result + lax.dot_general(
            attended, w[...].reshape(1024, 128), (((1,), (1,)), ((), ())),
            preferred_element_type=F32,
        )
    scratch[...] = result
    y = where[2]
    for j in range(NY):
        to = lax.rem(y + j, NY)
        part_ref[j] = scratch[pl.ds(pl.multiple_of(to * 32, 32), 32), :].astype(BF)


def finish(part, p1, p2, p3, gain, out):
    summed = part[0].astype(F32)
    for other in (p1, p2, p3):
        summed = summed + other[...].astype(F32)
    wide = summed.astype(BF).astype(F32)
    mean = jnp.mean(wide * wide, axis=1, keepdims=True)
    out[...] = (wide * lax.rsqrt(mean + EPS) * gain[...]).astype(BF)


def flat(z, x, y, c):
    return ((z * NX + x) * NY + y) * NC + c


def ring(j):
    return [(i, (i + j) % NY) for i in range(NY)]


def shift_pairs(stage, j):
    pairs = []
    for z in range(NZ):
        for x in range(NX):
            for y in range(NY):
                for c in range(NC):
                    along_x = (c == 0) == (stage == 2)
                    to = flat(z, (x + j) % NX, y, c) if along_x else flat(z, x, (y + j) % NY, c)
                    pairs.append((flat(z, x, y, c), to))
    return pairs


def layer(
    tokens, doc_ids, down_query, down_key, down_rotary, query_gain, key_gain,
    up_query, up_key, up_value, output_weight, out_gain,
):
    z = lax.axis_index("z")
    x = lax.axis_index("x")
    y = lax.axis_index("y")
    c = lax.axis_index("c")
    sp = z * NX + x
    here = jnp.stack([z, x, y, c]).astype(jnp.int32)
    swap = [(0, 1), (1, 0)]

    message = call(
        pack, jax.ShapeDtypeStruct((NS, 40, 128), BF), 1, 3, scratch=[VMEM((128, 128), F32)]
    )(here, down_query, down_key, down_rotary)
    gathered = lax.all_to_all(message, SP, 0, 0)

    rows = [tokens] + [lax.ppermute(tokens, "y", ring(j)) for j in range(1, NY)]

    heads = up_query.reshape(8, 2, NOPE + ROPE)
    plain = heads[:, :, :NOPE].reshape(8, 128)
    turning = heads[:, :, NOPE:].reshape(8, 2, 2, 4, 4).transpose(0, 1, 3, 2, 4).reshape(8, 64)
    docs = doc_ids.astype(BF).reshape(8, 32)
    mixed_rows = jnp.concatenate([turning, docs, jnp.zeros((8, 32), BF)], axis=1)
    later = jnp.concatenate([plain, up_key, up_value, mixed_rows], axis=0)
    later = jnp.broadcast_to(later[None], (NS, 32, 128))
    last = jnp.broadcast_to(output_weight.T[None], (NS, 32, 128))

    f32_base = (sp * 256).astype(F32)
    key_tok = lax.broadcasted_iota(jnp.int32, (8, 128), 1)
    key_row = lax.broadcasted_iota(jnp.int32, (8, 128), 0)
    key_pos = f32_base + (64 * (key_tok // 32) + 32 * c + key_tok % 32).astype(F32)
    key_freq = THETA ** (-(4 * y + key_row % 4).astype(F32) / 16)
    key_angle = key_pos * key_freq
    key_cos = jnp.cos(key_angle)
    key_sin = jnp.sin(key_angle) * jnp.where(key_row < 4, -1.0, 1.0)
    tok = lax.broadcasted_iota(jnp.int32, (256, 128), 0)
    lane = lax.broadcasted_iota(jnp.int32, (256, 128), 1)
    pos = f32_base + (64 * ((tok % 128) // 32) + 32 * (tok // 128) + tok % 32).astype(F32)
    freq = THETA ** (-(4 * ((lane % 32) // 8) + lane % 4).astype(F32) / 16)
    angle = pos * freq
    used = lane < 64
    is_low = (lane // 4) % 2 == 0
    cos = jnp.where(used, jnp.cos(angle), 0.0)
    sine = jnp.sin(angle)
    low_sin = jnp.where(used & is_low, -sine, 0.0)
    high_sin = jnp.where(used & ~is_low, sine, 0.0)

    q_part, k_part = call(
        project,
        (jax.ShapeDtypeStruct((64, 128), BF), jax.ShapeDtypeStruct((NZ, 72, 128), BF)),
        1, 7, scratch=[VMEM((128, 1024), BF)],
    )(here, *rows, gathered, key_cos, key_sin)

    stage1 = lax.all_to_all(k_part, "z", 0, 0)
    stage2 = [lax.ppermute(stage1, AXES, shift_pairs(2, j)) for j in range(1, 4)]
    held = jnp.stack([stage1] + stage2)
    stage3 = [lax.ppermute(held, AXES, shift_pairs(3, j)) for j in range(1, 4)]

    up_own = lax.all_to_all(later, SP, 0, 0)
    up_other = lax.ppermute(up_own, "c", swap)
    out_own = lax.all_to_all(last, SP, 0, 0)
    q_pair = jnp.stack([q_part, lax.ppermute(q_part, "c", swap)])
    q_all = [q_pair] + [lax.ppermute(q_pair, "y", ring(j)) for j in range(1, NY)]
    queries = call(
        make_queries, jax.ShapeDtypeStruct((2, 512, 256), BF), 1, 10,
        scratch=[VMEM((256, 256), F32)],
    )(here, *q_all, up_own, up_other, query_gain.reshape(2, 128), cos, low_sin, high_sin)

    all_docs = up_own[:, 24:32, 64:96].astype(F32)
    key_docs = lax.dynamic_index_in_dim(
        all_docs.reshape(NS, 4, 2, 32), c, 2, keepdims=False
    ).reshape(NS, 128)
    query_docs = doc_ids.astype(F32).reshape(4, 2, 32).transpose(1, 0, 2).reshape(2, 128)
    own_first = doc_ids[0].astype(F32)
    own_last = doc_ids[255].astype(F32)
    low = jnp.sum((all_docs[:, 7, 31] < own_first).astype(jnp.int32))
    high = NS - 1 - jnp.sum((all_docs[:, 0, 0] > own_last).astype(jnp.int32))
    where = jnp.stack([z, x, y, c, low, high]).astype(jnp.int32)

    keep, send, ml = call(
        attend,
        (
            jax.ShapeDtypeStruct((128, 256), F32),
            jax.ShapeDtypeStruct((128, 256), BF),
            jax.ShapeDtypeStruct((256, 128), F32),
        ),
        1, 10, any_from=6,
        scratch=[
            VMEM((4, 4, NZ, 72, 128), BF),
            VMEM((16, 4, 256, 256), F32),
            VMEM((16, 256, 256), BF),
            VMEM((4, 256, 128), F32),
            VMEM((4, 256, 128), F32),
            VMEM((256, 256), F32),
            VMEM((256, 256), BF),
            VMEM((256, 256), BF),
            VMEM((256, 128), F32),
            VMEM((256, 128), F32),
            pltpu.SemaphoreType.DMA((4,)),
        ],
    )(where, queries, up_own, up_other, key_gain.reshape(2, 128), key_docs, query_docs, held, *stage3)

    got = lax.ppermute(send, "c", swap)
    ml_got = lax.ppermute(ml, "c", swap)
    out_other = lax.ppermute(out_own, "c", swap)
    part, log_sums = call(
        combine,
        (jax.ShapeDtypeStruct((NY, 32, 1024), BF), jax.ShapeDtypeStruct((256, 2), F32)),
        1, 6, scratch=[VMEM((4, 256, 128), F32), VMEM((4, 256, 128), F32), VMEM((128, 1024), F32)],
    )(here, keep, got, ml, ml_got, out_own, out_other)
    parts = [
        lax.ppermute(part[j], "y", ring(j)) for j in range(1, NY)
    ]
    mixed = call(finish, jax.ShapeDtypeStruct((32, 1024), BF), 0, 5)(
        part, *parts, out_gain.reshape(1, 1024)
    )
    return mixed, log_sums


def solution(mesh):
    finer = Mesh(mesh.devices.reshape(NZ, NX, NY, NC), AXES)
    return jax.shard_map(
        layer,
        mesh=finer,
        in_specs=(
            P(AXES, None), P(SP), P(SP, None), P(SP, None), P(SP, None), P(), P(),
            P(SP, TP), P(SP, TP), P(SP, TP), P(TP, SP), P(),
        ),
        out_specs=(P(AXES, None), P(SP, TP)),
        check_vma=False,
    )
```

```python
import math

import jax
import jax.numpy as jnp
from jax import lax
from jax.experimental import pallas as pl
from jax.experimental.pallas import tpu as pltpu
from jax.sharding import Mesh
from jax.sharding import PartitionSpec as P


NOPE = 64
ROPE = 32
NZ, NX, NY, NC = 8, 4, 4, 2
NS = NZ * NX
AXES = ("z", "x", "y", "c")
SP = ("z", "x")
TP = ("y", "c")
NEG_BIG = -1e30
FLOOR = -1e20
THETA = 10000.0
EPS = 1e-06
LN2 = math.log(2.0)
SCALE2 = 1.0 / math.sqrt(NOPE + ROPE) / LN2
BF = jnp.bfloat16
F32 = jnp.float32


VMEM = pltpu.VMEM
SMEM_SPEC = pl.BlockSpec(memory_space=pltpu.SMEM)
VMEM_SPEC = pl.BlockSpec(memory_space=pltpu.VMEM)
ANY_SPEC = pl.BlockSpec(memory_space=pl.ANY)


def call(body, outs, n_smem, n_in, scratch=(), any_from=None, cost=None, room=16):
    specs = [SMEM_SPEC] * n_smem
    for i in range(n_in):
        specs.append(ANY_SPEC if any_from is not None and i >= any_from else VMEM_SPEC)
    single = not isinstance(outs, tuple)
    return pl.pallas_call(
        body,
        out_shape=outs,
        in_specs=specs,
        out_specs=VMEM_SPEC if single else tuple(VMEM_SPEC for _ in outs),
        scratch_shapes=list(scratch),
        compiler_params=pltpu.CompilerParams(vmem_limit_bytes=room * 1024 * 1024),
        cost_estimate=cost,
    )


def lanes(shape):
    return lax.broadcasted_iota(jnp.int32, shape, len(shape) - 1)


def column(row):
    return jnp.transpose(jnp.broadcast_to(row, (128, 128)))


def frequency(index):
    value = jnp.ones(index.shape, F32)
    for bit in range(4):
        factor = THETA ** (-(1 << bit) / 16)
        value = value * jnp.where((index // (1 << bit)) % 2 == 1, factor, 1.0)
    return value


def pack(where, dq, dk, dr, out, flipped):
    y = where[2]

    def chosen(ref):
        block = ref[:, 0:64]
        for k in range(1, NY):
            block = jnp.where(y == k, ref[:, 64 * k : 64 * (k + 1)], block)
        return block

    block = jnp.concatenate([chosen(dq), chosen(dk)], axis=1)
    rope = dr[...].astype(F32)
    rope = jnp.concatenate([rope, jnp.zeros((32, 96), F32)], axis=1)
    flipped[...] = jnp.transpose(jnp.concatenate([rope] * 4, axis=0))
    turned = jnp.concatenate([flipped[pl.ds(4 * y, 4), :], flipped[pl.ds(16 + 4 * y, 4), :]], axis=0)
    turned = turned.astype(BF)
    for s in range(NS):
        out[s, 0:32, :] = block
        out[s, 32:40, :] = turned


def project(where, t0, t1, t2, t3, gathered, q_ref, k_ref, tok):
    y = where[2]
    for j, part in enumerate((t0, t1, t2, t3)):
        at = lax.rem(y - j + NY, NY)
        tok[pl.ds(pl.multiple_of(at * 32, 32), 32), :] = part[...]
    rows = tok[...]
    weights = gathered[:, 0:32, :].reshape(NS * 32, 128)
    both = jnp.dot(rows, weights, preferred_element_type=F32)
    turned = jnp.transpose(both).astype(BF)
    q_ref[...] = turned[0:64, :]
    for t in range(NZ):
        k_ref[t, 0:64, :] = turned[64:128, :]
    group = lanes((8, 128)) // 32
    pieces = []
    for z in range(NZ):
        piece = gathered[4 * z, 32:40, :].astype(F32)
        for g in range(1, 4):
            piece = jnp.where(group == g, gathered[4 * z + g, 32:40, :].astype(F32), piece)
        pieces.append(piece)
    rope = jnp.concatenate(pieces, axis=1)
    rope = jnp.concatenate([rope, jnp.zeros_like(rope)], axis=0).astype(BF)
    raw = lax.dot_general(rope, rows, (((1,), (1,)), ((), ())), preferred_element_type=F32)
    raw = raw[0:8, :].astype(BF).astype(F32)
    at = lanes((8, 128))
    row = lax.broadcasted_iota(jnp.int32, (8, 128), 0)
    pos = where[4] + 64 * (at // 32) + 32 * where[3] + at % 32
    angle = pos.astype(F32) * frequency(4 * y + row % 4)
    sine = jnp.sin(angle)
    rotated = raw * jnp.cos(angle) + pltpu.roll(raw, 4, 0) * jnp.where(row < 4, -sine, sine)
    rotated = rotated.astype(BF)
    for t in range(NZ):
        k_ref[t, 64:72, :] = rotated


def make_queries(
    where, q0, q1, q2, q3, up_own, up_other, gain, out, latents
):
    y, c = where[2], where[3]
    for j, part in enumerate((q0, q1, q2, q3)):
        own, other = part[0].astype(F32), part[1].astype(F32)
        rows = pl.ds(pl.multiple_of(lax.rem(y - j + NY, NY) * 64, 64), 64)
        latents[rows, 0:128] = jnp.where(c == 0, own, other)
        latents[rows, 128:256] = jnp.where(c == 0, other, own)
    raw = latents[...]
    mean = jnp.sum(raw * raw, axis=0, keepdims=True) * (1.0 / 256.0)
    inverse = lax.rsqrt(mean + EPS)
    gains = jnp.concatenate([column(gain[0:1, :]), column(gain[1:2, :])], axis=0)
    gains = jnp.concatenate([gains, gains], axis=1)
    latent = raw * inverse * gains
    latent = jnp.transpose(latent).astype(BF)
    lane = lanes((256, 128))
    row = lax.broadcasted_iota(jnp.int32, (256, 128), 0)
    pos = where[4] + 64 * ((row % 128) // 32) + 32 * (row // 128) + row % 32
    angle = pos.astype(F32) * frequency(4 * ((lane % 32) // 8) + lane % 4)
    used = lane < 64
    is_low = (lane // 4) % 2 == 0
    cos = jnp.where(used, jnp.cos(angle), 0.0)
    sine = jnp.where(used, jnp.sin(angle), 0.0)
    low_sin = jnp.where(is_low, -sine, 0.0)
    high_sin = jnp.where(is_low, 0.0, sine)
    for p, up in enumerate((up_own, up_other)):
        wide = up[...].astype(F32)
        plain_w = wide[:, 0:8, :].reshape(256, 128).astype(BF)
        rope_w = wide[:, 24:32, :].reshape(256, 128).astype(BF)
        plain = jnp.dot(latent, plain_w, preferred_element_type=F32) * SCALE2
        raw = jnp.dot(latent, rope_w, preferred_element_type=F32) * SCALE2
        rope = (
            raw * cos
            + pltpu.roll(raw, 124, 1) * low_sin
            + pltpu.roll(raw, 4, 1) * high_sin
        )
        for i in range(2):
            own = slice(256 * i, 256 * (i + 1))
            out[p, own, 0:128] = jnp.where(lane // 64 == i, plain, 0.0).astype(BF)
            out[p, own, 128:256] = jnp.where(lane // 32 == i, rope, 0.0).astype(BF)


def attend(
    where, q_ref, up_own, up_other, gain, query_docs, b0, b1, b2, b3,
    keep_ref, send_ref, ml_ref, kb, s_buf, v_buf, mx, total, acc, uk, uv, gains, docs_col, key_docs, sems,
):
    x0, y0, c = where[1], where[2], where[3]
    copies = [
        pltpu.make_async_copy(part, kb.at[j], sems.at[j]) for j, part in enumerate((b0, b1, b2, b3))
    ]
    for copy in copies:
        copy.start()
    for p, up in enumerate((up_own, up_other)):
        wide = up[...].astype(F32)
        own = slice(128 * p, 128 * (p + 1))
        uk[own, :] = jnp.transpose(wide[:, 8:16, :].reshape(256, 128)).astype(BF)
        uv[own, :] = jnp.transpose(wide[:, 16:24, :].reshape(256, 128)).astype(BF)
    for i in range(2):
        gains[128 * i : 128 * (i + 1), :] = column(gain[i : i + 1, :])
        docs_col[128 * i : 128 * (i + 1), :] = column(query_docs[i : i + 1, :])
    docs = up_own[:, 24:32, :].astype(F32)
    at = lanes((NS, 8, 128))
    row = lax.broadcasted_iota(jnp.int32, (NS, 8, 128), 1)
    before = (row == 7) & (at == 95) & (docs < where[5].astype(F32))
    behind = (row == 0) & (at == 64) & (docs > where[6].astype(F32))
    low = jnp.sum(before.astype(jnp.int32))
    high = NS - 1 - jnp.sum(behind.astype(jnp.int32))
    spread = jnp.zeros((NS, 128), F32)
    at = lanes((NS, 128))
    for y in range(NY):
        piece = jnp.where(c == 0, docs[:, 2 * y, :], docs[:, 2 * y + 1, :])
        spread = jnp.where(at // 32 == y, pltpu.roll(piece, (32 * y + 64) % 128, 1), spread)
    key_docs[...] = spread
    mx[...] = jnp.full(mx.shape, NEG_BIG, F32)
    total[...] = jnp.zeros(total.shape, F32)
    acc[...] = jnp.zeros(acc.shape, F32)
    for copy in copies:
        copy.wait()
    first = low // 2
    last = high // 2 + 1

    def scores(tile, carry):
        z = tile // 2
        latents, ropes = [], []
        for half in range(2):
            x = 2 * lax.rem(tile, 2) + half
            jx = lax.rem(x0 - x + NX, NX)
            parts, turned = [], []
            for y in range(NY):
                jy = lax.rem(y0 - y + NY, NY)
                third = jnp.where(c == 0, jy, jx)
                second = jnp.where(c == 0, jx, jy)
                slab = kb[third, second, z].astype(F32)
                parts.append(slab[0:64, :])
                turned.append(slab[64:72, :])
            squares = parts[0] * parts[0]
            for part in parts[1:]:
                squares = squares + part * part
            mean = jnp.sum(squares, axis=0, keepdims=True) * (1.0 / 256.0)
            inverse = lax.rsqrt(mean + EPS)
            latent = jnp.concatenate(parts, axis=0) * inverse * gains[...]
            latents.append(latent.astype(BF))
            ropes.append(jnp.concatenate(turned, axis=0).astype(BF))
        latent = jnp.concatenate(latents, axis=1)
        rope = jnp.concatenate(ropes, axis=1)
        keys = jnp.dot(uk[...], latent, preferred_element_type=F32).astype(BF)
        values = jnp.dot(uv[...], latent, preferred_element_type=F32)
        v_buf[tile] = jnp.transpose(values).astype(BF)
        blank = jnp.zeros((64, 256), BF)
        same = []
        for half in range(2):
            docs_row = key_docs[pl.ds(2 * tile + half, 1), :]
            same.append(docs_col[...] == docs_row)
        for p in range(2):
            stack = jnp.concatenate([keys[128 * p : 128 * (p + 1), :], rope, rope, blank], axis=0)
            for i in range(2):
                own = slice(256 * i, 256 * (i + 1))
                got = jnp.dot(q_ref[p, own, :], stack, preferred_element_type=F32)
                lhs = jnp.where(same[0], got[:, 0:128], NEG_BIG)
                rhs = jnp.where(same[1], got[:, 128:256], NEG_BIG)
                s_buf[tile, 2 * p + i, :, 0:128] = lhs
                s_buf[tile, 2 * p + i, :, 128:256] = rhs
                mx[2 * p + i] = jnp.maximum(mx[2 * p + i], jnp.maximum(lhs, rhs))
        return carry

    lax.fori_loop(first, last, scores, 0)
    tops = []
    for h in range(4):
        top = jnp.max(mx[h], axis=1, keepdims=True)
        top = jnp.maximum(top, FLOOR)
        mx[h] = jnp.broadcast_to(top, (256, 128))
        tops.append(top)

    def weigh(tile, carry):
        v = v_buf[tile]
        lane = lanes((256, 256)) // 64
        result = acc[...]
        for h in range(4):
            top = mx[h]
            lhs = jnp.exp2(s_buf[tile, h, :, 0:128] - top)
            rhs = jnp.exp2(s_buf[tile, h, :, 128:256] - top)
            total[h] = total[h] + lhs + rhs
            weights = jnp.concatenate([lhs.astype(BF), rhs.astype(BF)], axis=1)
            own = jnp.where(lane == h, v, jnp.zeros_like(v))
            result = result + jnp.dot(weights, own, preferred_element_type=F32)
        acc[...] = result
        return carry

    lax.fori_loop(first, last, weigh, 0)
    lane = lanes((256, 128))
    packed = jnp.zeros((256, 128), F32)
    for h in range(4):
        packed = jnp.where(lane == h, tops[h], packed)
        packed = jnp.where(lane == 4 + h, jnp.sum(total[h], axis=1, keepdims=True), packed)
    ml_ref[...] = packed
    keep_ref[...] = acc[pl.ds(pl.multiple_of(c * 128, 128), 128), :]
    send_ref[...] = acc[pl.ds(pl.multiple_of((1 - c) * 128, 128), 128), :].astype(BF)


def combine(
    where, keep, got, ml_own, ml_got, w_own, w_other, part_ref, p1_ref, p2_ref, p3_ref, lse_ref,
    f_own, f_got, scratch,
):
    c = where[3]
    own = ml_own[...]
    other = ml_got[...]
    for h in range(4):
        k = (h + 2) % 4
        m0, l0 = own[:, h : h + 1], own[:, 4 + h : 5 + h]
        m1, l1 = other[:, k : k + 1], other[:, 4 + k : 5 + k]
        top = jnp.maximum(m0, m1)
        e0 = jnp.exp2(m0 - top)
        e1 = jnp.exp2(m1 - top)
        weight_sum = l0 * e0 + l1 * e1
        if h < 2:
            lse = (top + jnp.log2(weight_sum)) * LN2
            for half in range(2):
                for y in range(NY):
                    lse_ref[64 * y + 32 * half : 64 * y + 32 * half + 32, h : h + 1] = lse[
                        128 * half + 32 * y : 128 * half + 32 * y + 32, :
                    ]
        f_own[h] = jnp.broadcast_to(e0 / weight_sum, (256, 128))
        f_got[h] = jnp.broadcast_to(e1 / weight_sum, (256, 128))
    rows = pl.ds(pl.multiple_of(c * 128, 128), 128)
    lane = lanes((128, 128)) // 64
    result = jnp.zeros((128, 1024), F32)
    for p, w in enumerate((w_own, w_other)):
        a = jnp.where(lane == 0, f_own[2 * p, rows, :], f_own[2 * p + 1, rows, :])
        b = jnp.where(lane == 0, f_got[2 * p, rows, :], f_got[2 * p + 1, rows, :])
        mine = keep[:, 128 * p : 128 * (p + 1)]
        theirs = got[:, 128 * (1 - p) : 128 * (2 - p)].astype(F32)
        attended = (mine * a + theirs * b).astype(BF)
        result = result + lax.dot_general(
            attended, w[:, 32:64, :].reshape(1024, 128), (((1,), (1,)), ((), ())),
            preferred_element_type=F32,
        )
    scratch[...] = result
    y = where[2]
    for j, out in enumerate((part_ref, p1_ref, p2_ref, p3_ref)):
        to = lax.rem(y + j, NY)
        out[...] = scratch[pl.ds(pl.multiple_of(to * 32, 32), 32), :].astype(BF)


def finish(part, p1, p2, p3, gain, out):
    summed = part[...].astype(F32)
    for other in (p1, p2, p3):
        summed = summed + other[...].astype(F32)
    wide = summed.astype(BF).astype(F32)
    mean = jnp.mean(wide * wide, axis=1, keepdims=True)
    out[...] = (wide * lax.rsqrt(mean + EPS) * gain[...]).astype(BF)


def flat(z, x, y, c):
    return ((z * NX + x) * NY + y) * NC + c


def ring(j):
    return [(i, (i + j) % NY) for i in range(NY)]


def shift_pairs(stage, j):
    pairs = []
    for z in range(NZ):
        for x in range(NX):
            for y in range(NY):
                for c in range(NC):
                    along_x = (c == 0) == (stage == 2)
                    to = flat(z, (x + j) % NX, y, c) if along_x else flat(z, x, (y + j) % NY, c)
                    pairs.append((flat(z, x, y, c), to))
    return pairs


def layer(
    tokens, doc_ids, down_query, down_key, down_rotary, query_gain, key_gain,
    up_query, up_key, up_value, output_weight, out_gain,
):
    z = lax.axis_index("z")
    x = lax.axis_index("x")
    y = lax.axis_index("y")
    c = lax.axis_index("c")
    sp = z * NX + x
    here = jnp.stack([z, x, y, c, sp * 256]).astype(jnp.int32)
    swap = [(0, 1), (1, 0)]

    message = call(
        pack, jax.ShapeDtypeStruct((NS, 40, 128), BF), 1, 3, scratch=[VMEM((128, 128), F32)]
    )(here, down_query, down_key, down_rotary)
    gathered = lax.all_to_all(message, SP, 0, 0)

    rows = [tokens] + [lax.ppermute(tokens, "y", ring(j)) for j in range(1, NY)]

    heads = up_query.reshape(8, 2, NOPE + ROPE)
    plain = heads[:, :, :NOPE].reshape(8, 128)
    turning = heads[:, :, NOPE:].reshape(8, 2, 2, 4, 4).transpose(0, 1, 3, 2, 4).reshape(8, 64)
    docs = doc_ids.astype(BF).reshape(8, 32)
    mixed_rows = jnp.concatenate([turning, docs, jnp.zeros((8, 32), BF)], axis=1)
    later = jnp.concatenate([plain, up_key, up_value, mixed_rows, output_weight.T], axis=0)
    later = jnp.broadcast_to(later[None], (NS, 64, 128))

    q_part, k_part = call(
        project,
        (jax.ShapeDtypeStruct((64, 128), BF), jax.ShapeDtypeStruct((NZ, 72, 128), BF)),
        1, 5, scratch=[VMEM((128, 1024), BF)],
    )(here, *rows, gathered)

    stage1 = lax.all_to_all(k_part, "z", 0, 0)
    stage2 = [lax.ppermute(stage1, AXES, shift_pairs(2, j)) for j in range(1, 4)]
    held = jnp.stack([stage1] + stage2)
    stage3 = [lax.ppermute(held, AXES, shift_pairs(3, j)) for j in range(1, 4)]

    up_own = lax.all_to_all(later, SP, 0, 0)
    up_other = lax.ppermute(up_own, "c", swap)
    q_pair = jnp.stack([q_part, lax.ppermute(q_part, "c", swap)])
    q_all = [q_pair] + [lax.ppermute(q_pair, "y", ring(j)) for j in range(1, NY)]
    queries = call(
        make_queries, jax.ShapeDtypeStruct((2, 512, 256), BF), 1, 7,
        scratch=[VMEM((256, 256), F32)],
    )(here, *q_all, up_own, up_other, query_gain.reshape(2, 128))

    there = jnp.concatenate([here, doc_ids[:1], doc_ids[255:]])
    query_docs = doc_ids.astype(F32).reshape(4, 2, 32).transpose(1, 0, 2).reshape(2, 128)
    keep, send, ml = call(
        attend,
        (
            jax.ShapeDtypeStruct((128, 256), F32),
            jax.ShapeDtypeStruct((128, 256), BF),
            jax.ShapeDtypeStruct((256, 128), F32),
        ),
        1, 9, any_from=5, room=34,
        scratch=[
            VMEM((4, 4, NZ, 72, 128), BF),
            VMEM((16, 4, 256, 256), F32),
            VMEM((16, 256, 256), BF),
            VMEM((4, 256, 128), F32),
            VMEM((4, 256, 128), F32),
            VMEM((256, 256), F32),
            VMEM((256, 256), BF),
            VMEM((256, 256), BF),
            VMEM((256, 128), F32),
            VMEM((256, 128), F32),
            VMEM((NS, 128), F32),
            pltpu.SemaphoreType.DMA((4,)),
        ],
    )(there, queries, up_own, up_other, key_gain.reshape(2, 128), query_docs, held, *stage3)

    got = lax.ppermute(send, "c", swap)
    ml_got = lax.ppermute(ml, "c", swap)
    *parts, log_sums = call(
        combine,
        (jax.ShapeDtypeStruct((32, 1024), BF),) * NY + (jax.ShapeDtypeStruct((256, 2), F32),),
        1, 6, scratch=[VMEM((4, 256, 128), F32), VMEM((4, 256, 128), F32), VMEM((128, 1024), F32)],
    )(here, keep, got, ml, ml_got, up_own, up_other)
    parts[1:] = [lax.ppermute(parts[j], "y", ring(j)) for j in range(1, NY)]
    mixed = call(finish, jax.ShapeDtypeStruct((32, 1024), BF), 0, 5)(
        *parts, out_gain.reshape(1, 1024)
    )
    return mixed, log_sums


def solution(mesh):
    finer = Mesh(mesh.devices.reshape(NZ, NX, NY, NC), AXES)
    return jax.shard_map(
        layer,
        mesh=finer,
        in_specs=(
            P(AXES, None), P(SP), P(SP, None), P(SP, None), P(SP, None), P(), P(),
            P(SP, TP), P(SP, TP), P(SP, TP), P(TP, SP), P(),
        ),
        out_specs=(P(AXES, None), P(SP, TP)),
        check_vma=False,
    )
```

```python
import math

import jax
import jax.numpy as jnp
from jax import lax
from jax.experimental import pallas as pl
from jax.experimental.pallas import tpu as pltpu
from jax.sharding import Mesh
from jax.sharding import PartitionSpec as P


NOPE = 64
ROPE = 32
NZ, NX, NY, NC = 8, 4, 4, 2
NS = NZ * NX
AXES = ("z", "x", "y", "c")
SP = ("z", "x")
TP = ("y", "c")
NEG_BIG = -1e30
FLOOR = -1e20
THETA = 10000.0
EPS = 1e-06
LN2 = math.log(2.0)
SCALE2 = 1.0 / math.sqrt(NOPE + ROPE) / LN2
BF = jnp.bfloat16
F32 = jnp.float32


VMEM = pltpu.VMEM
SMEM_SPEC = pl.BlockSpec(memory_space=pltpu.SMEM)
VMEM_SPEC = pl.BlockSpec(memory_space=pltpu.VMEM)
ANY_SPEC = pl.BlockSpec(memory_space=pl.ANY)


def call(body, outs, n_smem, n_in, scratch=(), any_from=None, cost=None, room=16):
    specs = [SMEM_SPEC] * n_smem
    for i in range(n_in):
        specs.append(ANY_SPEC if any_from is not None and i >= any_from else VMEM_SPEC)
    single = not isinstance(outs, tuple)
    return pl.pallas_call(
        body,
        out_shape=outs,
        in_specs=specs,
        out_specs=VMEM_SPEC if single else tuple(VMEM_SPEC for _ in outs),
        scratch_shapes=list(scratch),
        compiler_params=pltpu.CompilerParams(vmem_limit_bytes=room * 1024 * 1024),
        cost_estimate=cost,
    )


def lanes(shape):
    return lax.broadcasted_iota(jnp.int32, shape, len(shape) - 1)


def column(row):
    return jnp.transpose(jnp.broadcast_to(row, (128, 128)))


def frequency(index):
    value = jnp.ones(index.shape, F32)
    for bit in range(4):
        factor = THETA ** (-(1 << bit) / 16)
        value = value * jnp.where((index // (1 << bit)) % 2 == 1, factor, 1.0)
    return value


def pack(where, dq, dk, dr, out, flipped):
    y = where[2]

    def chosen(ref):
        block = ref[:, 0:64]
        for k in range(1, NY):
            block = jnp.where(y == k, ref[:, 64 * k : 64 * (k + 1)], block)
        return block

    block = jnp.concatenate([chosen(dq), chosen(dk)], axis=1)
    rope = dr[...].astype(F32)
    rope = jnp.concatenate([rope, jnp.zeros((32, 96), F32)], axis=1)
    flipped[...] = jnp.transpose(jnp.concatenate([rope] * 4, axis=0))
    turned = jnp.concatenate([flipped[pl.ds(4 * y, 4), :], flipped[pl.ds(16 + 4 * y, 4), :]], axis=0)
    turned = turned.astype(BF)
    for s in range(NS):
        out[s, 0:32, :] = block
        out[s, 32:40, :] = turned


def project(where, t0, t1, t2, t3, gathered, q_ref, k_ref, tok):
    y = where[2]
    for j, part in enumerate((t0, t1, t2, t3)):
        at = lax.rem(y - j + NY, NY)
        tok[pl.ds(pl.multiple_of(at * 32, 32), 32), :] = part[...]
    rows = tok[...]
    weights = gathered[:, 0:32, :].reshape(NS * 32, 128)
    both = jnp.dot(rows, weights, preferred_element_type=F32)
    turned = jnp.transpose(both).astype(BF)
    q_ref[...] = turned[0:64, :]
    for t in range(NZ):
        k_ref[t, 0:64, :] = turned[64:128, :]
    group = lanes((8, 128)) // 32
    pieces = []
    for z in range(NZ):
        piece = gathered[4 * z, 32:40, :].astype(F32)
        for g in range(1, 4):
            piece = jnp.where(group == g, gathered[4 * z + g, 32:40, :].astype(F32), piece)
        pieces.append(piece)
    rope = jnp.concatenate(pieces, axis=1)
    rope = jnp.concatenate([rope, jnp.zeros_like(rope)], axis=0).astype(BF)
    raw = lax.dot_general(rope, rows, (((1,), (1,)), ((), ())), preferred_element_type=F32)
    raw = raw[0:8, :].astype(BF).astype(F32)
    at = lanes((8, 128))
    row = lax.broadcasted_iota(jnp.int32, (8, 128), 0)
    pos = where[4] + 64 * (at // 32) + 32 * where[3] + at % 32
    angle = pos.astype(F32) * frequency(4 * y + row % 4)
    sine = jnp.sin(angle)
    rotated = raw * jnp.cos(angle) + pltpu.roll(raw, 4, 0) * jnp.where(row < 4, -sine, sine)
    rotated = rotated.astype(BF)
    for t in range(NZ):
        k_ref[t, 64:72, :] = rotated


def make_queries(
    where, q0, q1, q2, q3, up_own, up_other, gain, out, uk_ref, uv_ref, docs_ref, latents
):
    y, c = where[2], where[3]
    for j, part in enumerate((q0, q1, q2, q3)):
        own, other = part[0].astype(F32), part[1].astype(F32)
        rows = pl.ds(pl.multiple_of(lax.rem(y - j + NY, NY) * 64, 64), 64)
        latents[rows, 0:128] = jnp.where(c == 0, own, other)
        latents[rows, 128:256] = jnp.where(c == 0, other, own)
    raw = latents[...]
    mean = jnp.sum(raw * raw, axis=0, keepdims=True) * (1.0 / 256.0)
    inverse = lax.rsqrt(mean + EPS)
    gains = jnp.concatenate([column(gain[0:1, :]), column(gain[1:2, :])], axis=0)
    gains = jnp.concatenate([gains, gains], axis=1)
    latent = (raw * inverse * gains).astype(BF)
    tok = lanes((64, 256))
    row = lax.broadcasted_iota(jnp.int32, (64, 256), 0)
    pos = where[4] + 64 * ((tok % 128) // 32) + 32 * (tok // 128) + tok % 32
    angle = pos.astype(F32) * frequency(4 * ((row % 32) // 8) + row % 4)
    is_low = (row // 4) % 2 == 0
    cos = jnp.cos(angle)
    sine = jnp.sin(angle)
    low_sin = jnp.where(is_low, -sine, 0.0)
    high_sin = jnp.where(is_low, 0.0, sine)
    for p, up in enumerate((up_own, up_other)):
        wide = up[:, 0:32, :].astype(F32)
        own = slice(128 * p, 128 * (p + 1))
        plain_w = jnp.transpose(wide[:, 0:8, :].reshape(256, 128)).astype(BF)
        rope_w = jnp.transpose(wide[:, 24:32, :].reshape(256, 128))[0:64, :].astype(BF)
        uk_ref[:, own] = wide[:, 8:16, :].reshape(256, 128).astype(BF)
        uv_ref[own, :] = jnp.transpose(wide[:, 16:24, :].reshape(256, 128)).astype(BF)
        plain = (jnp.dot(plain_w, latent, preferred_element_type=F32) * SCALE2).astype(BF)
        raw = jnp.dot(rope_w, latent, preferred_element_type=F32) * SCALE2
        rope = raw * cos + pltpu.roll(raw, 60, 0) * low_sin + pltpu.roll(raw, 4, 0) * high_sin
        rope = rope.astype(BF)
        for i in range(2):
            h = 2 * p + i
            out[h] = jnp.zeros((256, 256), BF)
            out[h, 64 * i : 64 * (i + 1), :] = plain[64 * i : 64 * (i + 1), :]
            out[h, 128:160, :] = rope[32 * i : 32 * (i + 1), :]
    docs = up_own[:, 24:32, :].astype(F32)
    at = lanes((NS, 128))
    spread = jnp.zeros((NS, 128), F32)
    for k in range(NY):
        piece = jnp.where(c == 0, docs[:, 2 * k, :], docs[:, 2 * k + 1, :])
        spread = jnp.where(at // 32 == k, pltpu.roll(piece, (32 * k + 64) % 128, 1), spread)
    docs_ref[...] = spread


def attend(
    where, q_ref, uk, uv, key_docs, gain, query_docs, b0, b1, b2, b3,
    keep_ref, send_ref, ml_ref, kb, s_buf, v_buf, mx, total, acc, gains,
):
    x0, y0, c = where[1], where[2], where[3]
    docs = key_docs[...]
    at = lanes((NS, 128))
    before = (at == 127) & (docs < where[5].astype(F32))
    behind = (at == 0) & (docs > where[6].astype(F32))
    low = jnp.sum(before.astype(jnp.int32))
    high = NS - 1 - jnp.sum(behind.astype(jnp.int32))
    first = low // 2
    last = jnp.maximum(high // 2, first) + 1

    def fetch(z, carry):
        for j, part in enumerate((b0, b1, b2, b3)):
            for k in range(4):
                kb[j, k, z] = part[k, z]
        return carry

    lax.fori_loop(first // 2, (last + 1) // 2, fetch, 0)
    for i in range(2):
        gains[128 * i : 128 * (i + 1), :] = column(gain[i : i + 1, :])
    mx[...] = jnp.full(mx.shape, NEG_BIG, F32)
    total[...] = jnp.zeros(total.shape, F32)
    acc[...] = jnp.zeros(acc.shape, F32)
    wanted = jnp.concatenate([query_docs[0:1, :], query_docs[1:2, :]], axis=1)

    def scores(tile, carry):
        z = tile // 2
        latents, ropes, same = [], [], []
        for half in range(2):
            x = 2 * lax.rem(tile, 2) + half
            jx = lax.rem(x0 - x + NX, NX)
            parts, turned = [], []
            for y in range(NY):
                jy = lax.rem(y0 - y + NY, NY)
                third = jnp.where(c == 0, jy, jx)
                second = jnp.where(c == 0, jx, jy)
                slab = kb[third, second, z].astype(F32)
                parts.append(slab[0:64, :])
                turned.append(slab[64:72, :])
            squares = parts[0] * parts[0]
            for part in parts[1:]:
                squares = squares + part * part
            mean = jnp.sum(squares, axis=0, keepdims=True) * (1.0 / 256.0)
            inverse = lax.rsqrt(mean + EPS)
            latents.append(jnp.concatenate(parts, axis=0) * inverse * gains[...])
            ropes.append(jnp.concatenate(turned, axis=0))
            docs_col = column(key_docs[pl.ds(2 * tile + half, 1), :])
            same.append(jnp.concatenate([docs_col, docs_col], axis=1) == wanted)
        latent = jnp.concatenate(latents, axis=1)
        v_buf[tile] = jnp.dot(uv[...], latent.astype(BF), preferred_element_type=F32).astype(BF)
        turned = jnp.transpose(latent).astype(BF)
        rope = jnp.concatenate(ropes, axis=1)
        rope = jnp.concatenate([rope, jnp.zeros((96, 256), F32)], axis=0)
        rope = jnp.transpose(rope).astype(BF)
        keys = jnp.dot(turned, uk[...], preferred_element_type=F32).astype(BF)
        for h in range(4):
            p = h // 2
            stack = jnp.concatenate([keys[:, 128 * p : 128 * (p + 1)], rope], axis=1)
            got = jnp.dot(stack, q_ref[h], preferred_element_type=F32)
            got = jnp.concatenate(
                [
                    jnp.where(same[0], got[0:128, :], NEG_BIG),
                    jnp.where(same[1], got[128:256, :], NEG_BIG),
                ],
                axis=0,
            )
            s_buf[tile, h] = got
            mx[h] = jnp.maximum(mx[h], jnp.max(got.reshape(32, 8, 256), axis=0))
        return carry

    lax.fori_loop(first, last, scores, 0)
    tops = []
    for h in range(4):
        top = jnp.maximum(jnp.max(mx[h], axis=0, keepdims=True), FLOOR)
        mx[h] = jnp.broadcast_to(top, (8, 256))
        tops.append(top)

    def weigh(tile, carry):
        for h in range(4):
            own = slice(64 * h, 64 * (h + 1))
            weights = jnp.exp2(s_buf[tile, h].reshape(32, 8, 256) - mx[h][None])
            total[h] = total[h] + jnp.sum(weights, axis=0)
            weights = weights.reshape(256, 256).astype(BF)
            acc[own, :] = acc[own, :] + jnp.dot(
                v_buf[tile, own, :], weights, preferred_element_type=F32
            )
        return carry

    lax.fori_loop(first, last, weigh, 0)
    for h in range(4):
        ml_ref[h : h + 1, :] = tops[h]
        ml_ref[4 + h : 5 + h, :] = jnp.sum(total[h], axis=0, keepdims=True)
    left, right = acc[:, 0:128], acc[:, 128:256]
    keep_ref[...] = jnp.where(c == 0, left, right)
    send_ref[...] = jnp.where(c == 0, right, left).astype(BF)


def combine(
    where, keep, got, ml_own, ml_got, w_own, w_other, part_ref, p1_ref, p2_ref, p3_ref, lse_ref,
    scratch,
):
    c = where[3]
    m0, l0 = ml_own[0:4, :], ml_own[4:8, :]
    m1 = jnp.concatenate([ml_got[2:4, :], ml_got[0:2, :]], axis=0)
    l1 = jnp.concatenate([ml_got[6:8, :], ml_got[4:6, :]], axis=0)
    top = jnp.maximum(m0, m1)
    e0 = jnp.exp2(m0 - top)
    e1 = jnp.exp2(m1 - top)
    weight_sum = l0 * e0 + l1 * e1
    lse_ref[...] = ((top + jnp.log2(weight_sum)) * LN2)[0:2, :]
    f0 = e0 / weight_sum
    f1 = e1 / weight_sum
    f0 = jnp.where(c == 0, f0[:, 0:128], f0[:, 128:256])
    f1 = jnp.where(c == 0, f1[:, 0:128], f1[:, 128:256])
    result = jnp.zeros((128, 1024), F32)
    for p, w in enumerate((w_own, w_other)):
        pieces = []
        for i in range(2):
            h, k = 2 * p + i, (2 * p + i + 2) % 4
            mine = keep[64 * h : 64 * (h + 1), :]
            theirs = got[64 * k : 64 * (k + 1), :].astype(F32)
            pieces.append(mine * f0[h : h + 1, :] + theirs * f1[h : h + 1, :])
        attended = jnp.transpose(jnp.concatenate(pieces, axis=0)).astype(BF)
        result = result + lax.dot_general(
            attended, w[:, 32:64, :].reshape(1024, 128), (((1,), (1,)), ((), ())),
            preferred_element_type=F32,
        )
    scratch[...] = result
    y = where[2]
    for j, out in enumerate((part_ref, p1_ref, p2_ref, p3_ref)):
        to = lax.rem(y + j, NY)
        out[...] = scratch[pl.ds(pl.multiple_of(to * 32, 32), 32), :].astype(BF)


def finish(part, p1, p2, p3, gain, out):
    summed = part[...].astype(F32)
    for other in (p1, p2, p3):
        summed = summed + other[...].astype(F32)
    wide = summed.astype(BF).astype(F32)
    mean = jnp.mean(wide * wide, axis=1, keepdims=True)
    out[...] = (wide * lax.rsqrt(mean + EPS) * gain[...]).astype(BF)


def flat(z, x, y, c):
    return ((z * NX + x) * NY + y) * NC + c


def ring(j):
    return [(i, (i + j) % NY) for i in range(NY)]


def shift_pairs(stage, j):
    pairs = []
    for z in range(NZ):
        for x in range(NX):
            for y in range(NY):
                for c in range(NC):
                    along_x = (c == 0) == (stage == 2)
                    to = flat(z, (x + j) % NX, y, c) if along_x else flat(z, x, (y + j) % NY, c)
                    pairs.append((flat(z, x, y, c), to))
    return pairs


def layer(
    tokens, doc_ids, down_query, down_key, down_rotary, query_gain, key_gain,
    up_query, up_key, up_value, output_weight, out_gain,
):
    z = lax.axis_index("z")
    x = lax.axis_index("x")
    y = lax.axis_index("y")
    c = lax.axis_index("c")
    sp = z * NX + x
    here = jnp.stack([z, x, y, c, sp * 256]).astype(jnp.int32)
    swap = [(0, 1), (1, 0)]

    message = call(
        pack, jax.ShapeDtypeStruct((NS, 40, 128), BF), 1, 3, scratch=[VMEM((128, 128), F32)]
    )(here, down_query, down_key, down_rotary)
    gathered = lax.all_to_all(message, SP, 0, 0)

    rows = [tokens] + [lax.ppermute(tokens, "y", ring(j)) for j in range(1, NY)]

    heads = up_query.reshape(8, 2, NOPE + ROPE)
    plain = heads[:, :, :NOPE].reshape(8, 128)
    turning = heads[:, :, NOPE:].reshape(8, 2, 2, 4, 4).transpose(0, 1, 3, 2, 4).reshape(8, 64)
    docs = doc_ids.astype(BF).reshape(8, 32)
    mixed_rows = jnp.concatenate([turning, docs, jnp.zeros((8, 32), BF)], axis=1)
    later = jnp.concatenate([plain, up_key, up_value, mixed_rows, output_weight.T], axis=0)
    later = jnp.broadcast_to(later[None], (NS, 64, 128))

    q_part, k_part = call(
        project,
        (jax.ShapeDtypeStruct((64, 128), BF), jax.ShapeDtypeStruct((NZ, 72, 128), BF)),
        1, 5, scratch=[VMEM((128, 1024), BF)],
    )(here, *rows, gathered)

    stage1 = lax.all_to_all(k_part, "z", 0, 0)
    stage2 = [lax.ppermute(stage1, AXES, shift_pairs(2, j)) for j in range(1, 4)]
    held = jnp.stack([stage1] + stage2)
    stage3 = [lax.ppermute(held, AXES, shift_pairs(3, j)) for j in range(1, 4)]

    up_own = lax.all_to_all(later, SP, 0, 0)
    up_other = lax.ppermute(up_own, "c", swap)
    q_pair = jnp.stack([q_part, lax.ppermute(q_part, "c", swap)])
    q_all = [q_pair] + [lax.ppermute(q_pair, "y", ring(j)) for j in range(1, NY)]
    queries, uk, uv, key_docs = call(
        make_queries,
        (
            jax.ShapeDtypeStruct((4, 256, 256), BF),
            jax.ShapeDtypeStruct((256, 256), BF),
            jax.ShapeDtypeStruct((256, 256), BF),
            jax.ShapeDtypeStruct((NS, 128), F32),
        ),
        1, 7, scratch=[VMEM((256, 256), F32)],
    )(here, *q_all, up_own, up_other, query_gain.reshape(2, 128))

    there = jnp.concatenate([here, doc_ids[:1], doc_ids[255:]])
    query_docs = doc_ids.astype(F32).reshape(4, 2, 32).transpose(1, 0, 2).reshape(2, 128)
    keep, send, ml = call(
        attend,
        (
            jax.ShapeDtypeStruct((256, 128), F32),
            jax.ShapeDtypeStruct((256, 128), BF),
            jax.ShapeDtypeStruct((8, 256), F32),
        ),
        1, 10, room=34,
        scratch=[
            VMEM((4, 4, NZ, 72, 128), BF),
            VMEM((16, 4, 256, 256), F32),
            VMEM((16, 256, 256), BF),
            VMEM((4, 8, 256), F32),
            VMEM((4, 8, 256), F32),
            VMEM((256, 256), F32),
            VMEM((256, 128), F32),
        ],
    )(there, queries, uk, uv, key_docs, key_gain.reshape(2, 128), query_docs, held, *stage3)

    got = lax.ppermute(send, "c", swap)
    ml_got = lax.ppermute(ml, "c", swap)
    *parts, log_sums = call(
        combine,
        (jax.ShapeDtypeStruct((32, 1024), BF),) * NY + (jax.ShapeDtypeStruct((2, 256), F32),),
        1, 6, scratch=[VMEM((128, 1024), F32)],
    )(here, keep, got, ml, ml_got, up_own, up_other)
    parts[1:] = [lax.ppermute(parts[j], "y", ring(j)) for j in range(1, NY)]
    mixed = call(finish, jax.ShapeDtypeStruct((32, 1024), BF), 0, 5)(
        *parts, out_gain.reshape(1, 1024)
    )
    log_sums = log_sums.reshape(2, 2, 4, 32).transpose(2, 1, 3, 0).reshape(256, 2)
    return mixed, log_sums


def solution(mesh):
    finer = Mesh(mesh.devices.reshape(NZ, NX, NY, NC), AXES)
    return jax.shard_map(
        layer,
        mesh=finer,
        in_specs=(
            P(AXES, None), P(SP), P(SP, None), P(SP, None), P(SP, None), P(), P(),
            P(SP, TP), P(SP, TP), P(SP, TP), P(TP, SP), P(),
        ),
        out_specs=(P(AXES, None), P(SP, TP)),
        check_vma=False,
    )
```

```python
import math

import jax
import jax.numpy as jnp
from jax import lax
from jax.experimental import pallas as pl
from jax.experimental.pallas import tpu as pltpu
from jax.sharding import Mesh
from jax.sharding import PartitionSpec as P


NOPE = 64
ROPE = 32
NZ, NX, NY, NC = 8, 4, 4, 2
NS = NZ * NX
AXES = ("z", "x", "y", "c")
SP = ("z", "x")
TP = ("y", "c")
NEG_BIG = -1e30
FLOOR = -1e20
THETA = 10000.0
EPS = 1e-06
LN2 = math.log(2.0)
SCALE2 = 1.0 / math.sqrt(NOPE + ROPE) / LN2
BF = jnp.bfloat16
F32 = jnp.float32


VMEM = pltpu.VMEM
SMEM_SPEC = pl.BlockSpec(memory_space=pltpu.SMEM)
VMEM_SPEC = pl.BlockSpec(memory_space=pltpu.VMEM)
ANY_SPEC = pl.BlockSpec(memory_space=pl.ANY)


def call(body, outs, n_smem, n_in, scratch=(), any_from=None, cost=None, room=16):
    specs = [SMEM_SPEC] * n_smem
    for i in range(n_in):
        specs.append(ANY_SPEC if any_from is not None and i >= any_from else VMEM_SPEC)
    single = not isinstance(outs, tuple)
    return pl.pallas_call(
        body,
        out_shape=outs,
        in_specs=specs,
        out_specs=VMEM_SPEC if single else tuple(VMEM_SPEC for _ in outs),
        scratch_shapes=list(scratch),
        compiler_params=pltpu.CompilerParams(vmem_limit_bytes=room * 1024 * 1024),
        cost_estimate=cost,
    )


def lanes(shape):
    return lax.broadcasted_iota(jnp.int32, shape, len(shape) - 1)


def column(row):
    return jnp.transpose(jnp.broadcast_to(row, (128, 128)))


def frequency(index):
    value = jnp.ones(index.shape, F32)
    for bit in range(4):
        factor = THETA ** (-(1 << bit) / 16)
        value = value * jnp.where((index // (1 << bit)) % 2 == 1, factor, 1.0)
    return value


def pack(where, dq, dk, dr, out, flipped):
    y = where[2]

    def chosen(ref):
        block = ref[:, 0:64]
        for k in range(1, NY):
            block = jnp.where(y == k, ref[:, 64 * k : 64 * (k + 1)], block)
        return block

    block = jnp.concatenate([chosen(dq), chosen(dk)], axis=1)
    rope = dr[...].astype(F32)
    rope = jnp.concatenate([rope, jnp.zeros((32, 96), F32)], axis=1)
    flipped[...] = jnp.transpose(jnp.concatenate([rope] * 4, axis=0))
    turned = jnp.concatenate([flipped[pl.ds(4 * y, 4), :], flipped[pl.ds(16 + 4 * y, 4), :]], axis=0)
    turned = turned.astype(BF)
    for z in range(NZ):
        out[z, 0:32, :] = block
        out[z, 32:40, :] = turned


def pack_later(up_query, up_key, up_value, docs_ref, out_t, out):
    src = lax.broadcasted_iota(jnp.int32, (192, 256), 0)
    lane = lanes((192, 256))
    plain = 96 * (lane // 64) + lane % 64
    turn = lane - 128
    rope = 64 + 96 * (turn // 32) + 16 * ((turn // 4) % 2) + 4 * ((turn % 32) // 8) + turn % 4
    chosen = jnp.where(lane < 128, plain, jnp.where(lane < 192, rope, -1))
    pick = jnp.where(src == chosen, 1.0, 0.0).astype(BF)
    sorted_query = jnp.dot(up_query[...], pick, preferred_element_type=F32)
    out[0:8, :] = sorted_query[:, 0:128].astype(BF)
    out[8:16, :] = up_key[...]
    out[16:24, :] = up_value[...]
    mixed = sorted_query[:, 128:256]
    docs = docs_ref[...].astype(F32)
    row = lax.broadcasted_iota(jnp.int32, (8, 128), 0)
    at = lanes((8, 128))
    for r in range(8):
        line = docs[r // 4 : r // 4 + 1, :]
        moved = pltpu.roll(jnp.broadcast_to(line, (8, 128)), (64 - 32 * (r % 4)) % 128, 1)
        mixed = jnp.where((row == r) & (at // 32 == 2), moved, mixed)
    out[24:32, :] = mixed.astype(BF)
    out[32:64, :] = out_t[...]


def project(where, t0, t1, t2, t3, g0, g1, g2, g3, q_ref, k_ref, tok, gathered):
    x = where[1]
    y = where[2]
    for j, part in enumerate((t0, t1, t2, t3)):
        at = lax.rem(y - j + NY, NY)
        tok[pl.ds(pl.multiple_of(at * 32, 32), 32), :] = part[...]
    for j, part in enumerate((g0, g1, g2, g3)):
        gathered[lax.rem(x - j + NX, NX)] = part[...]
    rows = tok[...]
    weights = jnp.concatenate(
        [gathered[k, z, 0:32, :] for z in range(NZ) for k in range(NX)], axis=0
    )
    both = jnp.dot(rows, weights, preferred_element_type=F32)
    turned = jnp.transpose(both).astype(BF)
    q_ref[...] = turned[0:64, :]
    for t in range(NZ):
        k_ref[t, 0:64, :] = turned[64:128, :]
    group = lanes((8, 128)) // 32
    pieces = []
    for z in range(NZ):
        piece = gathered[0, z, 32:40, :].astype(F32)
        for g in range(1, 4):
            piece = jnp.where(group == g, gathered[g, z, 32:40, :].astype(F32), piece)
        pieces.append(piece)
    rope = jnp.concatenate(pieces, axis=1)
    rope = jnp.concatenate([rope, jnp.zeros_like(rope)], axis=0).astype(BF)
    raw = lax.dot_general(rope, rows, (((1,), (1,)), ((), ())), preferred_element_type=F32)
    raw = raw[0:8, :].astype(BF).astype(F32)
    at = lanes((8, 128))
    row = lax.broadcasted_iota(jnp.int32, (8, 128), 0)
    pos = where[4] + 64 * (at // 32) + 32 * where[3] + at % 32
    angle = pos.astype(F32) * frequency(4 * y + row % 4)
    sine = jnp.sin(angle)
    rotated = raw * jnp.cos(angle) + pltpu.roll(raw, 4, 0) * jnp.where(row < 4, -sine, sine)
    rotated = rotated.astype(BF)
    for t in range(NZ):
        k_ref[t, 64:72, :] = rotated


def make_queries(
    where, q0, q1, q2, q3, up_own, up_other, gain, out, uk_ref, uv_ref, docs_ref, latents, ups
):
    x, y, c = where[1], where[2], where[3]
    for j, part in enumerate((q0, q1, q2, q3)):
        own, other = part[0].astype(F32), part[1].astype(F32)
        rows = pl.ds(pl.multiple_of(lax.rem(y - j + NY, NY) * 64, 64), 64)
        latents[rows, 0:128] = jnp.where(c == 0, own, other)
        latents[rows, 128:256] = jnp.where(c == 0, other, own)
    raw = latents[...]
    mean = jnp.sum(raw * raw, axis=0, keepdims=True) * (1.0 / 256.0)
    inverse = lax.rsqrt(mean + EPS)
    gains = jnp.concatenate([column(gain[0:1, :]), column(gain[1:2, :])], axis=0)
    gains = jnp.concatenate([gains, gains], axis=1)
    latent = (raw * inverse * gains).astype(BF)
    tok = lanes((64, 256))
    row = lax.broadcasted_iota(jnp.int32, (64, 256), 0)
    pos = where[4] + 64 * ((tok % 128) // 32) + 32 * (tok // 128) + tok % 32
    angle = pos.astype(F32) * frequency(4 * ((row % 32) // 8) + row % 4)
    is_low = (row // 4) % 2 == 0
    cos = jnp.cos(angle)
    sine = jnp.sin(angle)
    low_sin = jnp.where(is_low, -sine, 0.0)
    high_sin = jnp.where(is_low, 0.0, sine)
    for p, up in enumerate((up_own, up_other)):
        for j in range(NX):
            ups[p, :, lax.rem(x - j + NX, NX)] = up[:, j, 0:32, :]
        wide = ups[p].reshape(NS, 32, 128).astype(F32)
        own = slice(128 * p, 128 * (p + 1))
        plain_w = jnp.transpose(wide[:, 0:8, :].reshape(256, 128)).astype(BF)
        rope_w = jnp.transpose(wide[:, 24:32, :].reshape(256, 128))[0:64, :].astype(BF)
        uk_ref[:, own] = wide[:, 8:16, :].reshape(256, 128).astype(BF)
        uv_ref[own, :] = jnp.transpose(wide[:, 16:24, :].reshape(256, 128)).astype(BF)
        plain = (jnp.dot(plain_w, latent, preferred_element_type=F32) * SCALE2).astype(BF)
        raw = jnp.dot(rope_w, latent, preferred_element_type=F32) * SCALE2
        rope = raw * cos + pltpu.roll(raw, 60, 0) * low_sin + pltpu.roll(raw, 4, 0) * high_sin
        rope = rope.astype(BF)
        for i in range(2):
            h = 2 * p + i
            out[h] = jnp.zeros((256, 256), BF)
            out[h, 64 * i : 64 * (i + 1), :] = plain[64 * i : 64 * (i + 1), :]
            out[h, 128:160, :] = rope[32 * i : 32 * (i + 1), :]
    docs = ups[0].reshape(NS, 32, 128)[:, 24:32, :].astype(F32)
    at = lanes((NS, 128))
    spread = jnp.zeros((NS, 128), F32)
    for k in range(NY):
        piece = jnp.where(c == 0, docs[:, 2 * k, :], docs[:, 2 * k + 1, :])
        spread = jnp.where(at // 32 == k, pltpu.roll(piece, (32 * k + 64) % 128, 1), spread)
    docs_ref[...] = spread


def attend(
    where, ids, q_ref, uk, uv, key_docs, gain, query_docs, b0, b1, b2, b3,
    keep_ref, send_ref, ml_ref, kb, s_buf, v_buf, mx, total, acc, gains,
):
    x0, y0, c = where[1], where[2], where[3]
    docs = key_docs[...]
    at = lanes((NS, 128))
    before = (at == 127) & (docs < ids[0].astype(F32))
    behind = (at == 0) & (docs > ids[255].astype(F32))
    low = jnp.sum(before.astype(jnp.int32))
    high = NS - 1 - jnp.sum(behind.astype(jnp.int32))
    first = low // 2
    last = jnp.maximum(high // 2, first) + 1

    def fetch(z, carry):
        for j, part in enumerate((b0, b1, b2, b3)):
            for k in range(4):
                kb[j, k, z] = part[k, z]
        return carry

    lax.fori_loop(first // 2, (last + 1) // 2, fetch, 0)
    for i in range(2):
        gains[128 * i : 128 * (i + 1), :] = column(gain[i : i + 1, :])
    mx[...] = jnp.full(mx.shape, NEG_BIG, F32)
    total[...] = jnp.zeros(total.shape, F32)
    acc[...] = jnp.zeros(acc.shape, F32)
    wanted = jnp.concatenate([query_docs[0:1, :], query_docs[1:2, :]], axis=1)

    def scores(tile, carry):
        z = tile // 2
        latents, ropes, same = [], [], []
        for half in range(2):
            x = 2 * lax.rem(tile, 2) + half
            jx = lax.rem(x0 - x + NX, NX)
            parts, turned = [], []
            for y in range(NY):
                jy = lax.rem(y0 - y + NY, NY)
                third = jnp.where(c == 0, jy, jx)
                second = jnp.where(c == 0, jx, jy)
                slab = kb[third, second, z].astype(F32)
                parts.append(slab[0:64, :])
                turned.append(slab[64:72, :])
            squares = parts[0] * parts[0]
            for part in parts[1:]:
                squares = squares + part * part
            mean = jnp.sum(squares, axis=0, keepdims=True) * (1.0 / 256.0)
            inverse = lax.rsqrt(mean + EPS)
            latents.append(jnp.concatenate(parts, axis=0) * inverse * gains[...])
            ropes.append(jnp.concatenate(turned, axis=0))
            docs_col = column(key_docs[pl.ds(2 * tile + half, 1), :])
            same.append(jnp.concatenate([docs_col, docs_col], axis=1) == wanted)
        latent = jnp.concatenate(latents, axis=1)
        v_buf[tile] = jnp.dot(uv[...], latent.astype(BF), preferred_element_type=F32).astype(BF)
        turned = jnp.transpose(latent).astype(BF)
        rope = jnp.concatenate(ropes, axis=1)
        rope = jnp.concatenate([rope, jnp.zeros((96, 256), F32)], axis=0)
        rope = jnp.transpose(rope).astype(BF)
        keys = jnp.dot(turned, uk[...], preferred_element_type=F32).astype(BF)
        for h in range(4):
            p = h // 2
            stack = jnp.concatenate([keys[:, 128 * p : 128 * (p + 1)], rope], axis=1)
            got = jnp.dot(stack, q_ref[h], preferred_element_type=F32)
            got = jnp.concatenate(
                [
                    jnp.where(same[0], got[0:128, :], NEG_BIG),
                    jnp.where(same[1], got[128:256, :], NEG_BIG),
                ],
                axis=0,
            )
            s_buf[tile, h] = got
            mx[h] = jnp.maximum(mx[h], jnp.max(got.reshape(32, 8, 256), axis=0))
        return carry

    lax.fori_loop(first, last, scores, 0)
    tops = []
    for h in range(4):
        top = jnp.maximum(jnp.max(mx[h], axis=0, keepdims=True), FLOOR)
        mx[h] = jnp.broadcast_to(top, (8, 256))
        tops.append(top)

    def weigh(tile, carry):
        for h in range(4):
            own = slice(64 * h, 64 * (h + 1))
            weights = jnp.exp2(s_buf[tile, h].reshape(32, 8, 256) - mx[h][None])
            total[h] = total[h] + jnp.sum(weights, axis=0)
            weights = weights.reshape(256, 256).astype(BF)
            acc[own, :] = acc[own, :] + jnp.dot(
                v_buf[tile, own, :], weights, preferred_element_type=F32
            )
        return carry

    lax.fori_loop(first, last, weigh, 0)
    for h in range(4):
        ml_ref[h : h + 1, :] = tops[h]
        ml_ref[4 + h : 5 + h, :] = jnp.sum(total[h], axis=0, keepdims=True)
    left, right = acc[:, 0:128], acc[:, 128:256]
    keep_ref[...] = jnp.where(c == 0, left, right)
    send_ref[...] = jnp.where(c == 0, right, left).astype(BF)


def combine(
    where, keep, got, ml_own, ml_got, w_own, w_other, part_ref, p1_ref, p2_ref, p3_ref, lse_ref,
    scratch, outs,
):
    x, c = where[1], where[3]
    m0, l0 = ml_own[0:4, :], ml_own[4:8, :]
    m1 = jnp.concatenate([ml_got[2:4, :], ml_got[0:2, :]], axis=0)
    l1 = jnp.concatenate([ml_got[6:8, :], ml_got[4:6, :]], axis=0)
    top = jnp.maximum(m0, m1)
    e0 = jnp.exp2(m0 - top)
    e1 = jnp.exp2(m1 - top)
    weight_sum = l0 * e0 + l1 * e1
    lse_ref[...] = ((top + jnp.log2(weight_sum)) * LN2)[0:2, :]
    f0 = e0 / weight_sum
    f1 = e1 / weight_sum
    f0 = jnp.where(c == 0, f0[:, 0:128], f0[:, 128:256])
    f1 = jnp.where(c == 0, f1[:, 0:128], f1[:, 128:256])
    result = jnp.zeros((128, 1024), F32)
    for p, w in enumerate((w_own, w_other)):
        pieces = []
        for i in range(2):
            h, k = 2 * p + i, (2 * p + i + 2) % 4
            mine = keep[64 * h : 64 * (h + 1), :]
            theirs = got[64 * k : 64 * (k + 1), :].astype(F32)
            pieces.append(mine * f0[h : h + 1, :] + theirs * f1[h : h + 1, :])
        attended = jnp.transpose(jnp.concatenate(pieces, axis=0)).astype(BF)
        for j in range(NX):
            outs[p, :, lax.rem(x - j + NX, NX)] = w[:, j, 32:64, :]
        result = result + lax.dot_general(
            attended, outs[p].reshape(1024, 128), (((1,), (1,)), ((), ())),
            preferred_element_type=F32,
        )
    scratch[...] = result
    y = where[2]
    for j, out in enumerate((part_ref, p1_ref, p2_ref, p3_ref)):
        to = lax.rem(y + j, NY)
        out[...] = scratch[pl.ds(pl.multiple_of(to * 32, 32), 32), :].astype(BF)


def finish(part, p1, p2, p3, gain, out):
    summed = part[...].astype(F32)
    for other in (p1, p2, p3):
        summed = summed + other[...].astype(F32)
    wide = summed.astype(BF).astype(F32)
    mean = jnp.mean(wide * wide, axis=1, keepdims=True)
    out[...] = (wide * lax.rsqrt(mean + EPS) * gain[...]).astype(BF)


def flat(z, x, y, c):
    return ((z * NX + x) * NY + y) * NC + c


def ring(j):
    return [(i, (i + j) % NY) for i in range(NY)]


def shift_pairs(stage, j):
    pairs = []
    for z in range(NZ):
        for x in range(NX):
            for y in range(NY):
                for c in range(NC):
                    along_x = (c == 0) == (stage == 2)
                    to = flat(z, (x + j) % NX, y, c) if along_x else flat(z, x, (y + j) % NY, c)
                    pairs.append((flat(z, x, y, c), to))
    return pairs


def layer(
    tokens, doc_ids, down_query, down_key, down_rotary, query_gain, key_gain,
    up_query, up_key, up_value, output_weight, out_gain,
):
    z = lax.axis_index("z")
    x = lax.axis_index("x")
    y = lax.axis_index("y")
    c = lax.axis_index("c")
    sp = z * NX + x
    here = jnp.stack([z, x, y, c, sp * 256]).astype(jnp.int32)
    swap = [(0, 1), (1, 0)]

    message = call(
        pack, jax.ShapeDtypeStruct((NZ, 40, 128), BF), 1, 3, scratch=[VMEM((128, 128), F32)]
    )(here, down_query, down_key, down_rotary)
    gathered = lax.all_to_all(message, "z", 0, 0)
    gathered = [gathered] + [lax.ppermute(gathered, "x", ring(j)) for j in range(1, NX)]

    rows = [tokens] + [lax.ppermute(tokens, "y", ring(j)) for j in range(1, NY)]

    later = call(pack_later, jax.ShapeDtypeStruct((64, 128), BF), 0, 5)(
        up_query, up_key, up_value, doc_ids.reshape(2, 128), output_weight.T
    )
    later = [later] + [lax.ppermute(later, "x", ring(j)) for j in range(1, NX)]
    later = jnp.broadcast_to(jnp.stack(later)[None], (NZ, NX, 64, 128))

    q_part, k_part = call(
        project,
        (jax.ShapeDtypeStruct((64, 128), BF), jax.ShapeDtypeStruct((NZ, 72, 128), BF)),
        1, 8, scratch=[VMEM((128, 1024), BF), VMEM((NX, NZ, 40, 128), BF)],
    )(here, *rows, *gathered)

    stage1 = lax.all_to_all(k_part, "z", 0, 0)
    stage2 = [lax.ppermute(stage1, AXES, shift_pairs(2, j)) for j in range(1, 4)]
    held = jnp.stack([stage1] + stage2)
    stage3 = [lax.ppermute(held, AXES, shift_pairs(3, j)) for j in range(1, 4)]

    up_own = lax.all_to_all(later, "z", 0, 0)
    up_other = lax.ppermute(up_own, "c", swap)
    q_pair = jnp.stack([q_part, lax.ppermute(q_part, "c", swap)])
    q_all = [q_pair] + [lax.ppermute(q_pair, "y", ring(j)) for j in range(1, NY)]
    queries, uk, uv, key_docs = call(
        make_queries,
        (
            jax.ShapeDtypeStruct((4, 256, 256), BF),
            jax.ShapeDtypeStruct((256, 256), BF),
            jax.ShapeDtypeStruct((256, 256), BF),
            jax.ShapeDtypeStruct((NS, 128), F32),
        ),
        1, 7, scratch=[VMEM((256, 256), F32), VMEM((2, NZ, NX, 32, 128), BF)],
    )(here, *q_all, up_own, up_other, query_gain.reshape(2, 128))

    query_docs = doc_ids.astype(F32).reshape(4, 2, 32).transpose(1, 0, 2).reshape(2, 128)
    keep, send, ml = call(
        attend,
        (
            jax.ShapeDtypeStruct((256, 128), F32),
            jax.ShapeDtypeStruct((256, 128), BF),
            jax.ShapeDtypeStruct((8, 256), F32),
        ),
        2, 10, room=34,
        scratch=[
            VMEM((4, 4, NZ, 72, 128), BF),
            VMEM((16, 4, 256, 256), F32),
            VMEM((16, 256, 256), BF),
            VMEM((4, 8, 256), F32),
            VMEM((4, 8, 256), F32),
            VMEM((256, 256), F32),
            VMEM((256, 128), F32),
        ],
    )(here, doc_ids, queries, uk, uv, key_docs, key_gain.reshape(2, 128), query_docs, held, *stage3)

    got = lax.ppermute(send, "c", swap)
    ml_got = lax.ppermute(ml, "c", swap)
    *parts, log_sums = call(
        combine,
        (jax.ShapeDtypeStruct((32, 1024), BF),) * NY + (jax.ShapeDtypeStruct((2, 256), F32),),
        1, 6, scratch=[VMEM((128, 1024), F32), VMEM((2, NZ, NX, 32, 128), BF)],
    )(here, keep, got, ml, ml_got, up_own, up_other)
    parts[1:] = [lax.ppermute(parts[j], "y", ring(j)) for j in range(1, NY)]
    mixed = call(finish, jax.ShapeDtypeStruct((32, 1024), BF), 0, 5)(
        *parts, out_gain.reshape(1, 1024)
    )
    log_sums = log_sums.reshape(2, 2, 4, 32).transpose(2, 1, 3, 0).reshape(256, 2)
    return mixed, log_sums


def solution(mesh):
    finer = Mesh(mesh.devices.reshape(NZ, NX, NY, NC), AXES)
    return jax.shard_map(
        layer,
        mesh=finer,
        in_specs=(
            P(AXES, None), P(SP), P(SP, None), P(SP, None), P(SP, None), P(), P(),
            P(SP, TP), P(SP, TP), P(SP, TP), P(TP, SP), P(),
        ),
        out_specs=(P(AXES, None), P(SP, TP)),
        check_vma=False,
    )
```

```python
import math

import jax
import jax.numpy as jnp
import numpy as np
from jax import lax
from jax.experimental import pallas as pl
from jax.experimental.pallas import tpu as pltpu
from jax.sharding import Mesh
from jax.sharding import PartitionSpec as P


NOPE = 64
ROPE = 32
NZ, NX, NY, NC = 8, 4, 4, 2
NS = NZ * NX
AXES = ("z", "x", "y", "c")
SP = ("z", "x")
TP = ("y", "c")
NEG_BIG = -1e30
FLOOR = -1e20
THETA = 10000.0
EPS = 1e-06
LN2 = math.log(2.0)
SCALE2 = 1.0 / math.sqrt(NOPE + ROPE) / LN2
BF = jnp.bfloat16
F32 = jnp.float32


VMEM = pltpu.VMEM
SMEM_SPEC = pl.BlockSpec(memory_space=pltpu.SMEM)
VMEM_SPEC = pl.BlockSpec(memory_space=pltpu.VMEM)
ANY_SPEC = pl.BlockSpec(memory_space=pltpu.HBM)


def call(body, outs, n_smem, n_in, scratch=(), any_from=None, cost=None, room=16):
    specs = [SMEM_SPEC] * n_smem
    for i in range(n_in):
        specs.append(ANY_SPEC if any_from is not None and i >= any_from else VMEM_SPEC)
    single = not isinstance(outs, tuple)
    return pl.pallas_call(
        body,
        out_shape=outs,
        in_specs=specs,
        out_specs=VMEM_SPEC if single else tuple(VMEM_SPEC for _ in outs),
        scratch_shapes=list(scratch),
        compiler_params=pltpu.CompilerParams(vmem_limit_bytes=room * 1024 * 1024),
        cost_estimate=cost,
    )


def lanes(shape):
    return lax.broadcasted_iota(jnp.int32, shape, len(shape) - 1)


def column(row):
    return jnp.transpose(jnp.broadcast_to(row, (128, 128)))


def frequency(index):
    value = jnp.ones(index.shape, F32)
    for bit in range(4):
        factor = THETA ** (-(1 << bit) / 16)
        value = value * jnp.where((index // (1 << bit)) % 2 == 1, factor, 1.0)
    return value


def picks():
    pick = np.zeros((192, 256), np.float32)
    for lane in range(192):
        if lane < 128:
            src = 96 * (lane // 64) + lane % 64
        else:
            turn = lane - 128
            src = 64 + 96 * (turn // 32) + 16 * ((turn // 4) % 2) + 4 * ((turn % 32) // 8) + turn % 4
        pick[src, lane] = 1.0
    return pick


def pack(where, *refs):
    inputs, out, flipped, places, sems = refs[:9], refs[9], refs[10], refs[11:20], refs[20]
    copies = [
        pltpu.make_async_copy(source, place, sems.at[i])
        for i, (source, place) in enumerate(zip(inputs, places))
    ]
    for copy in copies:
        copy.start()
    for copy in copies:
        copy.wait()
    dq, dk, dr, up_query, pick, up_key, up_value, docs_ref, out_t = places
    y = where[2]

    def chosen(ref):
        block = ref[:, 0:64]
        for k in range(1, NY):
            block = jnp.where(y == k, ref[:, 64 * k : 64 * (k + 1)], block)
        return block

    block = jnp.concatenate([chosen(dq), chosen(dk)], axis=1)
    rope = dr[...].astype(F32)
    rope = jnp.concatenate([rope, jnp.zeros((32, 96), F32)], axis=1)
    flipped[...] = jnp.transpose(jnp.concatenate([rope] * 4, axis=0))
    turned = jnp.concatenate([flipped[pl.ds(4 * y, 4), :], flipped[pl.ds(16 + 4 * y, 4), :]], axis=0)
    turned = turned.astype(BF)
    sorted_query = jnp.dot(up_query[...], pick[...], preferred_element_type=F32)
    plain = sorted_query[:, 0:128].astype(BF)
    mixed = sorted_query[:, 128:256]
    docs = docs_ref[...].astype(F32)
    row = lax.broadcasted_iota(jnp.int32, (8, 128), 0)
    at = lanes((8, 128))
    for r in range(8):
        line = docs[r // 4 : r // 4 + 1, :]
        moved = pltpu.roll(jnp.broadcast_to(line, (8, 128)), (64 - 32 * (r % 4)) % 128, 1)
        mixed = jnp.where((row == r) & (at // 32 == 2), moved, mixed)
    mixed = mixed.astype(BF)
    for z in range(NZ):
        out[z, 0:32, :] = block
        out[z, 32:40, :] = turned
        out[z, 40:48, :] = plain
        out[z, 48:56, :] = up_key[...]
        out[z, 56:64, :] = up_value[...]
        out[z, 64:72, :] = mixed
        out[z, 72:104, :] = out_t[...]


def project(where, t0, t1, t2, t3, g0, g1, g2, g3, q_ref, k_ref, tok, gathered):
    x = where[1]
    y = where[2]
    for j, part in enumerate((t0, t1, t2, t3)):
        at = lax.rem(y - j + NY, NY)
        tok[pl.ds(pl.multiple_of(at * 32, 32), 32), :] = part[...]
    for j, part in enumerate((g0, g1, g2, g3)):
        gathered[lax.rem(x - j + NX, NX)] = part[:, 0:40, :]
    rows = tok[...]
    weights = jnp.concatenate(
        [gathered[k, z, 0:32, :] for z in range(NZ) for k in range(NX)], axis=0
    )
    both = jnp.dot(rows, weights, preferred_element_type=F32)
    turned = jnp.transpose(both).astype(BF)
    q_ref[...] = turned[0:64, :]
    for t in range(NZ):
        k_ref[t, 0:64, :] = turned[64:128, :]
    group = lanes((8, 128)) // 32
    pieces = []
    for z in range(NZ):
        piece = gathered[0, z, 32:40, :].astype(F32)
        for g in range(1, 4):
            piece = jnp.where(group == g, gathered[g, z, 32:40, :].astype(F32), piece)
        pieces.append(piece)
    rope = jnp.concatenate(pieces, axis=1)
    rope = jnp.concatenate([rope, jnp.zeros_like(rope)], axis=0).astype(BF)
    raw = lax.dot_general(rope, rows, (((1,), (1,)), ((), ())), preferred_element_type=F32)
    raw = raw[0:8, :].astype(BF).astype(F32)
    at = lanes((8, 128))
    row = lax.broadcasted_iota(jnp.int32, (8, 128), 0)
    pos = where[4] + 64 * (at // 32) + 32 * where[3] + at % 32
    angle = pos.astype(F32) * frequency(4 * y + row % 4)
    sine = jnp.sin(angle)
    rotated = raw * jnp.cos(angle) + pltpu.roll(raw, 4, 0) * jnp.where(row < 4, -sine, sine)
    rotated = rotated.astype(BF)
    for t in range(NZ):
        k_ref[t, 64:72, :] = rotated


def make_queries(
    where, q0, q1, q2, q3, up_own, up_other, gain, key_gain, out, uk_ref, uv_ref, docs_ref, col_ref,
    latents, ups,
):
    x, y, c = where[1], where[2], where[3]
    for j, part in enumerate((q0, q1, q2, q3)):
        own, other = part[0].astype(F32), part[1].astype(F32)
        rows = pl.ds(pl.multiple_of(lax.rem(y - j + NY, NY) * 64, 64), 64)
        latents[rows, 0:128] = jnp.where(c == 0, own, other)
        latents[rows, 128:256] = jnp.where(c == 0, other, own)
    raw = latents[...]
    mean = jnp.sum(raw * raw, axis=0, keepdims=True) * (1.0 / 256.0)
    inverse = lax.rsqrt(mean + EPS)
    gains = jnp.concatenate([column(gain[0:1, :]), column(gain[1:2, :])], axis=0)
    gains = jnp.concatenate([gains, gains], axis=1)
    for i in range(2):
        col_ref[128 * i : 128 * (i + 1), :] = column(key_gain[i : i + 1, :])
    latent = (raw * inverse * gains).astype(BF)
    tok = lanes((64, 256))
    row = lax.broadcasted_iota(jnp.int32, (64, 256), 0)
    pos = where[4] + 64 * ((tok % 128) // 32) + 32 * (tok // 128) + tok % 32
    angle = pos.astype(F32) * frequency(4 * ((row % 32) // 8) + row % 4)
    is_low = (row // 4) % 2 == 0
    cos = jnp.cos(angle)
    sine = jnp.sin(angle)
    low_sin = jnp.where(is_low, -sine, 0.0)
    high_sin = jnp.where(is_low, 0.0, sine)
    for p, up in enumerate((up_own, up_other)):
        for j in range(NX):
            ups[p, :, lax.rem(x - j + NX, NX)] = up[j, :, 0:32, :]
        wide = ups[p].reshape(NS, 32, 128).astype(F32)
        own = slice(128 * p, 128 * (p + 1))
        plain_w = jnp.transpose(wide[:, 0:8, :].reshape(256, 128)).astype(BF)
        rope_w = jnp.transpose(wide[:, 24:32, :].reshape(256, 128))[0:64, :].astype(BF)
        uk_ref[:, own] = wide[:, 8:16, :].reshape(256, 128).astype(BF)
        uv_ref[own, :] = jnp.transpose(wide[:, 16:24, :].reshape(256, 128)).astype(BF)
        plain = (jnp.dot(plain_w, latent, preferred_element_type=F32) * SCALE2).astype(BF)
        raw = jnp.dot(rope_w, latent, preferred_element_type=F32) * SCALE2
        rope = raw * cos + pltpu.roll(raw, 60, 0) * low_sin + pltpu.roll(raw, 4, 0) * high_sin
        rope = rope.astype(BF)
        for i in range(2):
            h = 2 * p + i
            out[h] = jnp.zeros((256, 256), BF)
            out[h, 64 * i : 64 * (i + 1), :] = plain[64 * i : 64 * (i + 1), :]
            out[h, 128:160, :] = rope[32 * i : 32 * (i + 1), :]
    docs = ups[0].reshape(NS, 32, 128)[:, 24:32, :].astype(F32)
    at = lanes((NS, 128))
    spread = jnp.zeros((NS, 128), F32)
    for k in range(NY):
        piece = jnp.where(c == 0, docs[:, 2 * k, :], docs[:, 2 * k + 1, :])
        spread = jnp.where(at // 32 == k, pltpu.roll(piece, (32 * k + 64) % 128, 1), spread)
    docs_ref[...] = spread


def attend(
    where, ids, q_ref, uk, uv, key_docs, gains, query_docs, b0, b1, b2, b3,
    keep_ref, send_ref, ml_ref, kb, s_buf, v_buf, mx, total, acc,
):
    x0, y0, c = where[1], where[2], where[3]
    docs = key_docs[...]
    at = lanes((NS, 128))
    before = (at == 127) & (docs < ids[0].astype(F32))
    behind = (at == 0) & (docs > ids[255].astype(F32))
    low = jnp.sum(before.astype(jnp.int32))
    high = NS - 1 - jnp.sum(behind.astype(jnp.int32))
    first = low // 2
    last = jnp.maximum(high // 2, first) + 1

    def fetch(z, carry):
        for j, part in enumerate((b0, b1, b2, b3)):
            for k in range(4):
                kb[j, k, z] = part[k, z]
        return carry

    lax.fori_loop(first // 2, (last + 1) // 2, fetch, 0)
    mx[...] = jnp.full(mx.shape, NEG_BIG, F32)
    total[...] = jnp.zeros(total.shape, F32)
    acc[...] = jnp.zeros(acc.shape, F32)
    wanted = jnp.concatenate([query_docs[0:1, :], query_docs[1:2, :]], axis=1)

    def scores(tile, carry):
        z = tile // 2
        latents, ropes, same = [], [], []
        for half in range(2):
            x = 2 * lax.rem(tile, 2) + half
            jx = lax.rem(x0 - x + NX, NX)
            parts, turned = [], []
            for y in range(NY):
                jy = lax.rem(y0 - y + NY, NY)
                third = jnp.where(c == 0, jy, jx)
                second = jnp.where(c == 0, jx, jy)
                slab = kb[third, second, z].astype(F32)
                parts.append(slab[0:64, :])
                turned.append(slab[64:72, :])
            squares = parts[0] * parts[0]
            for part in parts[1:]:
                squares = squares + part * part
            mean = jnp.sum(squares, axis=0, keepdims=True) * (1.0 / 256.0)
            inverse = lax.rsqrt(mean + EPS)
            latents.append(jnp.concatenate(parts, axis=0) * inverse * gains[...])
            ropes.append(jnp.concatenate(turned, axis=0))
            docs_col = column(key_docs[pl.ds(2 * tile + half, 1), :])
            same.append(jnp.concatenate([docs_col, docs_col], axis=1) == wanted)
        latent = jnp.concatenate(latents, axis=1)
        v_buf[tile] = jnp.dot(uv[...], latent.astype(BF), preferred_element_type=F32).astype(BF)
        turned = jnp.transpose(latent).astype(BF)
        rope = jnp.concatenate(ropes, axis=1)
        rope = jnp.concatenate([rope, jnp.zeros((96, 256), F32)], axis=0)
        rope = jnp.transpose(rope).astype(BF)
        keys = jnp.dot(turned, uk[...], preferred_element_type=F32).astype(BF)
        for h in range(4):
            p = h // 2
            stack = jnp.concatenate([keys[:, 128 * p : 128 * (p + 1)], rope], axis=1)
            got = jnp.dot(stack, q_ref[h], preferred_element_type=F32)
            got = jnp.concatenate(
                [
                    jnp.where(same[0], got[0:128, :], NEG_BIG),
                    jnp.where(same[1], got[128:256, :], NEG_BIG),
                ],
                axis=0,
            )
            s_buf[tile, h] = got
            mx[h] = jnp.maximum(mx[h], jnp.max(got.reshape(32, 8, 256), axis=0))
        return carry

    lax.fori_loop(first, last, scores, 0)
    tops = []
    for h in range(4):
        top = jnp.maximum(jnp.max(mx[h], axis=0, keepdims=True), FLOOR)
        mx[h] = jnp.broadcast_to(top, (8, 256))
        tops.append(top)

    def weigh(tile, carry):
        for h in range(4):
            own = slice(64 * h, 64 * (h + 1))
            weights = jnp.exp2(s_buf[tile, h].reshape(32, 8, 256) - mx[h][None])
            total[h] = total[h] + jnp.sum(weights, axis=0)
            weights = weights.reshape(256, 256).astype(BF)
            acc[own, :] = acc[own, :] + jnp.dot(
                v_buf[tile, own, :], weights, preferred_element_type=F32
            )
        return carry

    lax.fori_loop(first, last, weigh, 0)
    for h in range(4):
        ml_ref[h : h + 1, :] = tops[h]
        ml_ref[4 + h : 5 + h, :] = jnp.sum(total[h], axis=0, keepdims=True)
    left, right = acc[:, 0:128], acc[:, 128:256]
    keep_ref[...] = jnp.where(c == 0, left, right)
    send_ref[...] = jnp.where(c == 0, right, left).astype(BF)


def combine(
    where, keep, got, ml_own, ml_got, w_own, w_other, part_ref, p1_ref, p2_ref, p3_ref, lse_ref,
    scratch, outs,
):
    x, c = where[1], where[3]
    m0, l0 = ml_own[0:4, :], ml_own[4:8, :]
    m1 = jnp.concatenate([ml_got[2:4, :], ml_got[0:2, :]], axis=0)
    l1 = jnp.concatenate([ml_got[6:8, :], ml_got[4:6, :]], axis=0)
    top = jnp.maximum(m0, m1)
    e0 = jnp.exp2(m0 - top)
    e1 = jnp.exp2(m1 - top)
    weight_sum = l0 * e0 + l1 * e1
    lse_ref[...] = ((top + jnp.log2(weight_sum)) * LN2)[0:2, :]
    f0 = e0 / weight_sum
    f1 = e1 / weight_sum
    f0 = jnp.where(c == 0, f0[:, 0:128], f0[:, 128:256])
    f1 = jnp.where(c == 0, f1[:, 0:128], f1[:, 128:256])
    result = jnp.zeros((128, 1024), F32)
    for p, w in enumerate((w_own, w_other)):
        pieces = []
        for i in range(2):
            h, k = 2 * p + i, (2 * p + i + 2) % 4
            mine = keep[64 * h : 64 * (h + 1), :]
            theirs = got[64 * k : 64 * (k + 1), :].astype(F32)
            pieces.append(mine * f0[h : h + 1, :] + theirs * f1[h : h + 1, :])
        attended = jnp.transpose(jnp.concatenate(pieces, axis=0)).astype(BF)
        for j in range(NX):
            outs[p, :, lax.rem(x - j + NX, NX)] = w[j, :, 32:64, :]
        result = result + lax.dot_general(
            attended, outs[p].reshape(1024, 128), (((1,), (1,)), ((), ())),
            preferred_element_type=F32,
        )
    scratch[...] = result
    y = where[2]
    for j, out in enumerate((part_ref, p1_ref, p2_ref, p3_ref)):
        to = lax.rem(y + j, NY)
        out[...] = scratch[pl.ds(pl.multiple_of(to * 32, 32), 32), :].astype(BF)


def finish(part, p1, p2, p3, gain, out):
    summed = part[...].astype(F32)
    for other in (p1, p2, p3):
        summed = summed + other[...].astype(F32)
    wide = summed.astype(BF).astype(F32)
    mean = jnp.mean(wide * wide, axis=1, keepdims=True)
    out[...] = (wide * lax.rsqrt(mean + EPS) * gain[...]).astype(BF)


def flat(z, x, y, c):
    return ((z * NX + x) * NY + y) * NC + c


def ring(j):
    return [(i, (i + j) % NY) for i in range(NY)]


def shift_pairs(stage, j):
    pairs = []
    for z in range(NZ):
        for x in range(NX):
            for y in range(NY):
                for c in range(NC):
                    along_x = (c == 0) == (stage == 2)
                    to = flat(z, (x + j) % NX, y, c) if along_x else flat(z, x, (y + j) % NY, c)
                    pairs.append((flat(z, x, y, c), to))
    return pairs


def layer(
    tokens, doc_ids, down_query, down_key, down_rotary, query_gain, key_gain,
    up_query, up_key, up_value, output_weight, out_gain,
):
    z = lax.axis_index("z")
    x = lax.axis_index("x")
    y = lax.axis_index("y")
    c = lax.axis_index("c")
    sp = z * NX + x
    here = jnp.stack([z, x, y, c, sp * 256]).astype(jnp.int32)
    swap = [(0, 1), (1, 0)]

    sources = (
        down_query, down_key, down_rotary, up_query, jnp.asarray(picks(), BF), up_key,
        up_value, doc_ids.reshape(2, 128), output_weight.T,
    )
    message = call(
        pack, jax.ShapeDtypeStruct((NZ, 104, 128), BF), 1, 9, any_from=0,
        scratch=[VMEM((128, 128), F32)]
        + [VMEM(a.shape, a.dtype) for a in sources]
        + [pltpu.SemaphoreType.DMA((9,))],
    )(here, *(pltpu.with_memory_space_constraint(a, pltpu.HBM) for a in sources))
    arrived = lax.all_to_all(message, "z", 0, 0)
    sent = arrived[:, 0:40, :]
    gathered = [arrived] + [lax.ppermute(sent, "x", ring(j)) for j in range(1, NX)]

    rows = [tokens] + [lax.ppermute(tokens, "y", ring(j)) for j in range(1, NY)]

    q_part, k_part = call(
        project,
        (jax.ShapeDtypeStruct((64, 128), BF), jax.ShapeDtypeStruct((NZ, 72, 128), BF)),
        1, 8, scratch=[VMEM((128, 1024), BF), VMEM((NX, NZ, 40, 128), BF)],
    )(here, *rows, *gathered)

    stage1 = lax.all_to_all(k_part, "z", 0, 0)
    stage2 = [lax.ppermute(stage1, AXES, shift_pairs(2, j)) for j in range(1, 4)]
    held = jnp.stack([stage1] + stage2)
    stage3 = [lax.ppermute(held, AXES, shift_pairs(3, j)) for j in range(1, 4)]

    later = arrived[:, 40:104, :]
    later = [later] + [lax.ppermute(later, "x", ring(j)) for j in range(1, NX)]
    up_own = jnp.stack(later)
    up_other = lax.ppermute(up_own, "c", swap)
    q_pair = jnp.stack([q_part, lax.ppermute(q_part, "c", swap)])
    q_all = [q_pair] + [lax.ppermute(q_pair, "y", ring(j)) for j in range(1, NY)]
    queries, uk, uv, key_docs, gains = call(
        make_queries,
        (
            jax.ShapeDtypeStruct((4, 256, 256), BF),
            jax.ShapeDtypeStruct((256, 256), BF),
            jax.ShapeDtypeStruct((256, 256), BF),
            jax.ShapeDtypeStruct((NS, 128), F32),
            jax.ShapeDtypeStruct((256, 128), F32),
        ),
        1, 8, scratch=[VMEM((256, 256), F32), VMEM((2, NZ, NX, 32, 128), BF)],
    )(here, *q_all, up_own, up_other, query_gain.reshape(2, 128), key_gain.reshape(2, 128))

    query_docs = doc_ids.astype(F32).reshape(4, 2, 32).transpose(1, 0, 2).reshape(2, 128)
    keep, send, ml = call(
        attend,
        (
            jax.ShapeDtypeStruct((256, 128), F32),
            jax.ShapeDtypeStruct((256, 128), BF),
            jax.ShapeDtypeStruct((8, 256), F32),
        ),
        2, 10, room=34,
        scratch=[
            VMEM((4, 4, NZ, 72, 128), BF),
            VMEM((16, 4, 256, 256), F32),
            VMEM((16, 256, 256), BF),
            VMEM((4, 8, 256), F32),
            VMEM((4, 8, 256), F32),
            VMEM((256, 256), F32),
        ],
    )(here, doc_ids, queries, uk, uv, key_docs, gains, query_docs, held, *stage3)

    got = lax.ppermute(send, "c", swap)
    ml_got = lax.ppermute(ml, "c", swap)
    *parts, log_sums = call(
        combine,
        (jax.ShapeDtypeStruct((32, 1024), BF),) * NY + (jax.ShapeDtypeStruct((2, 256), F32),),
        1, 6, scratch=[VMEM((128, 1024), F32), VMEM((2, NZ, NX, 32, 128), BF)],
    )(here, keep, got, ml, ml_got, up_own, up_other)
    parts[1:] = [lax.ppermute(parts[j], "y", ring(j)) for j in range(1, NY)]
    mixed = call(finish, jax.ShapeDtypeStruct((32, 1024), BF), 0, 5)(
        *parts, out_gain.reshape(1, 1024)
    )
    log_sums = log_sums.reshape(2, 2, 4, 32).transpose(2, 1, 3, 0).reshape(256, 2)
    return mixed, log_sums


def solution(mesh):
    finer = Mesh(mesh.devices.reshape(NZ, NX, NY, NC), AXES)
    return jax.shard_map(
        layer,
        mesh=finer,
        in_specs=(
            P(AXES, None), P(SP), P(SP, None), P(SP, None), P(SP, None), P(), P(),
            P(SP, TP), P(SP, TP), P(SP, TP), P(TP, SP), P(),
        ),
        out_specs=(P(AXES, None), P(SP, TP)),
        check_vma=False,
    )
```

```python
import math

import jax
import jax.numpy as jnp
from jax import lax
from jax.experimental import pallas as pl
from jax.experimental.pallas import tpu as pltpu
from jax.sharding import Mesh
from jax.sharding import PartitionSpec as P


NOPE = 64
ROPE = 32
NZ, NX, NY, NC = 8, 4, 4, 2
NS = NZ * NX
AXES = ("z", "x", "y", "c")
SP = ("z", "x")
TP = ("y", "c")
NEG_BIG = -1e30
FLOOR = -1e20
THETA = 10000.0
EPS = 1e-06
LN2 = math.log(2.0)
SCALE2 = 1.0 / math.sqrt(NOPE + ROPE) / LN2
BF = jnp.bfloat16
F32 = jnp.float32


VMEM = pltpu.VMEM
SMEM_SPEC = pl.BlockSpec(memory_space=pltpu.SMEM)
VMEM_SPEC = pl.BlockSpec(memory_space=pltpu.VMEM)
ANY_SPEC = pl.BlockSpec(memory_space=pltpu.HBM)


def call(body, outs, n_smem, n_in, scratch=(), any_from=None, cost=None, room=16):
    specs = [SMEM_SPEC] * n_smem
    for i in range(n_in):
        specs.append(ANY_SPEC if any_from is not None and i >= any_from else VMEM_SPEC)
    single = not isinstance(outs, tuple)
    return pl.pallas_call(
        body,
        out_shape=outs,
        in_specs=specs,
        out_specs=VMEM_SPEC if single else tuple(VMEM_SPEC for _ in outs),
        scratch_shapes=list(scratch),
        compiler_params=pltpu.CompilerParams(vmem_limit_bytes=room * 1024 * 1024),
        cost_estimate=cost,
    )


def lanes(shape):
    return lax.broadcasted_iota(jnp.int32, shape, len(shape) - 1)


def column(row):
    return jnp.transpose(jnp.broadcast_to(row, (128, 128)))


def frequency(index):
    value = jnp.ones(index.shape, F32)
    for bit in range(4):
        factor = THETA ** (-(1 << bit) / 16)
        value = value * jnp.where((index // (1 << bit)) % 2 == 1, factor, 1.0)
    return value


def pack(where, dq_in, dk_in, dr_in, out, flipped, dq, dk, dr, sems):
    copies = [
        pltpu.make_async_copy(source, place, sems.at[i])
        for i, (source, place) in enumerate(((dq_in, dq), (dk_in, dk), (dr_in, dr)))
    ]
    for copy in copies:
        copy.start()
    for copy in copies:
        copy.wait()
    y = where[2]

    def chosen(ref):
        block = ref[:, 0:64]
        for k in range(1, NY):
            block = jnp.where(y == k, ref[:, 64 * k : 64 * (k + 1)], block)
        return block

    block = jnp.concatenate([chosen(dq), chosen(dk)], axis=1)
    rope = dr[...].astype(F32)
    rope = jnp.concatenate([rope, jnp.zeros((32, 96), F32)], axis=1)
    flipped[...] = jnp.transpose(jnp.concatenate([rope] * 4, axis=0))
    turned = jnp.concatenate([flipped[pl.ds(4 * y, 4), :], flipped[pl.ds(16 + 4 * y, 4), :]], axis=0)
    turned = turned.astype(BF)
    for z in range(NZ):
        out[z, 0:32, :] = block
        out[z, 32:40, :] = turned


def pack_later(up_query, up_key, up_value, docs_ref, out_t, out):
    src = lax.broadcasted_iota(jnp.int32, (192, 256), 0)
    lane = lanes((192, 256))
    plain = 96 * (lane // 64) + lane % 64
    turn = lane - 128
    rope = 64 + 96 * (turn // 32) + 16 * ((turn // 4) % 2) + 4 * ((turn % 32) // 8) + turn % 4
    chosen = jnp.where(lane < 128, plain, jnp.where(lane < 192, rope, -1))
    pick = jnp.where(src == chosen, 1.0, 0.0).astype(BF)
    sorted_query = jnp.dot(up_query[...], pick, preferred_element_type=F32)
    out[0:8, :] = sorted_query[:, 0:128].astype(BF)
    out[8:16, :] = up_key[...]
    out[16:24, :] = up_value[...]
    mixed = sorted_query[:, 128:256]
    docs = docs_ref[...].astype(F32)
    row = lax.broadcasted_iota(jnp.int32, (8, 128), 0)
    at = lanes((8, 128))
    for r in range(8):
        line = docs[r // 4 : r // 4 + 1, :]
        moved = pltpu.roll(jnp.broadcast_to(line, (8, 128)), (64 - 32 * (r % 4)) % 128, 1)
        mixed = jnp.where((row == r) & (at // 32 == 2), moved, mixed)
    out[24:32, :] = mixed.astype(BF)
    out[32:64, :] = out_t[...]


def project(where, t0, t1, t2, t3, g0, g1, g2, g3, q_ref, k_ref, tok, gathered):
    x = where[1]
    y = where[2]
    for j, part in enumerate((t0, t1, t2, t3)):
        at = lax.rem(y - j + NY, NY)
        tok[pl.ds(pl.multiple_of(at * 32, 32), 32), :] = part[...]
    for j, part in enumerate((g0, g1, g2, g3)):
        gathered[lax.rem(x - j + NX, NX)] = part[...]
    rows = tok[...]
    weights = jnp.concatenate(
        [gathered[k, z, 0:32, :] for z in range(NZ) for k in range(NX)], axis=0
    )
    both = jnp.dot(rows, weights, preferred_element_type=F32)
    turned = jnp.transpose(both).astype(BF)
    q_ref[...] = turned[0:64, :]
    for t in range(NZ):
        k_ref[t, 0:64, :] = turned[64:128, :]
    group = lanes((8, 128)) // 32
    pieces = []
    for z in range(NZ):
        piece = gathered[0, z, 32:40, :].astype(F32)
        for g in range(1, 4):
            piece = jnp.where(group == g, gathered[g, z, 32:40, :].astype(F32), piece)
        pieces.append(piece)
    rope = jnp.concatenate(pieces, axis=1)
    rope = jnp.concatenate([rope, jnp.zeros_like(rope)], axis=0).astype(BF)
    raw = lax.dot_general(rope, rows, (((1,), (1,)), ((), ())), preferred_element_type=F32)
    raw = raw[0:8, :].astype(BF).astype(F32)
    at = lanes((8, 128))
    row = lax.broadcasted_iota(jnp.int32, (8, 128), 0)
    pos = where[4] + 64 * (at // 32) + 32 * where[3] + at % 32
    angle = pos.astype(F32) * frequency(4 * y + row % 4)
    sine = jnp.sin(angle)
    rotated = raw * jnp.cos(angle) + pltpu.roll(raw, 4, 0) * jnp.where(row < 4, -sine, sine)
    rotated = rotated.astype(BF)
    for t in range(NZ):
        k_ref[t, 64:72, :] = rotated


def make_queries(
    where, q0, q1, q2, q3, q_other, up_own, up_other, gain, key_gain, docs_in,
    out, uk_ref, uv_ref, docs_ref, col_ref, row_ref, latents, ups,
):
    x, y, c = where[1], where[2], where[3]
    for j, part in enumerate((q0, q1, q2, q3)):
        own, other = part[...].astype(F32), q_other[j].astype(F32)
        rows = pl.ds(pl.multiple_of(lax.rem(y - j + NY, NY) * 64, 64), 64)
        latents[rows, 0:128] = jnp.where(c == 0, own, other)
        latents[rows, 128:256] = jnp.where(c == 0, other, own)
    raw = latents[...]
    mean = jnp.sum(raw * raw, axis=0, keepdims=True) * (1.0 / 256.0)
    inverse = lax.rsqrt(mean + EPS)
    gains = jnp.concatenate([column(gain[0:1, :]), column(gain[1:2, :])], axis=0)
    gains = jnp.concatenate([gains, gains], axis=1)
    tokens_docs = docs_in[...].astype(F32)
    at = lanes((1, 128))
    for i in range(2):
        col_ref[128 * i : 128 * (i + 1), :] = column(key_gain[i : i + 1, :])
        ordered = jnp.zeros((1, 128), F32)
        for k in range(NY):
            line = tokens_docs[k // 2 : k // 2 + 1, :]
            moved = pltpu.roll(line, (32 * k - 64 * (k % 2) - 32 * i) % 128, 1)
            ordered = jnp.where(at // 32 == k, moved, ordered)
        row_ref[i : i + 1, :] = ordered
    latent = (raw * inverse * gains).astype(BF)
    tok = lanes((64, 256))
    row = lax.broadcasted_iota(jnp.int32, (64, 256), 0)
    pos = where[4] + 64 * ((tok % 128) // 32) + 32 * (tok // 128) + tok % 32
    angle = pos.astype(F32) * frequency(4 * ((row % 32) // 8) + row % 4)
    is_low = (row // 4) % 2 == 0
    cos = jnp.cos(angle)
    sine = jnp.sin(angle)
    low_sin = jnp.where(is_low, -sine, 0.0)
    high_sin = jnp.where(is_low, 0.0, sine)
    for p, up in enumerate((up_own, up_other)):
        for j in range(NX):
            ups[p, :, lax.rem(x - j + NX, NX)] = up[:, j, 0:32, :]
        wide = ups[p].reshape(NS, 32, 128).astype(F32)
        own = slice(128 * p, 128 * (p + 1))
        plain_w = jnp.transpose(wide[:, 0:8, :].reshape(256, 128)).astype(BF)
        rope_w = jnp.transpose(wide[:, 24:32, :].reshape(256, 128))[0:64, :].astype(BF)
        uk_ref[:, own] = wide[:, 8:16, :].reshape(256, 128).astype(BF)
        uv_ref[own, :] = jnp.transpose(wide[:, 16:24, :].reshape(256, 128)).astype(BF)
        plain = (jnp.dot(plain_w, latent, preferred_element_type=F32) * SCALE2).astype(BF)
        raw = jnp.dot(rope_w, latent, preferred_element_type=F32) * SCALE2
        rope = raw * cos + pltpu.roll(raw, 60, 0) * low_sin + pltpu.roll(raw, 4, 0) * high_sin
        rope = rope.astype(BF)
        for i in range(2):
            h = 2 * p + i
            out[h] = jnp.zeros((256, 256), BF)
            out[h, 64 * i : 64 * (i + 1), :] = plain[64 * i : 64 * (i + 1), :]
            out[h, 128:160, :] = rope[32 * i : 32 * (i + 1), :]
    docs = ups[0].reshape(NS, 32, 128)[:, 24:32, :].astype(F32)
    at = lanes((NS, 128))
    spread = jnp.zeros((NS, 128), F32)
    for k in range(NY):
        piece = jnp.where(c == 0, docs[:, 2 * k, :], docs[:, 2 * k + 1, :])
        spread = jnp.where(at // 32 == k, pltpu.roll(piece, (32 * k + 64) % 128, 1), spread)
    docs_ref[...] = spread


def attend(
    where, ids, q_ref, uk, uv, key_docs, gains, query_docs, b0, b1, b2, b3,
    keep_ref, send_ref, ml_ref, kb, s_buf, v_buf, mx, total, acc,
):
    x0, y0, c = where[1], where[2], where[3]
    docs = key_docs[...]
    at = lanes((NS, 128))
    before = (at == 127) & (docs < ids[0].astype(F32))
    behind = (at == 0) & (docs > ids[255].astype(F32))
    low = jnp.sum(before.astype(jnp.int32))
    high = NS - 1 - jnp.sum(behind.astype(jnp.int32))
    first = low // 2
    last = jnp.maximum(high // 2, first) + 1

    def fetch(z, carry):
        for j, part in enumerate((b0, b1, b2, b3)):
            for k in range(4):
                kb[j, k, z] = part[k, z]
        return carry

    lax.fori_loop(first // 2, (last + 1) // 2, fetch, 0)
    mx[...] = jnp.full(mx.shape, NEG_BIG, F32)
    total[...] = jnp.zeros(total.shape, F32)
    acc[...] = jnp.zeros(acc.shape, F32)
    wanted = jnp.concatenate([query_docs[0:1, :], query_docs[1:2, :]], axis=1)

    def scores(tile, carry):
        z = tile // 2
        latents, ropes, same = [], [], []
        for half in range(2):
            x = 2 * lax.rem(tile, 2) + half
            jx = lax.rem(x0 - x + NX, NX)
            parts, turned = [], []
            for y in range(NY):
                jy = lax.rem(y0 - y + NY, NY)
                third = jnp.where(c == 0, jy, jx)
                second = jnp.where(c == 0, jx, jy)
                slab = kb[third, second, z].astype(F32)
                parts.append(slab[0:64, :])
                turned.append(slab[64:72, :])
            squares = parts[0] * parts[0]
            for part in parts[1:]:
                squares = squares + part * part
            mean = jnp.sum(squares, axis=0, keepdims=True) * (1.0 / 256.0)
            inverse = lax.rsqrt(mean + EPS)
            latents.append(jnp.concatenate(parts, axis=0) * inverse * gains[...])
            ropes.append(jnp.concatenate(turned, axis=0))
            docs_col = column(key_docs[pl.ds(2 * tile + half, 1), :])
            same.append(jnp.concatenate([docs_col, docs_col], axis=1) == wanted)
        latent = jnp.concatenate(latents, axis=1)
        v_buf[tile] = jnp.dot(uv[...], latent.astype(BF), preferred_element_type=F32).astype(BF)
        turned = jnp.transpose(latent).astype(BF)
        rope = jnp.concatenate(ropes, axis=1)
        rope = jnp.concatenate([rope, jnp.zeros((96, 256), F32)], axis=0)
        rope = jnp.transpose(rope).astype(BF)
        keys = jnp.dot(turned, uk[...], preferred_element_type=F32).astype(BF)
        for h in range(4):
            p = h // 2
            stack = jnp.concatenate([keys[:, 128 * p : 128 * (p + 1)], rope], axis=1)
            got = jnp.dot(stack, q_ref[h], preferred_element_type=F32)
            got = jnp.concatenate(
                [
                    jnp.where(same[0], got[0:128, :], NEG_BIG),
                    jnp.where(same[1], got[128:256, :], NEG_BIG),
                ],
                axis=0,
            )
            s_buf[tile, h] = got
            mx[h] = jnp.maximum(mx[h], jnp.max(got.reshape(32, 8, 256), axis=0))
        return carry

    lax.fori_loop(first, last, scores, 0)
    tops = []
    for h in range(4):
        top = jnp.maximum(jnp.max(mx[h], axis=0, keepdims=True), FLOOR)
        mx[h] = jnp.broadcast_to(top, (8, 256))
        tops.append(top)

    def weigh(tile, carry):
        for h in range(4):
            own = slice(64 * h, 64 * (h + 1))
            weights = jnp.exp2(s_buf[tile, h].reshape(32, 8, 256) - mx[h][None])
            total[h] = total[h] + jnp.sum(weights, axis=0)
            weights = weights.reshape(256, 256).astype(BF)
            acc[own, :] = acc[own, :] + jnp.dot(
                v_buf[tile, own, :], weights, preferred_element_type=F32
            )
        return carry

    lax.fori_loop(first, last, weigh, 0)
    for h in range(4):
        ml_ref[h : h + 1, :] = tops[h]
        ml_ref[4 + h : 5 + h, :] = jnp.sum(total[h], axis=0, keepdims=True)
    left, right = acc[:, 0:128], acc[:, 128:256]
    keep_ref[...] = jnp.where(c == 0, left, right)
    send_ref[...] = jnp.where(c == 0, right, left).astype(BF)


def combine(
    where, keep, got, ml_own, ml_got, w_own, w_other, part_ref, p1_ref, p2_ref, p3_ref, lse_ref,
    scratch, outs,
):
    x, c = where[1], where[3]
    m0, l0 = ml_own[0:4, :], ml_own[4:8, :]
    m1 = jnp.concatenate([ml_got[2:4, :], ml_got[0:2, :]], axis=0)
    l1 = jnp.concatenate([ml_got[6:8, :], ml_got[4:6, :]], axis=0)
    top = jnp.maximum(m0, m1)
    e0 = jnp.exp2(m0 - top)
    e1 = jnp.exp2(m1 - top)
    weight_sum = l0 * e0 + l1 * e1
    lse_ref[...] = ((top + jnp.log2(weight_sum)) * LN2)[0:2, :]
    f0 = e0 / weight_sum
    f1 = e1 / weight_sum
    f0 = jnp.where(c == 0, f0[:, 0:128], f0[:, 128:256])
    f1 = jnp.where(c == 0, f1[:, 0:128], f1[:, 128:256])
    result = jnp.zeros((128, 1024), F32)
    for p, w in enumerate((w_own, w_other)):
        pieces = []
        for i in range(2):
            h, k = 2 * p + i, (2 * p + i + 2) % 4
            mine = keep[64 * h : 64 * (h + 1), :]
            theirs = got[64 * k : 64 * (k + 1), :].astype(F32)
            pieces.append(mine * f0[h : h + 1, :] + theirs * f1[h : h + 1, :])
        attended = jnp.transpose(jnp.concatenate(pieces, axis=0)).astype(BF)
        for j in range(NX):
            outs[p, :, lax.rem(x - j + NX, NX)] = w[:, j, 32:64, :]
        result = result + lax.dot_general(
            attended, outs[p].reshape(1024, 128), (((1,), (1,)), ((), ())),
            preferred_element_type=F32,
        )
    scratch[...] = result
    y = where[2]
    for j, out in enumerate((part_ref, p1_ref, p2_ref, p3_ref)):
        to = lax.rem(y + j, NY)
        out[...] = scratch[pl.ds(pl.multiple_of(to * 32, 32), 32), :].astype(BF)


def finish(part, p1, p2, p3, gain, out):
    summed = part[...].astype(F32)
    for other in (p1, p2, p3):
        summed = summed + other[...].astype(F32)
    wide = summed.astype(BF).astype(F32)
    mean = jnp.mean(wide * wide, axis=1, keepdims=True)
    out[...] = (wide * lax.rsqrt(mean + EPS) * gain[...]).astype(BF)


def flat(z, x, y, c):
    return ((z * NX + x) * NY + y) * NC + c


def ring(j):
    return [(i, (i + j) % NY) for i in range(NY)]


def shift_pairs(stage, j):
    pairs = []
    for z in range(NZ):
        for x in range(NX):
            for y in range(NY):
                for c in range(NC):
                    along_x = (c == 0) == (stage == 2)
                    to = flat(z, (x + j) % NX, y, c) if along_x else flat(z, x, (y + j) % NY, c)
                    pairs.append((flat(z, x, y, c), to))
    return pairs


def layer(
    tokens, doc_ids, down_query, down_key, down_rotary, query_gain, key_gain,
    up_query, up_key, up_value, output_weight, out_gain,
):
    z = lax.axis_index("z")
    x = lax.axis_index("x")
    y = lax.axis_index("y")
    c = lax.axis_index("c")
    sp = z * NX + x
    here = jnp.stack([z, x, y, c, sp * 256]).astype(jnp.int32)
    swap = [(0, 1), (1, 0)]

    sources = (down_query, down_key, down_rotary)
    message = call(
        pack, jax.ShapeDtypeStruct((NZ, 40, 128), BF), 1, 3, any_from=0,
        scratch=[VMEM((128, 128), F32)]
        + [VMEM(a.shape, a.dtype) for a in sources]
        + [pltpu.SemaphoreType.DMA((3,))],
    )(here, *(pltpu.with_memory_space_constraint(a, pltpu.HBM) for a in sources))
    gathered = lax.all_to_all(message, "z", 0, 0)
    gathered = [gathered] + [lax.ppermute(gathered, "x", ring(j)) for j in range(1, NX)]

    rows = [tokens] + [lax.ppermute(tokens, "y", ring(j)) for j in range(1, NY)]

    later = call(pack_later, jax.ShapeDtypeStruct((64, 128), BF), 0, 5)(
        up_query, up_key, up_value, doc_ids.reshape(2, 128), output_weight.T
    )
    later = [later] + [lax.ppermute(later, "x", ring(j)) for j in range(1, NX)]
    later = jnp.broadcast_to(jnp.stack(later)[None], (NZ, NX, 64, 128))

    q_part, k_part = call(
        project,
        (jax.ShapeDtypeStruct((64, 128), BF), jax.ShapeDtypeStruct((NZ, 72, 128), BF)),
        1, 8, scratch=[VMEM((128, 1024), BF), VMEM((NX, NZ, 40, 128), BF)],
    )(here, *rows, *gathered)

    stage1 = lax.all_to_all(k_part, "z", 0, 0)
    stage2 = [lax.ppermute(stage1, AXES, shift_pairs(2, j)) for j in range(1, 4)]
    held = jnp.stack([stage1] + stage2)
    stage3 = [lax.ppermute(held, AXES, shift_pairs(3, j)) for j in range(1, 4)]

    up_own = lax.all_to_all(later, "z", 0, 0)
    up_other = lax.ppermute(up_own, "c", swap)
    q_all = [q_part] + [lax.ppermute(q_part, "y", ring(j)) for j in range(1, NY)]
    q_other = lax.ppermute(jnp.stack(q_all), "c", swap)
    queries, uk, uv, key_docs, gains, query_docs = call(
        make_queries,
        (
            jax.ShapeDtypeStruct((4, 256, 256), BF),
            jax.ShapeDtypeStruct((256, 256), BF),
            jax.ShapeDtypeStruct((256, 256), BF),
            jax.ShapeDtypeStruct((NS, 128), F32),
            jax.ShapeDtypeStruct((256, 128), F32),
            jax.ShapeDtypeStruct((2, 128), F32),
        ),
        1, 10, scratch=[VMEM((256, 256), F32), VMEM((2, NZ, NX, 32, 128), BF)],
    )(
        here, *q_all, q_other, up_own, up_other, query_gain.reshape(2, 128),
        key_gain.reshape(2, 128), doc_ids.reshape(2, 128),
    )

    keep, send, ml = call(
        attend,
        (
            jax.ShapeDtypeStruct((256, 128), F32),
            jax.ShapeDtypeStruct((256, 128), BF),
            jax.ShapeDtypeStruct((8, 256), F32),
        ),
        2, 10, room=34,
        scratch=[
            VMEM((4, 4, NZ, 72, 128), BF),
            VMEM((16, 4, 256, 256), F32),
            VMEM((16, 256, 256), BF),
            VMEM((4, 8, 256), F32),
            VMEM((4, 8, 256), F32),
            VMEM((256, 256), F32),
        ],
    )(here, doc_ids, queries, uk, uv, key_docs, gains, query_docs, held, *stage3)

    got = lax.ppermute(send, "c", swap)
    ml_got = lax.ppermute(ml, "c", swap)
    *parts, log_sums = call(
        combine,
        (jax.ShapeDtypeStruct((32, 1024), BF),) * NY + (jax.ShapeDtypeStruct((2, 256), F32),),
        1, 6, scratch=[VMEM((128, 1024), F32), VMEM((2, NZ, NX, 32, 128), BF)],
    )(here, keep, got, ml, ml_got, up_own, up_other)
    parts[1:] = [lax.ppermute(parts[j], "y", ring(j)) for j in range(1, NY)]
    mixed = call(finish, jax.ShapeDtypeStruct((32, 1024), BF), 0, 5)(
        *parts, out_gain.reshape(1, 1024)
    )
    log_sums = log_sums.reshape(2, 2, 4, 32).transpose(2, 1, 3, 0).reshape(256, 2)
    return mixed, log_sums


def solution(mesh):
    finer = Mesh(mesh.devices.reshape(NZ, NX, NY, NC), AXES)
    return jax.shard_map(
        layer,
        mesh=finer,
        in_specs=(
            P(AXES, None), P(SP), P(SP, None), P(SP, None), P(SP, None), P(), P(),
            P(SP, TP), P(SP, TP), P(SP, TP), P(TP, SP), P(),
        ),
        out_specs=(P(AXES, None), P(SP, TP)),
        check_vma=False,
    )
```

```python
import math

import jax
import jax.numpy as jnp
from jax import lax
from jax.experimental import pallas as pl
from jax.experimental.pallas import tpu as pltpu
from jax.sharding import Mesh
from jax.sharding import PartitionSpec as P


NOPE = 64
ROPE = 32
NZ, NX, NY, NC = 8, 4, 4, 2
NS = NZ * NX
AXES = ("z", "x", "y", "c")
SP = ("z", "x")
TP = ("y", "c")
NEG_BIG = -1e30
FLOOR = -1e20
THETA = 10000.0
EPS = 1e-06
LN2 = math.log(2.0)
SCALE2 = 1.0 / math.sqrt(NOPE + ROPE) / LN2
BF = jnp.bfloat16
F32 = jnp.float32


VMEM = pltpu.VMEM
SMEM_SPEC = pl.BlockSpec(memory_space=pltpu.SMEM)
VMEM_SPEC = pl.BlockSpec(memory_space=pltpu.VMEM)
ANY_SPEC = pl.BlockSpec(memory_space=pltpu.HBM)


def call(body, outs, n_smem, n_in, scratch=(), any_from=None, cost=None, room=16):
    specs = [SMEM_SPEC] * n_smem
    for i in range(n_in):
        specs.append(ANY_SPEC if any_from is not None and i >= any_from else VMEM_SPEC)
    single = not isinstance(outs, tuple)
    return pl.pallas_call(
        body,
        out_shape=outs,
        in_specs=specs,
        out_specs=VMEM_SPEC if single else tuple(VMEM_SPEC for _ in outs),
        scratch_shapes=list(scratch),
        compiler_params=pltpu.CompilerParams(vmem_limit_bytes=room * 1024 * 1024),
        cost_estimate=cost,
    )


def lanes(shape):
    return lax.broadcasted_iota(jnp.int32, shape, len(shape) - 1)


def column(row):
    return jnp.transpose(jnp.broadcast_to(row, (128, 128)))


def frequency(index):
    value = jnp.ones(index.shape, F32)
    for bit in range(4):
        factor = THETA ** (-(1 << bit) / 16)
        value = value * jnp.where((index // (1 << bit)) % 2 == 1, factor, 1.0)
    return value


def pack(where, dq_in, dk_in, dr_in, out, flipped, dq, dk, dr, sems):
    copies = [
        pltpu.make_async_copy(source, place, sems.at[i])
        for i, (source, place) in enumerate(((dq_in, dq), (dk_in, dk), (dr_in, dr)))
    ]
    for copy in copies:
        copy.start()
    for copy in copies:
        copy.wait()
    y = where[2]

    def chosen(ref):
        block = ref[:, 0:64]
        for k in range(1, NY):
            block = jnp.where(y == k, ref[:, 64 * k : 64 * (k + 1)], block)
        return block

    block = jnp.concatenate([chosen(dq), chosen(dk)], axis=1)
    rope = dr[...].astype(F32)
    rope = jnp.concatenate([rope, jnp.zeros((32, 96), F32)], axis=1)
    flipped[...] = jnp.transpose(jnp.concatenate([rope] * 4, axis=0))
    turned = jnp.concatenate([flipped[pl.ds(4 * y, 4), :], flipped[pl.ds(16 + 4 * y, 4), :]], axis=0)
    turned = turned.astype(BF)
    for z in range(NZ):
        out[z, 0:32, :] = block
        out[z, 32:40, :] = turned


def pack_later(up_query, up_key, up_value, docs_ref, out_t, out):
    src = lax.broadcasted_iota(jnp.int32, (192, 256), 0)
    lane = lanes((192, 256))
    plain = 96 * (lane // 64) + lane % 64
    turn = lane - 128
    rope = 64 + 96 * (turn // 32) + 16 * ((turn // 4) % 2) + 4 * ((turn % 32) // 8) + turn % 4
    chosen = jnp.where(lane < 128, plain, jnp.where(lane < 192, rope, -1))
    pick = jnp.where(src == chosen, 1.0, 0.0).astype(BF)
    sorted_query = jnp.dot(up_query[...], pick, preferred_element_type=F32)
    out[0:8, :] = sorted_query[:, 0:128].astype(BF)
    out[8:16, :] = up_key[...]
    out[16:24, :] = up_value[...]
    mixed = sorted_query[:, 128:256]
    docs = docs_ref[...].astype(F32)
    row = lax.broadcasted_iota(jnp.int32, (8, 128), 0)
    at = lanes((8, 128))
    for r in range(8):
        line = docs[r // 4 : r // 4 + 1, :]
        moved = pltpu.roll(jnp.broadcast_to(line, (8, 128)), (64 - 32 * (r % 4)) % 128, 1)
        mixed = jnp.where((row == r) & (at // 32 == 2), moved, mixed)
    out[24:32, :] = mixed.astype(BF)
    out[32:64, :] = out_t[...]


def project(where, t0, t1, t2, t3, g0, g1, g2, g3, q_ref, k_ref, tok, gathered):
    x = where[1]
    y = where[2]
    for j, part in enumerate((t0, t1, t2, t3)):
        at = lax.rem(y - j + NY, NY)
        tok[pl.ds(pl.multiple_of(at * 32, 32), 32), :] = part[...]
    for j, part in enumerate((g0, g1, g2, g3)):
        gathered[lax.rem(x - j + NX, NX)] = part[...]
    rows = tok[...]
    weights = jnp.concatenate(
        [gathered[k, z, 0:32, :] for z in range(NZ) for k in range(NX)], axis=0
    )
    both = jnp.dot(rows, weights, preferred_element_type=F32)
    turned = jnp.transpose(both).astype(BF)
    q_ref[...] = turned[0:64, :]
    for t in range(NZ):
        k_ref[t, 0:64, :] = turned[64:128, :]
    group = lanes((8, 128)) // 32
    pieces = []
    for z in range(NZ):
        piece = gathered[0, z, 32:40, :].astype(F32)
        for g in range(1, 4):
            piece = jnp.where(group == g, gathered[g, z, 32:40, :].astype(F32), piece)
        pieces.append(piece)
    rope = jnp.concatenate(pieces, axis=1)
    rope = jnp.concatenate([rope, jnp.zeros_like(rope)], axis=0).astype(BF)
    raw = lax.dot_general(rope, rows, (((1,), (1,)), ((), ())), preferred_element_type=F32)
    raw = raw[0:8, :].astype(BF).astype(F32)
    at = lanes((8, 128))
    row = lax.broadcasted_iota(jnp.int32, (8, 128), 0)
    pos = where[4] + 64 * (at // 32) + 32 * where[3] + at % 32
    angle = pos.astype(F32) * frequency(4 * y + row % 4)
    sine = jnp.sin(angle)
    rotated = raw * jnp.cos(angle) + pltpu.roll(raw, 4, 0) * jnp.where(row < 4, -sine, sine)
    rotated = rotated.astype(BF)
    for t in range(NZ):
        k_ref[t, 64:72, :] = rotated


def make_queries(
    where, q0, q1, q2, q3, q_other, up_own, up_other, gain, key_gain, docs_in,
    out, uk_ref, uv_ref, docs_ref, col_ref, row_ref, latents, ups,
):
    x, y, c = where[1], where[2], where[3]
    for j, part in enumerate((q0, q1, q2, q3)):
        own, other = part[...].astype(F32), q_other[j].astype(F32)
        rows = pl.ds(pl.multiple_of(lax.rem(y - j + NY, NY) * 64, 64), 64)
        latents[rows, 0:128] = jnp.where(c == 0, own, other)
        latents[rows, 128:256] = jnp.where(c == 0, other, own)
    raw = latents[...]
    mean = jnp.sum(raw * raw, axis=0, keepdims=True) * (1.0 / 256.0)
    inverse = lax.rsqrt(mean + EPS)
    gains = jnp.concatenate([column(gain[0:1, :]), column(gain[1:2, :])], axis=0)
    gains = jnp.concatenate([gains, gains], axis=1)
    tokens_docs = docs_in[...].astype(F32)
    at = lanes((1, 128))
    for i in range(2):
        col_ref[128 * i : 128 * (i + 1), :] = column(key_gain[i : i + 1, :])
        ordered = jnp.zeros((1, 128), F32)
        for k in range(NY):
            line = tokens_docs[k // 2 : k // 2 + 1, :]
            moved = pltpu.roll(line, (32 * k - 64 * (k % 2) - 32 * i) % 128, 1)
            ordered = jnp.where(at // 32 == k, moved, ordered)
        row_ref[i : i + 1, :] = ordered
    latent = (raw * inverse * gains).astype(BF)
    tok = lanes((64, 256))
    row = lax.broadcasted_iota(jnp.int32, (64, 256), 0)
    pos = where[4] + 64 * ((tok % 128) // 32) + 32 * (tok // 128) + tok % 32
    angle = pos.astype(F32) * frequency(4 * ((row % 32) // 8) + row % 4)
    is_low = (row // 4) % 2 == 0
    cos = jnp.cos(angle)
    sine = jnp.sin(angle)
    low_sin = jnp.where(is_low, -sine, 0.0)
    high_sin = jnp.where(is_low, 0.0, sine)
    for p, up in enumerate((up_own, up_other)):
        for j in range(NX):
            ups[p, :, lax.rem(x - j + NX, NX)] = up[:, j, 0:32, :]
        wide = ups[p].reshape(NS, 32, 128).astype(F32)
        own = slice(128 * p, 128 * (p + 1))
        plain_w = jnp.transpose(wide[:, 0:8, :].reshape(256, 128)).astype(BF)
        rope_w = jnp.transpose(wide[:, 24:32, :].reshape(256, 128))[0:64, :].astype(BF)
        uk_ref[:, own] = wide[:, 8:16, :].reshape(256, 128).astype(BF)
        uv_ref[own, :] = jnp.transpose(wide[:, 16:24, :].reshape(256, 128)).astype(BF)
        plain = (jnp.dot(plain_w, latent, preferred_element_type=F32) * SCALE2).astype(BF)
        raw = jnp.dot(rope_w, latent, preferred_element_type=F32) * SCALE2
        rope = raw * cos + pltpu.roll(raw, 60, 0) * low_sin + pltpu.roll(raw, 4, 0) * high_sin
        rope = rope.astype(BF)
        for i in range(2):
            h = 2 * p + i
            out[h] = jnp.zeros((256, 256), BF)
            out[h, 64 * i : 64 * (i + 1), :] = plain[64 * i : 64 * (i + 1), :]
            out[h, 128:160, :] = rope[32 * i : 32 * (i + 1), :]
    docs = ups[0].reshape(NS, 32, 128)[:, 24:32, :].astype(F32)
    at = lanes((NS, 128))
    spread = jnp.zeros((NS, 128), F32)
    for k in range(NY):
        piece = jnp.where(c == 0, docs[:, 2 * k, :], docs[:, 2 * k + 1, :])
        spread = jnp.where(at // 32 == k, pltpu.roll(piece, (32 * k + 64) % 128, 1), spread)
    docs_ref[...] = spread


def attend(
    where, ids, q_ref, uk, uv, key_docs, gains, query_docs, b0, b1, b2, b3,
    keep_ref, send_ref, ml_ref, kb, s_buf, v_buf, mx, total, acc,
):
    x0, y0, c = where[1], where[2], where[3]
    docs = key_docs[...]
    at = lanes((NS, 128))
    before = (at == 127) & (docs < ids[0].astype(F32))
    behind = (at == 0) & (docs > ids[255].astype(F32))
    low = jnp.sum(before.astype(jnp.int32))
    high = NS - 1 - jnp.sum(behind.astype(jnp.int32))
    count = (high - low) // 2 + 1
    begin = jnp.minimum(low, NS - 2 * count)

    def fetch(z, carry):
        for j, part in enumerate((b0, b1, b2, b3)):
            for k in range(4):
                kb[j, k, z] = part[k, z]
        return carry

    lax.fori_loop(begin // 4, (begin + 2 * count - 1) // 4 + 1, fetch, 0)
    mx[...] = jnp.full(mx.shape, NEG_BIG, F32)
    total[...] = jnp.zeros(total.shape, F32)
    acc[...] = jnp.zeros(acc.shape, F32)
    wanted = jnp.concatenate([query_docs[0:1, :], query_docs[1:2, :]], axis=1)

    def scores(tile, carry):
        latents, ropes, same = [], [], []
        for half in range(2):
            block = begin + 2 * tile + half
            z, x = block // NX, lax.rem(block, NX)
            jx = lax.rem(x0 - x + NX, NX)
            parts, turned = [], []
            for y in range(NY):
                jy = lax.rem(y0 - y + NY, NY)
                third = jnp.where(c == 0, jy, jx)
                second = jnp.where(c == 0, jx, jy)
                slab = kb[third, second, z].astype(F32)
                parts.append(slab[0:64, :])
                turned.append(slab[64:72, :])
            squares = parts[0] * parts[0]
            for part in parts[1:]:
                squares = squares + part * part
            mean = jnp.sum(squares, axis=0, keepdims=True) * (1.0 / 256.0)
            inverse = lax.rsqrt(mean + EPS)
            latents.append(jnp.concatenate(parts, axis=0) * inverse * gains[...])
            ropes.append(jnp.concatenate(turned, axis=0))
            docs_col = column(key_docs[pl.ds(block, 1), :])
            same.append(jnp.concatenate([docs_col, docs_col], axis=1) == wanted)
        latent = jnp.concatenate(latents, axis=1)
        v_buf[tile] = jnp.dot(uv[...], latent.astype(BF), preferred_element_type=F32).astype(BF)
        turned = jnp.transpose(latent).astype(BF)
        rope = jnp.concatenate(ropes, axis=1)
        rope = jnp.concatenate([rope, jnp.zeros((96, 256), F32)], axis=0)
        rope = jnp.transpose(rope).astype(BF)
        keys = jnp.dot(turned, uk[...], preferred_element_type=F32).astype(BF)
        for h in range(4):
            p = h // 2
            stack = jnp.concatenate([keys[:, 128 * p : 128 * (p + 1)], rope], axis=1)
            got = jnp.dot(stack, q_ref[h], preferred_element_type=F32)
            got = jnp.concatenate(
                [
                    jnp.where(same[0], got[0:128, :], NEG_BIG),
                    jnp.where(same[1], got[128:256, :], NEG_BIG),
                ],
                axis=0,
            )
            s_buf[tile, h] = got
            mx[h] = jnp.maximum(mx[h], jnp.max(got.reshape(32, 8, 256), axis=0))
        return carry

    lax.fori_loop(0, count, scores, 0)
    tops = []
    for h in range(4):
        top = jnp.maximum(jnp.max(mx[h], axis=0, keepdims=True), FLOOR)
        mx[h] = jnp.broadcast_to(top, (8, 256))
        tops.append(top)

    def weigh(tile, carry):
        for h in range(4):
            own = slice(64 * h, 64 * (h + 1))
            weights = jnp.exp2(s_buf[tile, h].reshape(32, 8, 256) - mx[h][None])
            total[h] = total[h] + jnp.sum(weights, axis=0)
            weights = weights.reshape(256, 256).astype(BF)
            acc[own, :] = acc[own, :] + jnp.dot(
                v_buf[tile, own, :], weights, preferred_element_type=F32
            )
        return carry

    lax.fori_loop(0, count, weigh, 0)
    for h in range(4):
        ml_ref[h : h + 1, :] = tops[h]
        ml_ref[4 + h : 5 + h, :] = jnp.sum(total[h], axis=0, keepdims=True)
    left, right = acc[:, 0:128], acc[:, 128:256]
    keep_ref[...] = jnp.where(c == 0, left, right)
    send_ref[...] = jnp.where(c == 0, right, left).astype(BF)


def combine(
    where, keep, got, ml_own, ml_got, w_own, w_other, part_ref, p1_ref, p2_ref, p3_ref, lse_ref,
    scratch, outs,
):
    x, c = where[1], where[3]
    m0, l0 = ml_own[0:4, :], ml_own[4:8, :]
    m1 = jnp.concatenate([ml_got[2:4, :], ml_got[0:2, :]], axis=0)
    l1 = jnp.concatenate([ml_got[6:8, :], ml_got[4:6, :]], axis=0)
    top = jnp.maximum(m0, m1)
    e0 = jnp.exp2(m0 - top)
    e1 = jnp.exp2(m1 - top)
    weight_sum = l0 * e0 + l1 * e1
    lse_ref[...] = ((top + jnp.log2(weight_sum)) * LN2)[0:2, :]
    f0 = e0 / weight_sum
    f1 = e1 / weight_sum
    f0 = jnp.where(c == 0, f0[:, 0:128], f0[:, 128:256])
    f1 = jnp.where(c == 0, f1[:, 0:128], f1[:, 128:256])
    result = jnp.zeros((128, 1024), F32)
    for p, w in enumerate((w_own, w_other)):
        pieces = []
        for i in range(2):
            h, k = 2 * p + i, (2 * p + i + 2) % 4
            mine = keep[64 * h : 64 * (h + 1), :]
            theirs = got[64 * k : 64 * (k + 1), :].astype(F32)
            pieces.append(mine * f0[h : h + 1, :] + theirs * f1[h : h + 1, :])
        attended = jnp.transpose(jnp.concatenate(pieces, axis=0)).astype(BF)
        for j in range(NX):
            outs[p, :, lax.rem(x - j + NX, NX)] = w[:, j, 32:64, :]
        result = result + lax.dot_general(
            attended, outs[p].reshape(1024, 128), (((1,), (1,)), ((), ())),
            preferred_element_type=F32,
        )
    scratch[...] = result
    y = where[2]
    for j, out in enumerate((part_ref, p1_ref, p2_ref, p3_ref)):
        to = lax.rem(y + j, NY)
        out[...] = scratch[pl.ds(pl.multiple_of(to * 32, 32), 32), :].astype(BF)


def finish(part, p1, p2, p3, gain, out):
    summed = part[...].astype(F32)
    for other in (p1, p2, p3):
        summed = summed + other[...].astype(F32)
    wide = summed.astype(BF).astype(F32)
    mean = jnp.mean(wide * wide, axis=1, keepdims=True)
    out[...] = (wide * lax.rsqrt(mean + EPS) * gain[...]).astype(BF)


def flat(z, x, y, c):
    return ((z * NX + x) * NY + y) * NC + c


def ring(j):
    return [(i, (i + j) % NY) for i in range(NY)]


def shift_pairs(stage, j):
    pairs = []
    for z in range(NZ):
        for x in range(NX):
            for y in range(NY):
                for c in range(NC):
                    along_x = (c == 0) == (stage == 2)
                    to = flat(z, (x + j) % NX, y, c) if along_x else flat(z, x, (y + j) % NY, c)
                    pairs.append((flat(z, x, y, c), to))
    return pairs


def layer(
    tokens, doc_ids, down_query, down_key, down_rotary, query_gain, key_gain,
    up_query, up_key, up_value, output_weight, out_gain,
):
    z = lax.axis_index("z")
    x = lax.axis_index("x")
    y = lax.axis_index("y")
    c = lax.axis_index("c")
    sp = z * NX + x
    here = jnp.stack([z, x, y, c, sp * 256]).astype(jnp.int32)
    swap = [(0, 1), (1, 0)]

    sources = (down_query, down_key, down_rotary)
    message = call(
        pack, jax.ShapeDtypeStruct((NZ, 40, 128), BF), 1, 3, any_from=0,
        scratch=[VMEM((128, 128), F32)]
        + [VMEM(a.shape, a.dtype) for a in sources]
        + [pltpu.SemaphoreType.DMA((3,))],
    )(here, *(pltpu.with_memory_space_constraint(a, pltpu.HBM) for a in sources))
    gathered = lax.all_to_all(message, "z", 0, 0)
    gathered = [gathered] + [lax.ppermute(gathered, "x", ring(j)) for j in range(1, NX)]

    rows = [tokens] + [lax.ppermute(tokens, "y", ring(j)) for j in range(1, NY)]

    later = call(pack_later, jax.ShapeDtypeStruct((64, 128), BF), 0, 5)(
        up_query, up_key, up_value, doc_ids.reshape(2, 128), output_weight.T
    )
    later = [later] + [lax.ppermute(later, "x", ring(j)) for j in range(1, NX)]
    later = jnp.broadcast_to(jnp.stack(later)[None], (NZ, NX, 64, 128))

    q_part, k_part = call(
        project,
        (jax.ShapeDtypeStruct((64, 128), BF), jax.ShapeDtypeStruct((NZ, 72, 128), BF)),
        1, 8, scratch=[VMEM((128, 1024), BF), VMEM((NX, NZ, 40, 128), BF)],
    )(here, *rows, *gathered)

    stage1 = lax.all_to_all(k_part, "z", 0, 0)
    stage2 = [lax.ppermute(stage1, AXES, shift_pairs(2, j)) for j in range(1, 4)]
    held = jnp.stack([stage1] + stage2)
    stage3 = [lax.ppermute(held, AXES, shift_pairs(3, j)) for j in range(1, 4)]

    up_own = lax.all_to_all(later, "z", 0, 0)
    up_other = lax.ppermute(up_own, "c", swap)
    q_all = [q_part] + [lax.ppermute(q_part, "y", ring(j)) for j in range(1, NY)]
    q_other = lax.ppermute(jnp.stack(q_all), "c", swap)
    queries, uk, uv, key_docs, gains, query_docs = call(
        make_queries,
        (
            jax.ShapeDtypeStruct((4, 256, 256), BF),
            jax.ShapeDtypeStruct((256, 256), BF),
            jax.ShapeDtypeStruct((256, 256), BF),
            jax.ShapeDtypeStruct((NS, 128), F32),
            jax.ShapeDtypeStruct((256, 128), F32),
            jax.ShapeDtypeStruct((2, 128), F32),
        ),
        1, 10, scratch=[VMEM((256, 256), F32), VMEM((2, NZ, NX, 32, 128), BF)],
    )(
        here, *q_all, q_other, up_own, up_other, query_gain.reshape(2, 128),
        key_gain.reshape(2, 128), doc_ids.reshape(2, 128),
    )

    keep, send, ml = call(
        attend,
        (
            jax.ShapeDtypeStruct((256, 128), F32),
            jax.ShapeDtypeStruct((256, 128), BF),
            jax.ShapeDtypeStruct((8, 256), F32),
        ),
        2, 10, room=34,
        scratch=[
            VMEM((4, 4, NZ, 72, 128), BF),
            VMEM((16, 4, 256, 256), F32),
            VMEM((16, 256, 256), BF),
            VMEM((4, 8, 256), F32),
            VMEM((4, 8, 256), F32),
            VMEM((256, 256), F32),
        ],
    )(here, doc_ids, queries, uk, uv, key_docs, gains, query_docs, held, *stage3)

    got = lax.ppermute(send, "c", swap)
    ml_got = lax.ppermute(ml, "c", swap)
    *parts, log_sums = call(
        combine,
        (jax.ShapeDtypeStruct((32, 1024), BF),) * NY + (jax.ShapeDtypeStruct((2, 256), F32),),
        1, 6, scratch=[VMEM((128, 1024), F32), VMEM((2, NZ, NX, 32, 128), BF)],
    )(here, keep, got, ml, ml_got, up_own, up_other)
    parts[1:] = [lax.ppermute(parts[j], "y", ring(j)) for j in range(1, NY)]
    mixed = call(finish, jax.ShapeDtypeStruct((32, 1024), BF), 0, 5)(
        *parts, out_gain.reshape(1, 1024)
    )
    log_sums = log_sums.reshape(2, 2, 4, 32).transpose(2, 1, 3, 0).reshape(256, 2)
    return mixed, log_sums


def solution(mesh):
    finer = Mesh(mesh.devices.reshape(NZ, NX, NY, NC), AXES)
    return jax.shard_map(
        layer,
        mesh=finer,
        in_specs=(
            P(AXES, None), P(SP), P(SP, None), P(SP, None), P(SP, None), P(), P(),
            P(SP, TP), P(SP, TP), P(SP, TP), P(TP, SP), P(),
        ),
        out_specs=(P(AXES, None), P(SP, TP)),
        check_vma=False,
    )
```

```python
import math

import jax
import jax.numpy as jnp
from jax import lax
from jax.experimental import pallas as pl
from jax.experimental.pallas import tpu as pltpu
from jax.sharding import Mesh
from jax.sharding import PartitionSpec as P


NOPE = 64
ROPE = 32
NZ, NX, NY, NC = 8, 4, 4, 2
NS = NZ * NX
AXES = ("z", "x", "y", "c")
SP = ("z", "x")
TP = ("y", "c")
NEG_BIG = -1e30
FLOOR = -1e20
THETA = 10000.0
EPS = 1e-06
LN2 = math.log(2.0)
SCALE2 = 1.0 / math.sqrt(NOPE + ROPE) / LN2
BF = jnp.bfloat16
F32 = jnp.float32


VMEM = pltpu.VMEM
SMEM_SPEC = pl.BlockSpec(memory_space=pltpu.SMEM)
VMEM_SPEC = pl.BlockSpec(memory_space=pltpu.VMEM)
ANY_SPEC = pl.BlockSpec(memory_space=pltpu.HBM)


def call(body, outs, n_smem, n_in, scratch=(), any_from=None, cost=None, room=16):
    specs = [SMEM_SPEC] * n_smem
    for i in range(n_in):
        specs.append(ANY_SPEC if any_from is not None and i >= any_from else VMEM_SPEC)
    single = not isinstance(outs, tuple)
    return pl.pallas_call(
        body,
        out_shape=outs,
        in_specs=specs,
        out_specs=VMEM_SPEC if single else tuple(VMEM_SPEC for _ in outs),
        scratch_shapes=list(scratch),
        compiler_params=pltpu.CompilerParams(vmem_limit_bytes=room * 1024 * 1024),
        cost_estimate=cost,
    )


def lanes(shape):
    return lax.broadcasted_iota(jnp.int32, shape, len(shape) - 1)


def column(row):
    return jnp.transpose(jnp.broadcast_to(row, (128, 128)))


def frequency(index):
    value = jnp.ones(index.shape, F32)
    for bit in range(4):
        factor = THETA ** (-(1 << bit) / 16)
        value = value * jnp.where((index // (1 << bit)) % 2 == 1, factor, 1.0)
    return value


def pack(where, dq_in, dk_in, dr_in, out, flipped, dq, dk, dr, sems):
    copies = [
        pltpu.make_async_copy(source, place, sems.at[i])
        for i, (source, place) in enumerate(((dq_in, dq), (dk_in, dk), (dr_in, dr)))
    ]
    for copy in copies:
        copy.start()
    for copy in copies:
        copy.wait()
    y = where[2]

    def chosen(ref):
        block = ref[:, 0:64]
        for k in range(1, NY):
            block = jnp.where(y == k, ref[:, 64 * k : 64 * (k + 1)], block)
        return block

    block = jnp.concatenate([chosen(dq), chosen(dk)], axis=1)
    rope = dr[...].astype(F32)
    rope = jnp.concatenate([rope, jnp.zeros((32, 96), F32)], axis=1)
    flipped[...] = jnp.transpose(jnp.concatenate([rope] * 4, axis=0))
    turned = jnp.concatenate([flipped[pl.ds(4 * y, 4), :], flipped[pl.ds(16 + 4 * y, 4), :]], axis=0)
    turned = turned.astype(BF)
    for z in range(NZ):
        out[z, 0:32, :] = block
        out[z, 32:40, :] = turned


def pack_later(up_query, up_key, up_value, docs_ref, out_t, out):
    src = lax.broadcasted_iota(jnp.int32, (192, 256), 0)
    lane = lanes((192, 256))
    plain = 96 * (lane // 64) + lane % 64
    turn = lane - 128
    rope = 64 + 96 * (turn // 32) + 16 * ((turn // 4) % 2) + 4 * ((turn % 32) // 8) + turn % 4
    chosen = jnp.where(lane < 128, plain, jnp.where(lane < 192, rope, -1))
    pick = jnp.where(src == chosen, 1.0, 0.0).astype(BF)
    sorted_query = jnp.dot(up_query[...], pick, preferred_element_type=F32)
    out[0:8, :] = sorted_query[:, 0:128].astype(BF)
    out[8:16, :] = up_key[...]
    out[16:24, :] = up_value[...]
    mixed = sorted_query[:, 128:256]
    docs = docs_ref[...].astype(F32)
    row = lax.broadcasted_iota(jnp.int32, (8, 128), 0)
    at = lanes((8, 128))
    for r in range(8):
        line = docs[r // 4 : r // 4 + 1, :]
        moved = pltpu.roll(jnp.broadcast_to(line, (8, 128)), (64 - 32 * (r % 4)) % 128, 1)
        mixed = jnp.where((row == r) & (at // 32 == 2), moved, mixed)
    out[24:32, :] = mixed.astype(BF)
    out[32:64, :] = out_t[...]


def project(where, t0, t1, t2, t3, g0, g1, g2, g3, q_ref, k_ref, tok, gathered):
    x = where[1]
    y = where[2]
    for j, part in enumerate((t0, t1, t2, t3)):
        at = lax.rem(y - j + NY, NY)
        tok[pl.ds(pl.multiple_of(at * 32, 32), 32), :] = part[...]
    for j, part in enumerate((g0, g1, g2, g3)):
        gathered[lax.rem(x - j + NX, NX)] = part[...]
    rows = tok[...]
    weights = jnp.concatenate(
        [gathered[k, z, 0:32, :] for z in range(NZ) for k in range(NX)], axis=0
    )
    both = jnp.dot(rows, weights, preferred_element_type=F32)
    turned = jnp.transpose(both).astype(BF)
    q_ref[...] = turned[0:64, :]
    for t in range(NZ):
        k_ref[t, 0:64, :] = turned[64:128, :]
    group = lanes((8, 128)) // 32
    pieces = []
    for z in range(NZ):
        piece = gathered[0, z, 32:40, :].astype(F32)
        for g in range(1, 4):
            piece = jnp.where(group == g, gathered[g, z, 32:40, :].astype(F32), piece)
        pieces.append(piece)
    rope = jnp.concatenate(pieces, axis=1)
    rope = jnp.concatenate([rope, jnp.zeros_like(rope)], axis=0).astype(BF)
    raw = lax.dot_general(rope, rows, (((1,), (1,)), ((), ())), preferred_element_type=F32)
    raw = raw[0:8, :].astype(BF).astype(F32)
    at = lanes((8, 128))
    row = lax.broadcasted_iota(jnp.int32, (8, 128), 0)
    pos = where[4] + 64 * (at // 32) + 32 * where[3] + at % 32
    angle = pos.astype(F32) * frequency(4 * y + row % 4)
    sine = jnp.sin(angle)
    rotated = raw * jnp.cos(angle) + pltpu.roll(raw, 4, 0) * jnp.where(row < 4, -sine, sine)
    rotated = rotated.astype(BF)
    for t in range(NZ):
        k_ref[t, 64:72, :] = rotated


def make_queries(
    where, q0, q1, q2, q3, up_own, up_other, gain, key_gain, docs_in,
    out, uk_ref, uv_ref, docs_ref, col_ref, row_ref, latents, ups,
):
    x, y, c = where[1], where[2], where[3]
    for j, part in enumerate((q0, q1, q2, q3)):
        own, other = part[0].astype(F32), part[1].astype(F32)
        rows = pl.ds(pl.multiple_of(lax.rem(y - j + NY, NY) * 64, 64), 64)
        latents[rows, 0:128] = jnp.where(c == 0, own, other)
        latents[rows, 128:256] = jnp.where(c == 0, other, own)
    raw = latents[...]
    mean = jnp.sum(raw * raw, axis=0, keepdims=True) * (1.0 / 256.0)
    inverse = lax.rsqrt(mean + EPS)
    gains = jnp.concatenate([column(gain[0:1, :]), column(gain[1:2, :])], axis=0)
    gains = jnp.concatenate([gains, gains], axis=1)
    tokens_docs = docs_in[...].astype(F32)
    at = lanes((1, 128))
    for i in range(2):
        col_ref[128 * i : 128 * (i + 1), :] = column(key_gain[i : i + 1, :])
        ordered = jnp.zeros((1, 128), F32)
        for k in range(NY):
            line = tokens_docs[k // 2 : k // 2 + 1, :]
            moved = pltpu.roll(line, (32 * k - 64 * (k % 2) - 32 * i) % 128, 1)
            ordered = jnp.where(at // 32 == k, moved, ordered)
        row_ref[i : i + 1, :] = ordered
    latent = (raw * inverse * gains).astype(BF)
    tok = lanes((64, 256))
    row = lax.broadcasted_iota(jnp.int32, (64, 256), 0)
    pos = where[4] + 64 * ((tok % 128) // 32) + 32 * (tok // 128) + tok % 32
    angle = pos.astype(F32) * frequency(4 * ((row % 32) // 8) + row % 4)
    is_low = (row // 4) % 2 == 0
    cos = jnp.cos(angle)
    sine = jnp.sin(angle)
    low_sin = jnp.where(is_low, -sine, 0.0)
    high_sin = jnp.where(is_low, 0.0, sine)
    for p, up in enumerate((up_own, up_other)):
        for j in range(NX):
            ups[p, :, lax.rem(x - j + NX, NX)] = up[:, j, 0:32, :]
        wide = ups[p].reshape(NS, 32, 128).astype(F32)
        own = slice(128 * p, 128 * (p + 1))
        plain_w = jnp.transpose(wide[:, 0:8, :].reshape(256, 128)).astype(BF)
        rope_w = jnp.transpose(wide[:, 24:32, :].reshape(256, 128))[0:64, :].astype(BF)
        uk_ref[:, own] = wide[:, 8:16, :].reshape(256, 128).astype(BF)
        uv_ref[own, :] = jnp.transpose(wide[:, 16:24, :].reshape(256, 128)).astype(BF)
        plain = (jnp.dot(plain_w, latent, preferred_element_type=F32) * SCALE2).astype(BF)
        raw = jnp.dot(rope_w, latent, preferred_element_type=F32) * SCALE2
        rope = raw * cos + pltpu.roll(raw, 60, 0) * low_sin + pltpu.roll(raw, 4, 0) * high_sin
        rope = rope.astype(BF)
        for i in range(2):
            h = 2 * p + i
            out[h] = jnp.zeros((256, 256), BF)
            out[h, 64 * i : 64 * (i + 1), :] = plain[64 * i : 64 * (i + 1), :]
            out[h, 128:160, :] = rope[32 * i : 32 * (i + 1), :]
    docs = ups[0].reshape(NS, 32, 128)[:, 24:32, :].astype(F32)
    at = lanes((NS, 128))
    spread = jnp.zeros((NS, 128), F32)
    for k in range(NY):
        piece = jnp.where(c == 0, docs[:, 2 * k, :], docs[:, 2 * k + 1, :])
        spread = jnp.where(at // 32 == k, pltpu.roll(piece, (32 * k + 64) % 128, 1), spread)
    docs_ref[...] = spread


def attend(
    where, ids, q_ref, uk, uv, key_docs, gains, query_docs, b0, b1, b2, b3,
    keep_ref, send_ref, ml_ref, kb, s_buf, v_buf, mx, total, acc,
):
    x0, y0, c = where[1], where[2], where[3]
    docs = key_docs[...]
    at = lanes((NS, 128))
    before = (at == 127) & (docs < ids[0].astype(F32))
    behind = (at == 0) & (docs > ids[255].astype(F32))
    low = jnp.sum(before.astype(jnp.int32))
    high = NS - 1 - jnp.sum(behind.astype(jnp.int32))
    count = (high - low) // 2 + 1
    begin = jnp.minimum(low, NS - 2 * count)

    def fetch(z, carry):
        for j, part in enumerate((b0, b1, b2, b3)):
            for k in range(4):
                kb[j, k, z] = part[k, z]
        return carry

    lax.fori_loop(begin // 4, (begin + 2 * count - 1) // 4 + 1, fetch, 0)
    mx[...] = jnp.full(mx.shape, NEG_BIG, F32)
    total[...] = jnp.zeros(total.shape, F32)
    acc[...] = jnp.zeros(acc.shape, F32)
    wanted = jnp.concatenate([query_docs[0:1, :], query_docs[1:2, :]], axis=1)

    def scores(tile, carry):
        latents, ropes, same = [], [], []
        for half in range(2):
            block = begin + 2 * tile + half
            z, x = block // NX, lax.rem(block, NX)
            jx = lax.rem(x0 - x + NX, NX)
            parts, turned = [], []
            for y in range(NY):
                jy = lax.rem(y0 - y + NY, NY)
                third = jnp.where(c == 0, jy, jx)
                second = jnp.where(c == 0, jx, jy)
                slab = kb[third, second, z].astype(F32)
                parts.append(slab[0:64, :])
                turned.append(slab[64:72, :])
            squares = parts[0] * parts[0]
            for part in parts[1:]:
                squares = squares + part * part
            mean = jnp.sum(squares, axis=0, keepdims=True) * (1.0 / 256.0)
            inverse = lax.rsqrt(mean + EPS)
            latents.append(jnp.concatenate(parts, axis=0) * inverse * gains[...])
            ropes.append(jnp.concatenate(turned, axis=0))
            docs_col = column(key_docs[pl.ds(block, 1), :])
            same.append(jnp.concatenate([docs_col, docs_col], axis=1) == wanted)
        latent = jnp.concatenate(latents, axis=1)
        v_buf[tile] = jnp.dot(uv[...], latent.astype(BF), preferred_element_type=F32).astype(BF)
        turned = jnp.transpose(latent).astype(BF)
        rope = jnp.concatenate(ropes, axis=1)
        rope = jnp.concatenate([rope, jnp.zeros((96, 256), F32)], axis=0)
        rope = jnp.transpose(rope).astype(BF)
        keys = jnp.dot(turned, uk[...], preferred_element_type=F32).astype(BF)
        for h in range(4):
            p = h // 2
            stack = jnp.concatenate([keys[:, 128 * p : 128 * (p + 1)], rope], axis=1)
            got = jnp.dot(stack, q_ref[h], preferred_element_type=F32)
            got = jnp.concatenate(
                [
                    jnp.where(same[0], got[0:128, :], NEG_BIG),
                    jnp.where(same[1], got[128:256, :], NEG_BIG),
                ],
                axis=0,
            )
            s_buf[tile, h] = got
            mx[h] = jnp.maximum(mx[h], jnp.max(got.reshape(32, 8, 256), axis=0))
        return carry

    lax.fori_loop(0, count, scores, 0)
    tops = []
    for h in range(4):
        top = jnp.maximum(jnp.max(mx[h], axis=0, keepdims=True), FLOOR)
        mx[h] = jnp.broadcast_to(top, (8, 256))
        tops.append(top)

    def weigh(tile, carry):
        for h in range(4):
            own = slice(64 * h, 64 * (h + 1))
            weights = jnp.exp2(s_buf[tile, h].reshape(32, 8, 256) - mx[h][None])
            total[h] = total[h] + jnp.sum(weights, axis=0)
            weights = weights.reshape(256, 256).astype(BF)
            acc[own, :] = acc[own, :] + jnp.dot(
                v_buf[tile, own, :], weights, preferred_element_type=F32
            )
        return carry

    lax.fori_loop(0, count, weigh, 0)
    for h in range(4):
        ml_ref[h : h + 1, :] = tops[h]
        ml_ref[4 + h : 5 + h, :] = jnp.sum(total[h], axis=0, keepdims=True)
    left, right = acc[:, 0:128], acc[:, 128:256]
    keep_ref[...] = jnp.where(c == 0, left, right)
    send_ref[...] = jnp.where(c == 0, right, left).astype(BF)


def combine(
    where, keep, got, ml_own, ml_got, w_own, w_other, part_ref, p1_ref, p2_ref, p3_ref, lse_ref,
    scratch, outs,
):
    x, c = where[1], where[3]
    m0, l0 = ml_own[0:4, :], ml_own[4:8, :]
    m1 = jnp.concatenate([ml_got[2:4, :], ml_got[0:2, :]], axis=0)
    l1 = jnp.concatenate([ml_got[6:8, :], ml_got[4:6, :]], axis=0)
    top = jnp.maximum(m0, m1)
    e0 = jnp.exp2(m0 - top)
    e1 = jnp.exp2(m1 - top)
    weight_sum = l0 * e0 + l1 * e1
    lse_ref[...] = ((top + jnp.log2(weight_sum)) * LN2)[0:2, :]
    f0 = e0 / weight_sum
    f1 = e1 / weight_sum
    f0 = jnp.where(c == 0, f0[:, 0:128], f0[:, 128:256])
    f1 = jnp.where(c == 0, f1[:, 0:128], f1[:, 128:256])
    result = jnp.zeros((128, 1024), F32)
    for p, w in enumerate((w_own, w_other)):
        pieces = []
        for i in range(2):
            h, k = 2 * p + i, (2 * p + i + 2) % 4
            mine = keep[64 * h : 64 * (h + 1), :]
            theirs = got[64 * k : 64 * (k + 1), :].astype(F32)
            pieces.append(mine * f0[h : h + 1, :] + theirs * f1[h : h + 1, :])
        attended = jnp.transpose(jnp.concatenate(pieces, axis=0)).astype(BF)
        for j in range(NX):
            outs[p, :, lax.rem(x - j + NX, NX)] = w[:, j, 32:64, :]
        result = result + lax.dot_general(
            attended, outs[p].reshape(1024, 128), (((1,), (1,)), ((), ())),
            preferred_element_type=F32,
        )
    scratch[...] = result
    y = where[2]
    for j, out in enumerate((part_ref, p1_ref, p2_ref, p3_ref)):
        to = lax.rem(y + j, NY)
        out[...] = scratch[pl.ds(pl.multiple_of(to * 32, 32), 32), :].astype(BF)


def finish(part, p1, p2, p3, gain, out):
    summed = part[...].astype(F32)
    for other in (p1, p2, p3):
        summed = summed + other[...].astype(F32)
    wide = summed.astype(BF).astype(F32)
    mean = jnp.mean(wide * wide, axis=1, keepdims=True)
    out[...] = (wide * lax.rsqrt(mean + EPS) * gain[...]).astype(BF)


def flat(z, x, y, c):
    return ((z * NX + x) * NY + y) * NC + c


def ring(j):
    return [(i, (i + j) % NY) for i in range(NY)]


def shift_pairs(stage, j):
    pairs = []
    for z in range(NZ):
        for x in range(NX):
            for y in range(NY):
                for c in range(NC):
                    along_x = (c == 0) == (stage == 2)
                    to = flat(z, (x + j) % NX, y, c) if along_x else flat(z, x, (y + j) % NY, c)
                    pairs.append((flat(z, x, y, c), to))
    return pairs


def layer(
    tokens, doc_ids, down_query, down_key, down_rotary, query_gain, key_gain,
    up_query, up_key, up_value, output_weight, out_gain,
):
    z = lax.axis_index("z")
    x = lax.axis_index("x")
    y = lax.axis_index("y")
    c = lax.axis_index("c")
    sp = z * NX + x
    here = jnp.stack([z, x, y, c, sp * 256]).astype(jnp.int32)
    swap = [(0, 1), (1, 0)]

    sources = (down_query, down_key, down_rotary)
    message = call(
        pack, jax.ShapeDtypeStruct((NZ, 40, 128), BF), 1, 3, any_from=0,
        scratch=[VMEM((128, 128), F32)]
        + [VMEM(a.shape, a.dtype) for a in sources]
        + [pltpu.SemaphoreType.DMA((3,))],
    )(here, *(pltpu.with_memory_space_constraint(a, pltpu.HBM) for a in sources))
    gathered = lax.all_to_all(message, "z", 0, 0)
    gathered = [gathered] + [lax.ppermute(gathered, "x", ring(j)) for j in range(1, NX)]

    rows = [tokens] + [lax.ppermute(tokens, "y", ring(j)) for j in range(1, NY)]

    later = call(pack_later, jax.ShapeDtypeStruct((64, 128), BF), 0, 5)(
        up_query, up_key, up_value, doc_ids.reshape(2, 128), output_weight.T
    )
    later = [later] + [lax.ppermute(later, "x", ring(j)) for j in range(1, NX)]
    later = jnp.broadcast_to(jnp.stack(later)[None], (NZ, NX, 64, 128))

    q_part, k_part = call(
        project,
        (jax.ShapeDtypeStruct((64, 128), BF), jax.ShapeDtypeStruct((NZ, 72, 128), BF)),
        1, 8, scratch=[VMEM((128, 1024), BF), VMEM((NX, NZ, 40, 128), BF)],
    )(here, *rows, *gathered)

    stage1 = lax.all_to_all(k_part, "z", 0, 0)
    stage2 = [lax.ppermute(stage1, AXES, shift_pairs(2, j)) for j in range(1, 4)]
    held = jnp.stack([stage1] + stage2)
    stage3 = [lax.ppermute(held, AXES, shift_pairs(3, j)) for j in range(1, 4)]

    up_own = lax.all_to_all(later, "z", 0, 0)
    up_other = lax.ppermute(up_own, "c", swap)
    q_pair = jnp.stack([q_part, lax.ppermute(q_part, "c", swap)])
    q_all = [q_pair] + [lax.ppermute(q_pair, "y", ring(j)) for j in range(1, NY)]
    queries, uk, uv, key_docs, gains, query_docs = call(
        make_queries,
        (
            jax.ShapeDtypeStruct((4, 256, 256), BF),
            jax.ShapeDtypeStruct((256, 256), BF),
            jax.ShapeDtypeStruct((256, 256), BF),
            jax.ShapeDtypeStruct((NS, 128), F32),
            jax.ShapeDtypeStruct((256, 128), F32),
            jax.ShapeDtypeStruct((2, 128), F32),
        ),
        1, 9, scratch=[VMEM((256, 256), F32), VMEM((2, NZ, NX, 32, 128), BF)],
    )(
        here, *q_all, up_own, up_other, query_gain.reshape(2, 128),
        key_gain.reshape(2, 128), doc_ids.reshape(2, 128),
    )

    keep, send, ml = call(
        attend,
        (
            jax.ShapeDtypeStruct((256, 128), F32),
            jax.ShapeDtypeStruct((256, 128), BF),
            jax.ShapeDtypeStruct((8, 256), F32),
        ),
        2, 10, room=34,
        scratch=[
            VMEM((4, 4, NZ, 72, 128), BF),
            VMEM((16, 4, 256, 256), F32),
            VMEM((16, 256, 256), BF),
            VMEM((4, 8, 256), F32),
            VMEM((4, 8, 256), F32),
            VMEM((256, 256), F32),
        ],
    )(here, doc_ids, queries, uk, uv, key_docs, gains, query_docs, held, *stage3)

    got = lax.ppermute(send, "c", swap)
    ml_got = lax.ppermute(ml, "c", swap)
    *parts, log_sums = call(
        combine,
        (jax.ShapeDtypeStruct((32, 1024), BF),) * NY + (jax.ShapeDtypeStruct((2, 256), F32),),
        1, 6, scratch=[VMEM((128, 1024), F32), VMEM((2, NZ, NX, 32, 128), BF)],
    )(here, keep, got, ml, ml_got, up_own, up_other)
    parts[1:] = [lax.ppermute(parts[j], "y", ring(j)) for j in range(1, NY)]
    mixed = call(finish, jax.ShapeDtypeStruct((32, 1024), BF), 0, 5)(
        *parts, out_gain.reshape(1, 1024)
    )
    log_sums = log_sums.reshape(2, 2, 4, 32).transpose(2, 1, 3, 0).reshape(256, 2)
    return mixed, log_sums


def solution(mesh):
    finer = Mesh(mesh.devices.reshape(NZ, NX, NY, NC), AXES)
    return jax.shard_map(
        layer,
        mesh=finer,
        in_specs=(
            P(AXES, None), P(SP), P(SP, None), P(SP, None), P(SP, None), P(), P(),
            P(SP, TP), P(SP, TP), P(SP, TP), P(TP, SP), P(),
        ),
        out_specs=(P(AXES, None), P(SP, TP)),
        check_vma=False,
    )
```

```python
import math

import jax
import jax.numpy as jnp
from jax import lax
from jax.experimental import pallas as pl
from jax.experimental.pallas import tpu as pltpu
from jax.sharding import Mesh
from jax.sharding import PartitionSpec as P


NOPE = 64
ROPE = 32
NZ, NX, NY, NC = 8, 4, 4, 2
NS = NZ * NX
AXES = ("z", "x", "y", "c")
SP = ("z", "x")
TP = ("y", "c")
NEG_BIG = -1e30
FLOOR = -1e20
THETA = 10000.0
EPS = 1e-06
LN2 = math.log(2.0)
SCALE2 = 1.0 / math.sqrt(NOPE + ROPE) / LN2
BF = jnp.bfloat16
F32 = jnp.float32


VMEM = pltpu.VMEM
SMEM_SPEC = pl.BlockSpec(memory_space=pltpu.SMEM)
VMEM_SPEC = pl.BlockSpec(memory_space=pltpu.VMEM)
ANY_SPEC = pl.BlockSpec(memory_space=pltpu.HBM)


def call(body, outs, n_smem, n_in, scratch=(), any_from=None, cost=None, room=16):
    specs = [SMEM_SPEC] * n_smem
    for i in range(n_in):
        specs.append(ANY_SPEC if any_from is not None and i >= any_from else VMEM_SPEC)
    single = not isinstance(outs, tuple)
    return pl.pallas_call(
        body,
        out_shape=outs,
        in_specs=specs,
        out_specs=VMEM_SPEC if single else tuple(VMEM_SPEC for _ in outs),
        scratch_shapes=list(scratch),
        compiler_params=pltpu.CompilerParams(vmem_limit_bytes=room * 1024 * 1024),
        cost_estimate=cost,
    )


def lanes(shape):
    return lax.broadcasted_iota(jnp.int32, shape, len(shape) - 1)


def column(row):
    return jnp.transpose(jnp.broadcast_to(row, (128, 128)))


def frequency(index):
    value = jnp.ones(index.shape, F32)
    for bit in range(4):
        factor = THETA ** (-(1 << bit) / 16)
        value = value * jnp.where((index // (1 << bit)) % 2 == 1, factor, 1.0)
    return value


def pack(where, dq_in, dk_in, dr_in, out, flipped, dq, dk, dr, sems):
    copies = [
        pltpu.make_async_copy(source, place, sems.at[i])
        for i, (source, place) in enumerate(((dq_in, dq), (dk_in, dk), (dr_in, dr)))
    ]
    for copy in copies:
        copy.start()
    for copy in copies:
        copy.wait()
    y = where[2]

    def chosen(ref):
        block = ref[:, 0:64]
        for k in range(1, NY):
            block = jnp.where(y == k, ref[:, 64 * k : 64 * (k + 1)], block)
        return block

    block = jnp.concatenate([chosen(dq), chosen(dk)], axis=1)
    rope = dr[...].astype(F32)
    rope = jnp.concatenate([rope, jnp.zeros((32, 96), F32)], axis=1)
    flipped[...] = jnp.transpose(jnp.concatenate([rope] * 4, axis=0))
    turned = jnp.concatenate([flipped[pl.ds(4 * y, 4), :], flipped[pl.ds(16 + 4 * y, 4), :]], axis=0)
    turned = turned.astype(BF)
    for z in range(NZ):
        out[z, 0:32, :] = block
        out[z, 32:40, :] = turned


def pack_later(*refs):
    inputs, out, table, places, sems = refs[:7], refs[7], refs[8], refs[9:16], refs[16]
    copies = [
        pltpu.make_async_copy(source, place, sems.at[i])
        for i, (source, place) in enumerate(zip(inputs, places))
    ]
    for copy in copies:
        copy.start()
    for copy in copies:
        copy.wait()
    up_query, up_key, up_value, docs_ref, out_t, query_gain, key_gain = places
    table[0:2, :] = query_gain[...]
    table[2:4, :] = key_gain[...]
    table[4:6, :] = docs_ref[...].astype(F32)
    src = lax.broadcasted_iota(jnp.int32, (192, 256), 0)
    lane = lanes((192, 256))
    plain = 96 * (lane // 64) + lane % 64
    turn = lane - 128
    rope = 64 + 96 * (turn // 32) + 16 * ((turn // 4) % 2) + 4 * ((turn % 32) // 8) + turn % 4
    chosen = jnp.where(lane < 128, plain, jnp.where(lane < 192, rope, -1))
    pick = jnp.where(src == chosen, 1.0, 0.0).astype(BF)
    sorted_query = jnp.dot(up_query[...], pick, preferred_element_type=F32)
    out[0:8, :] = sorted_query[:, 0:128].astype(BF)
    out[8:16, :] = up_key[...]
    out[16:24, :] = up_value[...]
    mixed = sorted_query[:, 128:256]
    docs = docs_ref[...].astype(F32)
    row = lax.broadcasted_iota(jnp.int32, (8, 128), 0)
    at = lanes((8, 128))
    for r in range(8):
        line = docs[r // 4 : r // 4 + 1, :]
        moved = pltpu.roll(jnp.broadcast_to(line, (8, 128)), (64 - 32 * (r % 4)) % 128, 1)
        mixed = jnp.where((row == r) & (at // 32 == 2), moved, mixed)
    out[24:32, :] = mixed.astype(BF)
    out[32:64, :] = out_t[...]


def project(where, t0, t1, t2, t3, g0, g1, g2, g3, q_ref, k_ref, tok, gathered):
    x = where[1]
    y = where[2]
    for j, part in enumerate((t0, t1, t2, t3)):
        at = lax.rem(y - j + NY, NY)
        tok[pl.ds(pl.multiple_of(at * 32, 32), 32), :] = part[...]
    for j, part in enumerate((g0, g1, g2, g3)):
        gathered[lax.rem(x - j + NX, NX)] = part[...]
    rows = tok[...]
    weights = jnp.concatenate(
        [gathered[k, z, 0:32, :] for z in range(NZ) for k in range(NX)], axis=0
    )
    both = jnp.dot(rows, weights, preferred_element_type=F32)
    turned = jnp.transpose(both).astype(BF)
    q_ref[...] = turned[0:64, :]
    for t in range(NZ):
        k_ref[t, 0:64, :] = turned[64:128, :]
    group = lanes((8, 128)) // 32
    pieces = []
    for z in range(NZ):
        piece = gathered[0, z, 32:40, :].astype(F32)
        for g in range(1, 4):
            piece = jnp.where(group == g, gathered[g, z, 32:40, :].astype(F32), piece)
        pieces.append(piece)
    rope = jnp.concatenate(pieces, axis=1)
    rope = jnp.concatenate([rope, jnp.zeros_like(rope)], axis=0).astype(BF)
    raw = lax.dot_general(rope, rows, (((1,), (1,)), ((), ())), preferred_element_type=F32)
    raw = raw[0:8, :].astype(BF).astype(F32)
    at = lanes((8, 128))
    row = lax.broadcasted_iota(jnp.int32, (8, 128), 0)
    pos = where[4] + 64 * (at // 32) + 32 * where[3] + at % 32
    angle = pos.astype(F32) * frequency(4 * y + row % 4)
    sine = jnp.sin(angle)
    rotated = raw * jnp.cos(angle) + pltpu.roll(raw, 4, 0) * jnp.where(row < 4, -sine, sine)
    rotated = rotated.astype(BF)
    for t in range(NZ):
        k_ref[t, 64:72, :] = rotated


def make_queries(
    where, q0, q1, q2, q3, up_own, up_other, table,
    out, uk_ref, uv_ref, docs_ref, col_ref, row_ref, latents, ups,
):
    x, y, c = where[1], where[2], where[3]
    for j, part in enumerate((q0, q1, q2, q3)):
        own, other = part[0].astype(F32), part[1].astype(F32)
        rows = pl.ds(pl.multiple_of(lax.rem(y - j + NY, NY) * 64, 64), 64)
        latents[rows, 0:128] = jnp.where(c == 0, own, other)
        latents[rows, 128:256] = jnp.where(c == 0, other, own)
    raw = latents[...]
    mean = jnp.sum(raw * raw, axis=0, keepdims=True) * (1.0 / 256.0)
    inverse = lax.rsqrt(mean + EPS)
    gains = jnp.concatenate([column(table[0:1, :]), column(table[1:2, :])], axis=0)
    gains = jnp.concatenate([gains, gains], axis=1)
    tokens_docs = table[4:6, :]
    at = lanes((1, 128))
    for i in range(2):
        col_ref[128 * i : 128 * (i + 1), :] = column(table[2 + i : 3 + i, :])
        ordered = jnp.zeros((1, 128), F32)
        for k in range(NY):
            line = tokens_docs[k // 2 : k // 2 + 1, :]
            moved = pltpu.roll(line, (32 * k - 64 * (k % 2) - 32 * i) % 128, 1)
            ordered = jnp.where(at // 32 == k, moved, ordered)
        row_ref[i : i + 1, :] = ordered
    latent = (raw * inverse * gains).astype(BF)
    tok = lanes((64, 256))
    row = lax.broadcasted_iota(jnp.int32, (64, 256), 0)
    pos = where[4] + 64 * ((tok % 128) // 32) + 32 * (tok // 128) + tok % 32
    angle = pos.astype(F32) * frequency(4 * ((row % 32) // 8) + row % 4)
    is_low = (row // 4) % 2 == 0
    cos = jnp.cos(angle)
    sine = jnp.sin(angle)
    low_sin = jnp.where(is_low, -sine, 0.0)
    high_sin = jnp.where(is_low, 0.0, sine)
    for p, up in enumerate((up_own, up_other)):
        for j in range(NX):
            ups[p, :, lax.rem(x - j + NX, NX)] = up[:, j, 0:32, :]
        wide = ups[p].reshape(NS, 32, 128).astype(F32)
        own = slice(128 * p, 128 * (p + 1))
        plain_w = jnp.transpose(wide[:, 0:8, :].reshape(256, 128)).astype(BF)
        rope_w = jnp.transpose(wide[:, 24:32, :].reshape(256, 128))[0:64, :].astype(BF)
        uk_ref[:, own] = wide[:, 8:16, :].reshape(256, 128).astype(BF)
        uv_ref[own, :] = jnp.transpose(wide[:, 16:24, :].reshape(256, 128)).astype(BF)
        plain = (jnp.dot(plain_w, latent, preferred_element_type=F32) * SCALE2).astype(BF)
        raw = jnp.dot(rope_w, latent, preferred_element_type=F32) * SCALE2
        rope = raw * cos + pltpu.roll(raw, 60, 0) * low_sin + pltpu.roll(raw, 4, 0) * high_sin
        rope = rope.astype(BF)
        for i in range(2):
            h = 2 * p + i
            out[h] = jnp.zeros((256, 256), BF)
            out[h, 64 * i : 64 * (i + 1), :] = plain[64 * i : 64 * (i + 1), :]
            out[h, 128:160, :] = rope[32 * i : 32 * (i + 1), :]
    docs = ups[0].reshape(NS, 32, 128)[:, 24:32, :].astype(F32)
    at = lanes((NS, 128))
    spread = jnp.zeros((NS, 128), F32)
    for k in range(NY):
        piece = jnp.where(c == 0, docs[:, 2 * k, :], docs[:, 2 * k + 1, :])
        spread = jnp.where(at // 32 == k, pltpu.roll(piece, (32 * k + 64) % 128, 1), spread)
    docs_ref[...] = spread


def attend(
    where, ids, q_ref, uk, uv, key_docs, gains, query_docs, b0, b1, b2, b3,
    keep_ref, send_ref, ml_ref, kb, s_buf, v_buf, mx, total, acc,
):
    x0, y0, c = where[1], where[2], where[3]
    docs = key_docs[...]
    at = lanes((NS, 128))
    before = (at == 127) & (docs < ids[0].astype(F32))
    behind = (at == 0) & (docs > ids[255].astype(F32))
    low = jnp.sum(before.astype(jnp.int32))
    high = NS - 1 - jnp.sum(behind.astype(jnp.int32))
    count = (high - low) // 2 + 1
    begin = jnp.minimum(low, NS - 2 * count)

    def fetch(z, carry):
        for j, part in enumerate((b0, b1, b2, b3)):
            for k in range(4):
                kb[j, k, z] = part[k, z]
        return carry

    lax.fori_loop(begin // 4, (begin + 2 * count - 1) // 4 + 1, fetch, 0)
    mx[...] = jnp.full(mx.shape, NEG_BIG, F32)
    total[...] = jnp.zeros(total.shape, F32)
    acc[...] = jnp.zeros(acc.shape, F32)
    wanted = jnp.concatenate([query_docs[0:1, :], query_docs[1:2, :]], axis=1)

    def scores(tile, carry):
        latents, ropes, same = [], [], []
        for half in range(2):
            block = begin + 2 * tile + half
            z, x = block // NX, lax.rem(block, NX)
            jx = lax.rem(x0 - x + NX, NX)
            parts, turned = [], []
            for y in range(NY):
                jy = lax.rem(y0 - y + NY, NY)
                third = jnp.where(c == 0, jy, jx)
                second = jnp.where(c == 0, jx, jy)
                slab = kb[third, second, z].astype(F32)
                parts.append(slab[0:64, :])
                turned.append(slab[64:72, :])
            squares = parts[0] * parts[0]
            for part in parts[1:]:
                squares = squares + part * part
            mean = jnp.sum(squares, axis=0, keepdims=True) * (1.0 / 256.0)
            inverse = lax.rsqrt(mean + EPS)
            latents.append(jnp.concatenate(parts, axis=0) * inverse * gains[...])
            ropes.append(jnp.concatenate(turned, axis=0))
            docs_col = column(key_docs[pl.ds(block, 1), :])
            same.append(jnp.concatenate([docs_col, docs_col], axis=1) == wanted)
        latent = jnp.concatenate(latents, axis=1)
        v_buf[tile] = jnp.dot(uv[...], latent.astype(BF), preferred_element_type=F32).astype(BF)
        turned = jnp.transpose(latent).astype(BF)
        rope = jnp.concatenate(ropes, axis=1)
        rope = jnp.concatenate([rope, jnp.zeros((96, 256), F32)], axis=0)
        rope = jnp.transpose(rope).astype(BF)
        keys = jnp.dot(turned, uk[...], preferred_element_type=F32).astype(BF)
        for h in range(4):
            p = h // 2
            stack = jnp.concatenate([keys[:, 128 * p : 128 * (p + 1)], rope], axis=1)
            got = jnp.dot(stack, q_ref[h], preferred_element_type=F32)
            got = jnp.concatenate(
                [
                    jnp.where(same[0], got[0:128, :], NEG_BIG),
                    jnp.where(same[1], got[128:256, :], NEG_BIG),
                ],
                axis=0,
            )
            s_buf[tile, h] = got
            mx[h] = jnp.maximum(mx[h], jnp.max(got.reshape(32, 8, 256), axis=0))
        return carry

    lax.fori_loop(0, count, scores, 0)
    tops = []
    for h in range(4):
        top = jnp.maximum(jnp.max(mx[h], axis=0, keepdims=True), FLOOR)
        mx[h] = jnp.broadcast_to(top, (8, 256))
        tops.append(top)

    def weigh(tile, carry):
        for h in range(4):
            own = slice(64 * h, 64 * (h + 1))
            weights = jnp.exp2(s_buf[tile, h].reshape(32, 8, 256) - mx[h][None])
            total[h] = total[h] + jnp.sum(weights, axis=0)
            weights = weights.reshape(256, 256).astype(BF)
            acc[own, :] = acc[own, :] + jnp.dot(
                v_buf[tile, own, :], weights, preferred_element_type=F32
            )
        return carry

    lax.fori_loop(0, count, weigh, 0)
    for h in range(4):
        ml_ref[h : h + 1, :] = tops[h]
        ml_ref[4 + h : 5 + h, :] = jnp.sum(total[h], axis=0, keepdims=True)
    left, right = acc[:, 0:128], acc[:, 128:256]
    keep_ref[...] = jnp.where(c == 0, left, right)
    send_ref[...] = jnp.where(c == 0, right, left).astype(BF)


def combine(
    where, keep, got, ml_own, ml_got, w_own, w_other, part_ref, p1_ref, p2_ref, p3_ref, lse_ref,
    scratch, outs,
):
    x, c = where[1], where[3]
    m0, l0 = ml_own[0:4, :], ml_own[4:8, :]
    m1 = jnp.concatenate([ml_got[2:4, :], ml_got[0:2, :]], axis=0)
    l1 = jnp.concatenate([ml_got[6:8, :], ml_got[4:6, :]], axis=0)
    top = jnp.maximum(m0, m1)
    e0 = jnp.exp2(m0 - top)
    e1 = jnp.exp2(m1 - top)
    weight_sum = l0 * e0 + l1 * e1
    lse_ref[...] = ((top + jnp.log2(weight_sum)) * LN2)[0:2, :]
    f0 = e0 / weight_sum
    f1 = e1 / weight_sum
    f0 = jnp.where(c == 0, f0[:, 0:128], f0[:, 128:256])
    f1 = jnp.where(c == 0, f1[:, 0:128], f1[:, 128:256])
    result = jnp.zeros((128, 1024), F32)
    for p, w in enumerate((w_own, w_other)):
        pieces = []
        for i in range(2):
            h, k = 2 * p + i, (2 * p + i + 2) % 4
            mine = keep[64 * h : 64 * (h + 1), :]
            theirs = got[64 * k : 64 * (k + 1), :].astype(F32)
            pieces.append(mine * f0[h : h + 1, :] + theirs * f1[h : h + 1, :])
        attended = jnp.transpose(jnp.concatenate(pieces, axis=0)).astype(BF)
        for j in range(NX):
            outs[p, :, lax.rem(x - j + NX, NX)] = w[:, j, 32:64, :]
        result = result + lax.dot_general(
            attended, outs[p].reshape(1024, 128), (((1,), (1,)), ((), ())),
            preferred_element_type=F32,
        )
    scratch[...] = result
    y = where[2]
    for j, out in enumerate((part_ref, p1_ref, p2_ref, p3_ref)):
        to = lax.rem(y + j, NY)
        out[...] = scratch[pl.ds(pl.multiple_of(to * 32, 32), 32), :].astype(BF)


def finish(part, p1, p2, p3, gain, out):
    summed = part[...].astype(F32)
    for other in (p1, p2, p3):
        summed = summed + other[...].astype(F32)
    wide = summed.astype(BF).astype(F32)
    mean = jnp.mean(wide * wide, axis=1, keepdims=True)
    out[...] = (wide * lax.rsqrt(mean + EPS) * gain[...]).astype(BF)


def flat(z, x, y, c):
    return ((z * NX + x) * NY + y) * NC + c


def ring(j):
    return [(i, (i + j) % NY) for i in range(NY)]


def shift_pairs(stage, j):
    pairs = []
    for z in range(NZ):
        for x in range(NX):
            for y in range(NY):
                for c in range(NC):
                    along_x = (c == 0) == (stage == 2)
                    to = flat(z, (x + j) % NX, y, c) if along_x else flat(z, x, (y + j) % NY, c)
                    pairs.append((flat(z, x, y, c), to))
    return pairs


def layer(
    tokens, doc_ids, down_query, down_key, down_rotary, query_gain, key_gain,
    up_query, up_key, up_value, output_weight, out_gain,
):
    z = lax.axis_index("z")
    x = lax.axis_index("x")
    y = lax.axis_index("y")
    c = lax.axis_index("c")
    sp = z * NX + x
    here = jnp.stack([z, x, y, c, sp * 256]).astype(jnp.int32)
    swap = [(0, 1), (1, 0)]

    sources = (down_query, down_key, down_rotary)
    message = call(
        pack, jax.ShapeDtypeStruct((NZ, 40, 128), BF), 1, 3, any_from=0,
        scratch=[VMEM((128, 128), F32)]
        + [VMEM(a.shape, a.dtype) for a in sources]
        + [pltpu.SemaphoreType.DMA((3,))],
    )(here, *(pltpu.with_memory_space_constraint(a, pltpu.HBM) for a in sources))
    gathered = lax.all_to_all(message, "z", 0, 0)
    gathered = [gathered] + [lax.ppermute(gathered, "x", ring(j)) for j in range(1, NX)]

    rows = [tokens] + [lax.ppermute(tokens, "y", ring(j)) for j in range(1, NY)]

    sources = (
        up_query, up_key, up_value, doc_ids.reshape(2, 128), output_weight.T,
        query_gain.reshape(2, 128), key_gain.reshape(2, 128),
    )
    later, table = call(
        pack_later, (jax.ShapeDtypeStruct((64, 128), BF), jax.ShapeDtypeStruct((6, 128), F32)),
        0, 7, any_from=0,
        scratch=[VMEM(a.shape, a.dtype) for a in sources] + [pltpu.SemaphoreType.DMA((7,))],
    )(*(pltpu.with_memory_space_constraint(a, pltpu.HBM) for a in sources))
    later = [later] + [lax.ppermute(later, "x", ring(j)) for j in range(1, NX)]
    later = jnp.broadcast_to(jnp.stack(later)[None], (NZ, NX, 64, 128))

    q_part, k_part = call(
        project,
        (jax.ShapeDtypeStruct((64, 128), BF), jax.ShapeDtypeStruct((NZ, 72, 128), BF)),
        1, 8, scratch=[VMEM((128, 1024), BF), VMEM((NX, NZ, 40, 128), BF)],
    )(here, *rows, *gathered)

    stage1 = lax.all_to_all(k_part, "z", 0, 0)
    stage2 = [lax.ppermute(stage1, AXES, shift_pairs(2, j)) for j in range(1, 4)]
    held = jnp.stack([stage1] + stage2)
    stage3 = [lax.ppermute(held, AXES, shift_pairs(3, j)) for j in range(1, 4)]

    up_own = lax.all_to_all(later, "z", 0, 0)
    up_other = lax.ppermute(up_own, "c", swap)
    q_pair = jnp.stack([q_part, lax.ppermute(q_part, "c", swap)])
    q_all = [q_pair] + [lax.ppermute(q_pair, "y", ring(j)) for j in range(1, NY)]
    queries, uk, uv, key_docs, gains, query_docs = call(
        make_queries,
        (
            jax.ShapeDtypeStruct((4, 256, 256), BF),
            jax.ShapeDtypeStruct((256, 256), BF),
            jax.ShapeDtypeStruct((256, 256), BF),
            jax.ShapeDtypeStruct((NS, 128), F32),
            jax.ShapeDtypeStruct((256, 128), F32),
            jax.ShapeDtypeStruct((2, 128), F32),
        ),
        1, 7, scratch=[VMEM((256, 256), F32), VMEM((2, NZ, NX, 32, 128), BF)],
    )(
        here, *q_all, up_own, up_other, table
    )

    keep, send, ml = call(
        attend,
        (
            jax.ShapeDtypeStruct((256, 128), F32),
            jax.ShapeDtypeStruct((256, 128), BF),
            jax.ShapeDtypeStruct((8, 256), F32),
        ),
        2, 10, room=34,
        scratch=[
            VMEM((4, 4, NZ, 72, 128), BF),
            VMEM((16, 4, 256, 256), F32),
            VMEM((16, 256, 256), BF),
            VMEM((4, 8, 256), F32),
            VMEM((4, 8, 256), F32),
            VMEM((256, 256), F32),
        ],
    )(here, doc_ids, queries, uk, uv, key_docs, gains, query_docs, held, *stage3)

    got = lax.ppermute(send, "c", swap)
    ml_got = lax.ppermute(ml, "c", swap)
    *parts, log_sums = call(
        combine,
        (jax.ShapeDtypeStruct((32, 1024), BF),) * NY + (jax.ShapeDtypeStruct((2, 256), F32),),
        1, 6, scratch=[VMEM((128, 1024), F32), VMEM((2, NZ, NX, 32, 128), BF)],
    )(here, keep, got, ml, ml_got, up_own, up_other)
    parts[1:] = [lax.ppermute(parts[j], "y", ring(j)) for j in range(1, NY)]
    mixed = call(finish, jax.ShapeDtypeStruct((32, 1024), BF), 0, 5)(
        *parts, out_gain.reshape(1, 1024)
    )
    log_sums = log_sums.reshape(2, 2, 4, 32).transpose(2, 1, 3, 0).reshape(256, 2)
    return mixed, log_sums


def solution(mesh):
    finer = Mesh(mesh.devices.reshape(NZ, NX, NY, NC), AXES)
    return jax.shard_map(
        layer,
        mesh=finer,
        in_specs=(
            P(AXES, None), P(SP), P(SP, None), P(SP, None), P(SP, None), P(), P(),
            P(SP, TP), P(SP, TP), P(SP, TP), P(TP, SP), P(),
        ),
        out_specs=(P(AXES, None), P(SP, TP)),
        check_vma=False,
    )
```

```python
import math

import jax
import jax.numpy as jnp
from jax import lax
from jax.experimental import pallas as pl
from jax.experimental.pallas import tpu as pltpu
from jax.sharding import Mesh
from jax.sharding import PartitionSpec as P


NOPE = 64
ROPE = 32
NZ, NX, NY, NC = 8, 4, 4, 2
NS = NZ * NX
AXES = ("z", "x", "y", "c")
SP = ("z", "x")
TP = ("y", "c")
NEG_BIG = -1e30
FLOOR = -1e20
THETA = 10000.0
EPS = 1e-06
LN2 = math.log(2.0)
SCALE2 = 1.0 / math.sqrt(NOPE + ROPE) / LN2
BF = jnp.bfloat16
F32 = jnp.float32


VMEM = pltpu.VMEM
SMEM_SPEC = pl.BlockSpec(memory_space=pltpu.SMEM)
VMEM_SPEC = pl.BlockSpec(memory_space=pltpu.VMEM)
ANY_SPEC = pl.BlockSpec(memory_space=pltpu.HBM)


def call(body, outs, n_smem, n_in, scratch=(), any_from=None, cost=None, room=16):
    specs = [SMEM_SPEC] * n_smem
    for i in range(n_in):
        specs.append(ANY_SPEC if any_from is not None and i >= any_from else VMEM_SPEC)
    single = not isinstance(outs, tuple)
    return pl.pallas_call(
        body,
        out_shape=outs,
        in_specs=specs,
        out_specs=VMEM_SPEC if single else tuple(VMEM_SPEC for _ in outs),
        scratch_shapes=list(scratch),
        compiler_params=pltpu.CompilerParams(vmem_limit_bytes=room * 1024 * 1024),
        cost_estimate=cost,
    )


def lanes(shape):
    return lax.broadcasted_iota(jnp.int32, shape, len(shape) - 1)


def column(row):
    return jnp.transpose(jnp.broadcast_to(row, (128, 128)))


def by_twos(step, count):
    def both(i, carry):
        step(2 * i)
        step(2 * i + 1)
        return carry

    lax.fori_loop(0, count // 2, both, 0)

    @pl.when(lax.rem(count, 2) == 1)
    def _():
        step(count - 1)


def frequency(index):
    value = jnp.ones(index.shape, F32)
    for bit in range(4):
        factor = THETA ** (-(1 << bit) / 16)
        value = value * jnp.where((index // (1 << bit)) % 2 == 1, factor, 1.0)
    return value


def pack(where, dq_in, dk_in, dr_in, out, flipped, dq, dk, dr, sems):
    copies = [
        pltpu.make_async_copy(source, place, sems.at[i])
        for i, (source, place) in enumerate(((dq_in, dq), (dk_in, dk), (dr_in, dr)))
    ]
    for copy in copies:
        copy.start()
    for copy in copies:
        copy.wait()
    y = where[2]

    def chosen(ref):
        block = ref[:, 0:64]
        for k in range(1, NY):
            block = jnp.where(y == k, ref[:, 64 * k : 64 * (k + 1)], block)
        return block

    block = jnp.concatenate([chosen(dq), chosen(dk)], axis=1)
    rope = dr[...].astype(F32)
    rope = jnp.concatenate([rope, jnp.zeros((32, 96), F32)], axis=1)
    flipped[...] = jnp.transpose(jnp.concatenate([rope] * 4, axis=0))
    turned = jnp.concatenate([flipped[pl.ds(4 * y, 4), :], flipped[pl.ds(16 + 4 * y, 4), :]], axis=0)
    turned = turned.astype(BF)
    for z in range(NZ):
        out[z, 0:32, :] = block
        out[z, 32:40, :] = turned


def pack_later(*refs):
    inputs, out, table, places, sems = refs[:7], refs[7], refs[8], refs[9:16], refs[16]
    copies = [
        pltpu.make_async_copy(source, place, sems.at[i])
        for i, (source, place) in enumerate(zip(inputs, places))
    ]
    for copy in copies:
        copy.start()
    for copy in copies:
        copy.wait()
    up_query, up_key, up_value, docs_ref, out_t, query_gain, key_gain = places
    table[0:2, :] = query_gain[...]
    table[2:4, :] = key_gain[...]
    table[4:6, :] = docs_ref[...].astype(F32)
    src = lax.broadcasted_iota(jnp.int32, (192, 256), 0)
    lane = lanes((192, 256))
    plain = 96 * (lane // 64) + lane % 64
    turn = lane - 128
    rope = 64 + 96 * (turn // 32) + 16 * ((turn // 4) % 2) + 4 * ((turn % 32) // 8) + turn % 4
    chosen = jnp.where(lane < 128, plain, jnp.where(lane < 192, rope, -1))
    pick = jnp.where(src == chosen, 1.0, 0.0).astype(BF)
    sorted_query = jnp.dot(up_query[...], pick, preferred_element_type=F32)
    out[0:8, :] = sorted_query[:, 0:128].astype(BF)
    out[8:16, :] = up_key[...]
    out[16:24, :] = up_value[...]
    mixed = sorted_query[:, 128:256]
    docs = docs_ref[...].astype(F32)
    row = lax.broadcasted_iota(jnp.int32, (8, 128), 0)
    at = lanes((8, 128))
    for r in range(8):
        line = docs[r // 4 : r // 4 + 1, :]
        moved = pltpu.roll(jnp.broadcast_to(line, (8, 128)), (64 - 32 * (r % 4)) % 128, 1)
        mixed = jnp.where((row == r) & (at // 32 == 2), moved, mixed)
    out[24:32, :] = mixed.astype(BF)
    out[32:64, :] = out_t[...]


def project(where, t0, t1, t2, t3, g0, g1, g2, g3, q_ref, k_ref, tok, gathered):
    x = where[1]
    y = where[2]
    for j, part in enumerate((t0, t1, t2, t3)):
        at = lax.rem(y - j + NY, NY)
        tok[pl.ds(pl.multiple_of(at * 32, 32), 32), :] = part[...]
    for j, part in enumerate((g0, g1, g2, g3)):
        gathered[lax.rem(x - j + NX, NX)] = part[...]
    rows = tok[...]
    weights = jnp.concatenate(
        [gathered[k, z, 0:32, :] for z in range(NZ) for k in range(NX)], axis=0
    )
    both = jnp.dot(rows, weights, preferred_element_type=F32)
    turned = jnp.transpose(both).astype(BF)
    q_ref[...] = turned[0:64, :]
    for t in range(NZ):
        k_ref[t, 0:64, :] = turned[64:128, :]
    group = lanes((8, 128)) // 32
    pieces = []
    for z in range(NZ):
        piece = gathered[0, z, 32:40, :].astype(F32)
        for g in range(1, 4):
            piece = jnp.where(group == g, gathered[g, z, 32:40, :].astype(F32), piece)
        pieces.append(piece)
    rope = jnp.concatenate(pieces, axis=1)
    rope = jnp.concatenate([rope, jnp.zeros_like(rope)], axis=0).astype(BF)
    raw = lax.dot_general(rope, rows, (((1,), (1,)), ((), ())), preferred_element_type=F32)
    raw = raw[0:8, :].astype(BF).astype(F32)
    at = lanes((8, 128))
    row = lax.broadcasted_iota(jnp.int32, (8, 128), 0)
    pos = where[4] + 64 * (at // 32) + 32 * where[3] + at % 32
    angle = pos.astype(F32) * frequency(4 * y + row % 4)
    sine = jnp.sin(angle)
    rotated = raw * jnp.cos(angle) + pltpu.roll(raw, 4, 0) * jnp.where(row < 4, -sine, sine)
    rotated = rotated.astype(BF)
    for t in range(NZ):
        k_ref[t, 64:72, :] = rotated


def make_queries(
    where, q0, q1, q2, q3, up_own, up_other, table,
    out, uk_ref, uv_ref, docs_ref, col_ref, row_ref, latents, ups,
):
    x, y, c = where[1], where[2], where[3]
    for j, part in enumerate((q0, q1, q2, q3)):
        own, other = part[0].astype(F32), part[1].astype(F32)
        rows = pl.ds(pl.multiple_of(lax.rem(y - j + NY, NY) * 64, 64), 64)
        latents[rows, 0:128] = jnp.where(c == 0, own, other)
        latents[rows, 128:256] = jnp.where(c == 0, other, own)
    raw = latents[...]
    mean = jnp.sum(raw * raw, axis=0, keepdims=True) * (1.0 / 256.0)
    inverse = lax.rsqrt(mean + EPS)
    gains = jnp.concatenate([column(table[0:1, :]), column(table[1:2, :])], axis=0)
    gains = jnp.concatenate([gains, gains], axis=1)
    tokens_docs = table[4:6, :]
    at = lanes((1, 128))
    for i in range(2):
        col_ref[128 * i : 128 * (i + 1), :] = column(table[2 + i : 3 + i, :])
        ordered = jnp.zeros((1, 128), F32)
        for k in range(NY):
            line = tokens_docs[k // 2 : k // 2 + 1, :]
            moved = pltpu.roll(line, (32 * k - 64 * (k % 2) - 32 * i) % 128, 1)
            ordered = jnp.where(at // 32 == k, moved, ordered)
        row_ref[i : i + 1, :] = ordered
    latent = (raw * inverse * gains).astype(BF)
    tok = lanes((64, 256))
    row = lax.broadcasted_iota(jnp.int32, (64, 256), 0)
    pos = where[4] + 64 * ((tok % 128) // 32) + 32 * (tok // 128) + tok % 32
    angle = pos.astype(F32) * frequency(4 * ((row % 32) // 8) + row % 4)
    is_low = (row // 4) % 2 == 0
    cos = jnp.cos(angle)
    sine = jnp.sin(angle)
    low_sin = jnp.where(is_low, -sine, 0.0)
    high_sin = jnp.where(is_low, 0.0, sine)
    for p, up in enumerate((up_own, up_other)):
        for j in range(NX):
            ups[p, :, lax.rem(x - j + NX, NX)] = up[:, j, 0:32, :]
        wide = ups[p].reshape(NS, 32, 128).astype(F32)
        own = slice(128 * p, 128 * (p + 1))
        plain_w = jnp.transpose(wide[:, 0:8, :].reshape(256, 128)).astype(BF)
        rope_w = jnp.transpose(wide[:, 24:32, :].reshape(256, 128))[0:64, :].astype(BF)
        uk_ref[:, own] = wide[:, 8:16, :].reshape(256, 128).astype(BF)
        uv_ref[own, :] = jnp.transpose(wide[:, 16:24, :].reshape(256, 128)).astype(BF)
        plain = (jnp.dot(plain_w, latent, preferred_element_type=F32) * SCALE2).astype(BF)
        raw = jnp.dot(rope_w, latent, preferred_element_type=F32) * SCALE2
        rope = raw * cos + pltpu.roll(raw, 60, 0) * low_sin + pltpu.roll(raw, 4, 0) * high_sin
        rope = rope.astype(BF)
        for i in range(2):
            h = 2 * p + i
            out[h] = jnp.zeros((256, 256), BF)
            out[h, 64 * i : 64 * (i + 1), :] = plain[64 * i : 64 * (i + 1), :]
            out[h, 128:160, :] = rope[32 * i : 32 * (i + 1), :]
    docs = ups[0].reshape(NS, 32, 128)[:, 24:32, :].astype(F32)
    at = lanes((NS, 128))
    spread = jnp.zeros((NS, 128), F32)
    for k in range(NY):
        piece = jnp.where(c == 0, docs[:, 2 * k, :], docs[:, 2 * k + 1, :])
        spread = jnp.where(at // 32 == k, pltpu.roll(piece, (32 * k + 64) % 128, 1), spread)
    docs_ref[...] = spread


def attend(
    where, q_ref, uk, uv, key_docs, gains, query_docs, b0, b1, b2, b3,
    keep_ref, send_ref, ml_ref, kb, s_buf, v_buf, mx, total, acc,
):
    x0, y0, c = where[1], where[2], where[3]
    docs = key_docs[...]
    at = lanes((NS, 128))
    before = (at == 127) & (docs < query_docs[0:1, 0:1])
    behind = (at == 0) & (docs > query_docs[1:2, 127:128])
    low = jnp.sum(before.astype(jnp.int32))
    high = NS - 1 - jnp.sum(behind.astype(jnp.int32))
    count = (high - low) // 2 + 1
    begin = jnp.minimum(low, NS - 2 * count)

    def fetch(z, carry):
        for j, part in enumerate((b0, b1, b2, b3)):
            for k in range(4):
                kb[j, k, z] = part[k, z]
        return carry

    lax.fori_loop(begin // 4, (begin + 2 * count - 1) // 4 + 1, fetch, 0)
    mx[...] = jnp.full(mx.shape, NEG_BIG, F32)
    total[...] = jnp.zeros(total.shape, F32)
    acc[...] = jnp.zeros(acc.shape, F32)
    wanted = jnp.concatenate([query_docs[0:1, :], query_docs[1:2, :]], axis=1)

    def scores(tile):
        latents, ropes, same = [], [], []
        for half in range(2):
            block = begin + 2 * tile + half
            z, x = block // NX, lax.rem(block, NX)
            jx = lax.rem(x0 - x + NX, NX)
            parts, turned = [], []
            for y in range(NY):
                jy = lax.rem(y0 - y + NY, NY)
                third = jnp.where(c == 0, jy, jx)
                second = jnp.where(c == 0, jx, jy)
                slab = kb[third, second, z].astype(F32)
                parts.append(slab[0:64, :])
                turned.append(slab[64:72, :])
            squares = parts[0] * parts[0]
            for part in parts[1:]:
                squares = squares + part * part
            mean = jnp.sum(squares, axis=0, keepdims=True) * (1.0 / 256.0)
            inverse = lax.rsqrt(mean + EPS)
            latents.append(jnp.concatenate(parts, axis=0) * inverse * gains[...])
            ropes.append(jnp.concatenate(turned, axis=0))
            docs_col = column(key_docs[pl.ds(block, 1), :])
            same.append(jnp.concatenate([docs_col, docs_col], axis=1) == wanted)
        latent = jnp.concatenate(latents, axis=1)
        v_buf[tile] = jnp.dot(uv[...], latent.astype(BF), preferred_element_type=F32).astype(BF)
        turned = jnp.transpose(latent).astype(BF)
        rope = jnp.concatenate(ropes, axis=1)
        rope = jnp.concatenate([rope, jnp.zeros((96, 256), F32)], axis=0)
        rope = jnp.transpose(rope).astype(BF)
        keys = jnp.dot(turned, uk[...], preferred_element_type=F32).astype(BF)
        for h in range(4):
            p = h // 2
            stack = jnp.concatenate([keys[:, 128 * p : 128 * (p + 1)], rope], axis=1)
            got = jnp.dot(stack, q_ref[h], preferred_element_type=F32)
            got = jnp.concatenate(
                [
                    jnp.where(same[0], got[0:128, :], NEG_BIG),
                    jnp.where(same[1], got[128:256, :], NEG_BIG),
                ],
                axis=0,
            )
            s_buf[tile, h] = got
            mx[h] = jnp.maximum(mx[h], jnp.max(got.reshape(32, 8, 256), axis=0))

    by_twos(scores, count)
    tops = []
    for h in range(4):
        top = jnp.maximum(jnp.max(mx[h], axis=0, keepdims=True), FLOOR)
        mx[h] = jnp.broadcast_to(top, (8, 256))
        tops.append(top)

    def weigh(tile):
        for h in range(4):
            own = slice(64 * h, 64 * (h + 1))
            weights = jnp.exp2(s_buf[tile, h].reshape(32, 8, 256) - mx[h][None])
            total[h] = total[h] + jnp.sum(weights, axis=0)
            weights = weights.reshape(256, 256).astype(BF)
            acc[own, :] = acc[own, :] + jnp.dot(
                v_buf[tile, own, :], weights, preferred_element_type=F32
            )

    by_twos(weigh, count)
    for h in range(4):
        ml_ref[h : h + 1, :] = tops[h]
        ml_ref[4 + h : 5 + h, :] = jnp.sum(total[h], axis=0, keepdims=True)
    left, right = acc[:, 0:128], acc[:, 128:256]
    keep_ref[...] = jnp.where(c == 0, left, right)
    send_ref[...] = jnp.where(c == 0, right, left).astype(BF)


def combine(
    where, keep, got, ml_own, ml_got, w_own, w_other, part_ref, p1_ref, p2_ref, p3_ref, lse_ref,
    scratch, outs,
):
    x, c = where[1], where[3]
    m0, l0 = ml_own[0:4, :], ml_own[4:8, :]
    m1 = jnp.concatenate([ml_got[2:4, :], ml_got[0:2, :]], axis=0)
    l1 = jnp.concatenate([ml_got[6:8, :], ml_got[4:6, :]], axis=0)
    top = jnp.maximum(m0, m1)
    e0 = jnp.exp2(m0 - top)
    e1 = jnp.exp2(m1 - top)
    weight_sum = l0 * e0 + l1 * e1
    lse_ref[...] = ((top + jnp.log2(weight_sum)) * LN2)[0:2, :]
    f0 = e0 / weight_sum
    f1 = e1 / weight_sum
    f0 = jnp.where(c == 0, f0[:, 0:128], f0[:, 128:256])
    f1 = jnp.where(c == 0, f1[:, 0:128], f1[:, 128:256])
    result = jnp.zeros((128, 1024), F32)
    for p, w in enumerate((w_own, w_other)):
        pieces = []
        for i in range(2):
            h, k = 2 * p + i, (2 * p + i + 2) % 4
            mine = keep[64 * h : 64 * (h + 1), :]
            theirs = got[64 * k : 64 * (k + 1), :].astype(F32)
            pieces.append(mine * f0[h : h + 1, :] + theirs * f1[h : h + 1, :])
        attended = jnp.transpose(jnp.concatenate(pieces, axis=0)).astype(BF)
        for j in range(NX):
            outs[p, :, lax.rem(x - j + NX, NX)] = w[:, j, 32:64, :]
        result = result + lax.dot_general(
            attended, outs[p].reshape(1024, 128), (((1,), (1,)), ((), ())),
            preferred_element_type=F32,
        )
    scratch[...] = result
    y = where[2]
    for j, out in enumerate((part_ref, p1_ref, p2_ref, p3_ref)):
        to = lax.rem(y + j, NY)
        out[...] = scratch[pl.ds(pl.multiple_of(to * 32, 32), 32), :].astype(BF)


def finish(part, p1, p2, p3, gain, out):
    summed = part[...].astype(F32)
    for other in (p1, p2, p3):
        summed = summed + other[...].astype(F32)
    wide = summed.astype(BF).astype(F32)
    mean = jnp.mean(wide * wide, axis=1, keepdims=True)
    out[...] = (wide * lax.rsqrt(mean + EPS) * gain[...]).astype(BF)


def flat(z, x, y, c):
    return ((z * NX + x) * NY + y) * NC + c


def ring(j):
    return [(i, (i + j) % NY) for i in range(NY)]


def shift_pairs(stage, j):
    pairs = []
    for z in range(NZ):
        for x in range(NX):
            for y in range(NY):
                for c in range(NC):
                    along_x = (c == 0) == (stage == 2)
                    to = flat(z, (x + j) % NX, y, c) if along_x else flat(z, x, (y + j) % NY, c)
                    pairs.append((flat(z, x, y, c), to))
    return pairs


def layer(
    tokens, doc_ids, down_query, down_key, down_rotary, query_gain, key_gain,
    up_query, up_key, up_value, output_weight, out_gain,
):
    z = lax.axis_index("z")
    x = lax.axis_index("x")
    y = lax.axis_index("y")
    c = lax.axis_index("c")
    sp = z * NX + x
    here = jnp.stack([z, x, y, c, sp * 256]).astype(jnp.int32)
    swap = [(0, 1), (1, 0)]

    sources = (down_query, down_key, down_rotary)
    message = call(
        pack, jax.ShapeDtypeStruct((NZ, 40, 128), BF), 1, 3, any_from=0,
        scratch=[VMEM((128, 128), F32)]
        + [VMEM(a.shape, a.dtype) for a in sources]
        + [pltpu.SemaphoreType.DMA((3,))],
    )(here, *(pltpu.with_memory_space_constraint(a, pltpu.HBM) for a in sources))
    gathered = lax.all_to_all(message, "z", 0, 0)
    gathered = [gathered] + [lax.ppermute(gathered, "x", ring(j)) for j in range(1, NX)]

    rows = [tokens] + [lax.ppermute(tokens, "y", ring(j)) for j in range(1, NY)]

    sources = (
        up_query, up_key, up_value, doc_ids.reshape(2, 128), output_weight.T,
        query_gain.reshape(2, 128), key_gain.reshape(2, 128),
    )
    later, table = call(
        pack_later, (jax.ShapeDtypeStruct((64, 128), BF), jax.ShapeDtypeStruct((6, 128), F32)),
        0, 7, any_from=0,
        scratch=[VMEM(a.shape, a.dtype) for a in sources] + [pltpu.SemaphoreType.DMA((7,))],
    )(*(pltpu.with_memory_space_constraint(a, pltpu.HBM) for a in sources))
    later = [later] + [lax.ppermute(later, "x", ring(j)) for j in range(1, NX)]
    later = jnp.broadcast_to(jnp.stack(later)[None], (NZ, NX, 64, 128))

    q_part, k_part = call(
        project,
        (jax.ShapeDtypeStruct((64, 128), BF), jax.ShapeDtypeStruct((NZ, 72, 128), BF)),
        1, 8, scratch=[VMEM((128, 1024), BF), VMEM((NX, NZ, 40, 128), BF)],
    )(here, *rows, *gathered)

    stage1 = lax.all_to_all(k_part, "z", 0, 0)
    stage2 = [lax.ppermute(stage1, AXES, shift_pairs(2, j)) for j in range(1, 4)]
    held = jnp.stack([stage1] + stage2)
    stage3 = [lax.ppermute(held, AXES, shift_pairs(3, j)) for j in range(1, 4)]

    up_own = lax.all_to_all(later, "z", 0, 0)
    up_other = lax.ppermute(up_own, "c", swap)
    q_pair = jnp.stack([q_part, lax.ppermute(q_part, "c", swap)])
    q_all = [q_pair] + [lax.ppermute(q_pair, "y", ring(j)) for j in range(1, NY)]
    queries, uk, uv, key_docs, gains, query_docs = call(
        make_queries,
        (
            jax.ShapeDtypeStruct((4, 256, 256), BF),
            jax.ShapeDtypeStruct((256, 256), BF),
            jax.ShapeDtypeStruct((256, 256), BF),
            jax.ShapeDtypeStruct((NS, 128), F32),
            jax.ShapeDtypeStruct((256, 128), F32),
            jax.ShapeDtypeStruct((2, 128), F32),
        ),
        1, 7, scratch=[VMEM((256, 256), F32), VMEM((2, NZ, NX, 32, 128), BF)],
    )(
        here, *q_all, up_own, up_other, table
    )

    keep, send, ml = call(
        attend,
        (
            jax.ShapeDtypeStruct((256, 128), F32),
            jax.ShapeDtypeStruct((256, 128), BF),
            jax.ShapeDtypeStruct((8, 256), F32),
        ),
        1, 10, room=34,
        scratch=[
            VMEM((4, 4, NZ, 72, 128), BF),
            VMEM((16, 4, 256, 256), F32),
            VMEM((16, 256, 256), BF),
            VMEM((4, 8, 256), F32),
            VMEM((4, 8, 256), F32),
            VMEM((256, 256), F32),
        ],
    )(here, queries, uk, uv, key_docs, gains, query_docs, held, *stage3)

    got = lax.ppermute(send, "c", swap)
    ml_got = lax.ppermute(ml, "c", swap)
    *parts, log_sums = call(
        combine,
        (jax.ShapeDtypeStruct((32, 1024), BF),) * NY + (jax.ShapeDtypeStruct((2, 256), F32),),
        1, 6, scratch=[VMEM((128, 1024), F32), VMEM((2, NZ, NX, 32, 128), BF)],
    )(here, keep, got, ml, ml_got, up_own, up_other)
    parts[1:] = [lax.ppermute(parts[j], "y", ring(j)) for j in range(1, NY)]
    mixed = call(finish, jax.ShapeDtypeStruct((32, 1024), BF), 0, 5)(
        *parts, out_gain.reshape(1, 1024)
    )
    log_sums = log_sums.reshape(2, 2, 4, 32).transpose(2, 1, 3, 0).reshape(256, 2)
    return mixed, log_sums


def solution(mesh):
    finer = Mesh(mesh.devices.reshape(NZ, NX, NY, NC), AXES)
    return jax.shard_map(
        layer,
        mesh=finer,
        in_specs=(
            P(AXES, None), P(SP), P(SP, None), P(SP, None), P(SP, None), P(), P(),
            P(SP, TP), P(SP, TP), P(SP, TP), P(TP, SP), P(),
        ),
        out_specs=(P(AXES, None), P(SP, TP)),
        check_vma=False,
    )
```

```python
import math

import jax
import jax.numpy as jnp
from jax import lax
from jax.experimental import pallas as pl
from jax.experimental.pallas import tpu as pltpu
from jax.sharding import Mesh
from jax.sharding import PartitionSpec as P


NOPE = 64
ROPE = 32
NZ, NX, NY, NC = 8, 4, 4, 2
NS = NZ * NX
AXES = ("z", "x", "y", "c")
SP = ("z", "x")
TP = ("y", "c")
NEG_BIG = -1e30
FLOOR = -1e20
THETA = 10000.0
EPS = 1e-06
LN2 = math.log(2.0)
SCALE2 = 1.0 / math.sqrt(NOPE + ROPE) / LN2
BF = jnp.bfloat16
F32 = jnp.float32


VMEM = pltpu.VMEM
SMEM_SPEC = pl.BlockSpec(memory_space=pltpu.SMEM)
VMEM_SPEC = pl.BlockSpec(memory_space=pltpu.VMEM)
ANY_SPEC = pl.BlockSpec(memory_space=pltpu.HBM)


def call(body, outs, n_smem, n_in, scratch=(), any_from=None, cost=None, room=16):
    specs = [SMEM_SPEC] * n_smem
    for i in range(n_in):
        specs.append(ANY_SPEC if any_from is not None and i >= any_from else VMEM_SPEC)
    single = not isinstance(outs, tuple)
    return pl.pallas_call(
        body,
        out_shape=outs,
        in_specs=specs,
        out_specs=VMEM_SPEC if single else tuple(VMEM_SPEC for _ in outs),
        scratch_shapes=list(scratch),
        compiler_params=pltpu.CompilerParams(vmem_limit_bytes=room * 1024 * 1024),
        cost_estimate=cost,
    )


def lanes(shape):
    return lax.broadcasted_iota(jnp.int32, shape, len(shape) - 1)


def column(row):
    return jnp.transpose(jnp.broadcast_to(row, (128, 128)))


def by_fours(step, count):
    def four(i, carry):
        for k in range(4):
            step(4 * i + k)
        return carry

    lax.fori_loop(0, count // 4, four, 0)
    done = count // 4 * 4

    @pl.when(lax.rem(count, 4) >= 2)
    def _():
        step(done)
        step(done + 1)

    @pl.when(lax.rem(count, 2) == 1)
    def _():
        step(count - 1)


def frequency(index):
    value = jnp.ones(index.shape, F32)
    for bit in range(4):
        factor = THETA ** (-(1 << bit) / 16)
        value = value * jnp.where((index // (1 << bit)) % 2 == 1, factor, 1.0)
    return value


def pack(where, dq_in, dk_in, dr_in, out, flipped, dq, dk, dr, sems):
    copies = [
        pltpu.make_async_copy(source, place, sems.at[i])
        for i, (source, place) in enumerate(((dq_in, dq), (dk_in, dk), (dr_in, dr)))
    ]
    for copy in copies:
        copy.start()
    for copy in copies:
        copy.wait()
    y = where[2]

    def chosen(ref):
        block = ref[:, 0:64]
        for k in range(1, NY):
            block = jnp.where(y == k, ref[:, 64 * k : 64 * (k + 1)], block)
        return block

    block = jnp.concatenate([chosen(dq), chosen(dk)], axis=1)
    rope = dr[...].astype(F32)
    rope = jnp.concatenate([rope, jnp.zeros((32, 96), F32)], axis=1)
    flipped[...] = jnp.transpose(jnp.concatenate([rope] * 4, axis=0))
    turned = jnp.concatenate([flipped[pl.ds(4 * y, 4), :], flipped[pl.ds(16 + 4 * y, 4), :]], axis=0)
    turned = turned.astype(BF)
    for z in range(NZ):
        out[z, 0:32, :] = block
        out[z, 32:40, :] = turned


def pack_later(*refs):
    inputs, out, table, places, sems = refs[:7], refs[7], refs[8], refs[9:16], refs[16]
    copies = [
        pltpu.make_async_copy(source, place, sems.at[i])
        for i, (source, place) in enumerate(zip(inputs, places))
    ]
    for copy in copies:
        copy.start()
    for copy in copies:
        copy.wait()
    up_query, up_key, up_value, docs_ref, out_t, query_gain, key_gain = places
    table[0:2, :] = query_gain[...]
    table[2:4, :] = key_gain[...]
    table[4:6, :] = docs_ref[...].astype(F32)
    src = lax.broadcasted_iota(jnp.int32, (192, 256), 0)
    lane = lanes((192, 256))
    plain = 96 * (lane // 64) + lane % 64
    turn = lane - 128
    rope = 64 + 96 * (turn // 32) + 16 * ((turn // 4) % 2) + 4 * ((turn % 32) // 8) + turn % 4
    chosen = jnp.where(lane < 128, plain, jnp.where(lane < 192, rope, -1))
    pick = jnp.where(src == chosen, 1.0, 0.0).astype(BF)
    sorted_query = jnp.dot(up_query[...], pick, preferred_element_type=F32)
    out[0:8, :] = sorted_query[:, 0:128].astype(BF)
    out[8:16, :] = up_key[...]
    out[16:24, :] = up_value[...]
    mixed = sorted_query[:, 128:256]
    docs = docs_ref[...].astype(F32)
    row = lax.broadcasted_iota(jnp.int32, (8, 128), 0)
    at = lanes((8, 128))
    for r in range(8):
        line = docs[r // 4 : r // 4 + 1, :]
        moved = pltpu.roll(jnp.broadcast_to(line, (8, 128)), (64 - 32 * (r % 4)) % 128, 1)
        mixed = jnp.where((row == r) & (at // 32 == 2), moved, mixed)
    out[24:32, :] = mixed.astype(BF)
    out[32:64, :] = out_t[...]


def project(where, t0, t1, t2, t3, g0, g1, g2, g3, q_ref, k_ref, tok, gathered):
    x = where[1]
    y = where[2]
    for j, part in enumerate((t0, t1, t2, t3)):
        at = lax.rem(y - j + NY, NY)
        tok[pl.ds(pl.multiple_of(at * 32, 32), 32), :] = part[...]
    for j, part in enumerate((g0, g1, g2, g3)):
        gathered[lax.rem(x - j + NX, NX)] = part[...]
    rows = tok[...]
    weights = jnp.concatenate(
        [gathered[k, z, 0:32, :] for z in range(NZ) for k in range(NX)], axis=0
    )
    both = jnp.dot(rows, weights, preferred_element_type=F32)
    turned = jnp.transpose(both).astype(BF)
    q_ref[...] = turned[0:64, :]
    for t in range(NZ):
        k_ref[t, 0:64, :] = turned[64:128, :]
    group = lanes((8, 128)) // 32
    pieces = []
    for z in range(NZ):
        piece = gathered[0, z, 32:40, :].astype(F32)
        for g in range(1, 4):
            piece = jnp.where(group == g, gathered[g, z, 32:40, :].astype(F32), piece)
        pieces.append(piece)
    rope = jnp.concatenate(pieces, axis=1)
    rope = jnp.concatenate([rope, jnp.zeros_like(rope)], axis=0).astype(BF)
    raw = lax.dot_general(rope, rows, (((1,), (1,)), ((), ())), preferred_element_type=F32)
    raw = raw[0:8, :].astype(BF).astype(F32)
    at = lanes((8, 128))
    row = lax.broadcasted_iota(jnp.int32, (8, 128), 0)
    pos = where[4] + 64 * (at // 32) + 32 * where[3] + at % 32
    angle = pos.astype(F32) * frequency(4 * y + row % 4)
    sine = jnp.sin(angle)
    rotated = raw * jnp.cos(angle) + pltpu.roll(raw, 4, 0) * jnp.where(row < 4, -sine, sine)
    rotated = rotated.astype(BF)
    for t in range(NZ):
        k_ref[t, 64:72, :] = rotated


def make_queries(
    where, q0, q1, q2, q3, up_own, up_other, table,
    out, uk_ref, uv_ref, docs_ref, col_ref, row_ref, latents, ups,
):
    x, y, c = where[1], where[2], where[3]
    for j, part in enumerate((q0, q1, q2, q3)):
        own, other = part[0].astype(F32), part[1].astype(F32)
        rows = pl.ds(pl.multiple_of(lax.rem(y - j + NY, NY) * 64, 64), 64)
        latents[rows, 0:128] = jnp.where(c == 0, own, other)
        latents[rows, 128:256] = jnp.where(c == 0, other, own)
    raw = latents[...]
    mean = jnp.sum(raw * raw, axis=0, keepdims=True) * (1.0 / 256.0)
    inverse = lax.rsqrt(mean + EPS)
    gains = jnp.concatenate([column(table[0:1, :]), column(table[1:2, :])], axis=0)
    gains = jnp.concatenate([gains, gains], axis=1)
    tokens_docs = table[4:6, :]
    at = lanes((1, 128))
    for i in range(2):
        col_ref[128 * i : 128 * (i + 1), :] = column(table[2 + i : 3 + i, :])
        ordered = jnp.zeros((1, 128), F32)
        for k in range(NY):
            line = tokens_docs[k // 2 : k // 2 + 1, :]
            moved = pltpu.roll(line, (32 * k - 64 * (k % 2) - 32 * i) % 128, 1)
            ordered = jnp.where(at // 32 == k, moved, ordered)
        row_ref[i : i + 1, :] = ordered
    latent = (raw * inverse * gains).astype(BF)
    tok = lanes((64, 256))
    row = lax.broadcasted_iota(jnp.int32, (64, 256), 0)
    pos = where[4] + 64 * ((tok % 128) // 32) + 32 * (tok // 128) + tok % 32
    angle = pos.astype(F32) * frequency(4 * ((row % 32) // 8) + row % 4)
    is_low = (row // 4) % 2 == 0
    cos = jnp.cos(angle)
    sine = jnp.sin(angle)
    low_sin = jnp.where(is_low, -sine, 0.0)
    high_sin = jnp.where(is_low, 0.0, sine)
    for p, up in enumerate((up_own, up_other)):
        for j in range(NX):
            ups[p, :, lax.rem(x - j + NX, NX)] = up[:, j, 0:32, :]
        wide = ups[p].reshape(NS, 32, 128).astype(F32)
        own = slice(128 * p, 128 * (p + 1))
        plain_w = jnp.transpose(wide[:, 0:8, :].reshape(256, 128)).astype(BF)
        rope_w = jnp.transpose(wide[:, 24:32, :].reshape(256, 128))[0:64, :].astype(BF)
        uk_ref[:, own] = wide[:, 8:16, :].reshape(256, 128).astype(BF)
        uv_ref[own, :] = jnp.transpose(wide[:, 16:24, :].reshape(256, 128)).astype(BF)
        plain = (jnp.dot(plain_w, latent, preferred_element_type=F32) * SCALE2).astype(BF)
        raw = jnp.dot(rope_w, latent, preferred_element_type=F32) * SCALE2
        rope = raw * cos + pltpu.roll(raw, 60, 0) * low_sin + pltpu.roll(raw, 4, 0) * high_sin
        rope = rope.astype(BF)
        for i in range(2):
            h = 2 * p + i
            out[h] = jnp.zeros((256, 256), BF)
            out[h, 64 * i : 64 * (i + 1), :] = plain[64 * i : 64 * (i + 1), :]
            out[h, 128:160, :] = rope[32 * i : 32 * (i + 1), :]
    docs = ups[0].reshape(NS, 32, 128)[:, 24:32, :].astype(F32)
    at = lanes((NS, 128))
    spread = jnp.zeros((NS, 128), F32)
    for k in range(NY):
        piece = jnp.where(c == 0, docs[:, 2 * k, :], docs[:, 2 * k + 1, :])
        spread = jnp.where(at // 32 == k, pltpu.roll(piece, (32 * k + 64) % 128, 1), spread)
    docs_ref[...] = spread


def attend(
    where, q_ref, uk, uv, key_docs, gains, query_docs, b0, b1, b2, b3,
    keep_ref, send_ref, ml_ref, kb, s_buf, v_buf, mx, total, acc,
):
    x0, y0, c = where[1], where[2], where[3]
    docs = key_docs[...]
    at = lanes((NS, 128))
    before = (at == 127) & (docs < query_docs[0:1, 0:1])
    behind = (at == 0) & (docs > query_docs[1:2, 127:128])
    low = jnp.sum(before.astype(jnp.int32))
    high = NS - 1 - jnp.sum(behind.astype(jnp.int32))
    count = (high - low) // 2 + 1
    begin = jnp.minimum(low, NS - 2 * count)

    def fetch(z, carry):
        for j, part in enumerate((b0, b1, b2, b3)):
            for k in range(4):
                kb[j, k, z] = part[k, z]
        return carry

    lax.fori_loop(begin // 4, (begin + 2 * count - 1) // 4 + 1, fetch, 0)
    mx[...] = jnp.full(mx.shape, NEG_BIG, F32)
    total[...] = jnp.zeros(total.shape, F32)
    acc[...] = jnp.zeros(acc.shape, F32)
    wanted = jnp.concatenate([query_docs[0:1, :], query_docs[1:2, :]], axis=1)

    def scores(tile):
        latents, ropes, same = [], [], []
        for half in range(2):
            block = begin + 2 * tile + half
            z, x = block // NX, lax.rem(block, NX)
            jx = lax.rem(x0 - x + NX, NX)
            parts, turned = [], []
            for y in range(NY):
                jy = lax.rem(y0 - y + NY, NY)
                third = jnp.where(c == 0, jy, jx)
                second = jnp.where(c == 0, jx, jy)
                slab = kb[third, second, z].astype(F32)
                parts.append(slab[0:64, :])
                turned.append(slab[64:72, :])
            squares = parts[0] * parts[0]
            for part in parts[1:]:
                squares = squares + part * part
            mean = jnp.sum(squares, axis=0, keepdims=True) * (1.0 / 256.0)
            inverse = lax.rsqrt(mean + EPS)
            latents.append(jnp.concatenate(parts, axis=0) * inverse * gains[...])
            ropes.append(jnp.concatenate(turned, axis=0))
            docs_col = column(key_docs[pl.ds(block, 1), :])
            same.append(jnp.concatenate([docs_col, docs_col], axis=1) == wanted)
        latent = jnp.concatenate(latents, axis=1)
        v_buf[tile] = jnp.dot(uv[...], latent.astype(BF), preferred_element_type=F32).astype(BF)
        turned = jnp.transpose(latent).astype(BF)
        rope = jnp.concatenate(ropes, axis=1)
        rope = jnp.concatenate([rope, jnp.zeros((96, 256), F32)], axis=0)
        rope = jnp.transpose(rope).astype(BF)
        keys = jnp.dot(turned, uk[...], preferred_element_type=F32).astype(BF)
        for h in range(4):
            p = h // 2
            stack = jnp.concatenate([keys[:, 128 * p : 128 * (p + 1)], rope], axis=1)
            got = jnp.dot(stack, q_ref[h], preferred_element_type=F32)
            got = jnp.concatenate(
                [
                    jnp.where(same[0], got[0:128, :], NEG_BIG),
                    jnp.where(same[1], got[128:256, :], NEG_BIG),
                ],
                axis=0,
            )
            s_buf[tile, h] = got
            mx[h] = jnp.maximum(mx[h], jnp.max(got.reshape(32, 8, 256), axis=0))

    by_fours(scores, count)
    tops = []
    for h in range(4):
        top = jnp.maximum(jnp.max(mx[h], axis=0, keepdims=True), FLOOR)
        mx[h] = jnp.broadcast_to(top, (8, 256))
        tops.append(top)

    def weigh(tile):
        for h in range(4):
            own = slice(64 * h, 64 * (h + 1))
            weights = jnp.exp2(s_buf[tile, h].reshape(32, 8, 256) - mx[h][None])
            total[h] = total[h] + jnp.sum(weights, axis=0)
            weights = weights.reshape(256, 256).astype(BF)
            acc[own, :] = acc[own, :] + jnp.dot(
                v_buf[tile, own, :], weights, preferred_element_type=F32
            )

    by_fours(weigh, count)
    for h in range(4):
        ml_ref[h : h + 1, :] = tops[h]
        ml_ref[4 + h : 5 + h, :] = jnp.sum(total[h], axis=0, keepdims=True)
    left, right = acc[:, 0:128], acc[:, 128:256]
    keep_ref[...] = jnp.where(c == 0, left, right)
    send_ref[...] = jnp.where(c == 0, right, left).astype(BF)


def combine(
    where, keep, got, ml_own, ml_got, w_own, w_other, part_ref, p1_ref, p2_ref, p3_ref, lse_ref,
    scratch, outs,
):
    x, c = where[1], where[3]
    m0, l0 = ml_own[0:4, :], ml_own[4:8, :]
    m1 = jnp.concatenate([ml_got[2:4, :], ml_got[0:2, :]], axis=0)
    l1 = jnp.concatenate([ml_got[6:8, :], ml_got[4:6, :]], axis=0)
    top = jnp.maximum(m0, m1)
    e0 = jnp.exp2(m0 - top)
    e1 = jnp.exp2(m1 - top)
    weight_sum = l0 * e0 + l1 * e1
    lse_ref[...] = ((top + jnp.log2(weight_sum)) * LN2)[0:2, :]
    f0 = e0 / weight_sum
    f1 = e1 / weight_sum
    f0 = jnp.where(c == 0, f0[:, 0:128], f0[:, 128:256])
    f1 = jnp.where(c == 0, f1[:, 0:128], f1[:, 128:256])
    result = jnp.zeros((128, 1024), F32)
    for p, w in enumerate((w_own, w_other)):
        pieces = []
        for i in range(2):
            h, k = 2 * p + i, (2 * p + i + 2) % 4
            mine = keep[64 * h : 64 * (h + 1), :]
            theirs = got[64 * k : 64 * (k + 1), :].astype(F32)
            pieces.append(mine * f0[h : h + 1, :] + theirs * f1[h : h + 1, :])
        attended = jnp.transpose(jnp.concatenate(pieces, axis=0)).astype(BF)
        for j in range(NX):
            outs[p, :, lax.rem(x - j + NX, NX)] = w[:, j, 32:64, :]
        result = result + lax.dot_general(
            attended, outs[p].reshape(1024, 128), (((1,), (1,)), ((), ())),
            preferred_element_type=F32,
        )
    scratch[...] = result
    y = where[2]
    for j, out in enumerate((part_ref, p1_ref, p2_ref, p3_ref)):
        to = lax.rem(y + j, NY)
        out[...] = scratch[pl.ds(pl.multiple_of(to * 32, 32), 32), :].astype(BF)


def finish(part, p1, p2, p3, gain, out):
    summed = part[...].astype(F32)
    for other in (p1, p2, p3):
        summed = summed + other[...].astype(F32)
    wide = summed.astype(BF).astype(F32)
    mean = jnp.mean(wide * wide, axis=1, keepdims=True)
    out[...] = (wide * lax.rsqrt(mean + EPS) * gain[...]).astype(BF)


def flat(z, x, y, c):
    return ((z * NX + x) * NY + y) * NC + c


def ring(j):
    return [(i, (i + j) % NY) for i in range(NY)]


def shift_pairs(stage, j):
    pairs = []
    for z in range(NZ):
        for x in range(NX):
            for y in range(NY):
                for c in range(NC):
                    along_x = (c == 0) == (stage == 2)
                    to = flat(z, (x + j) % NX, y, c) if along_x else flat(z, x, (y + j) % NY, c)
                    pairs.append((flat(z, x, y, c), to))
    return pairs


def layer(
    tokens, doc_ids, down_query, down_key, down_rotary, query_gain, key_gain,
    up_query, up_key, up_value, output_weight, out_gain,
):
    z = lax.axis_index("z")
    x = lax.axis_index("x")
    y = lax.axis_index("y")
    c = lax.axis_index("c")
    sp = z * NX + x
    here = jnp.stack([z, x, y, c, sp * 256]).astype(jnp.int32)
    swap = [(0, 1), (1, 0)]

    sources = (down_query, down_key, down_rotary)
    message = call(
        pack, jax.ShapeDtypeStruct((NZ, 40, 128), BF), 1, 3, any_from=0,
        scratch=[VMEM((128, 128), F32)]
        + [VMEM(a.shape, a.dtype) for a in sources]
        + [pltpu.SemaphoreType.DMA((3,))],
    )(here, *(pltpu.with_memory_space_constraint(a, pltpu.HBM) for a in sources))
    gathered = lax.all_to_all(message, "z", 0, 0)
    gathered = [gathered] + [lax.ppermute(gathered, "x", ring(j)) for j in range(1, NX)]

    rows = [tokens] + [lax.ppermute(tokens, "y", ring(j)) for j in range(1, NY)]

    sources = (
        up_query, up_key, up_value, doc_ids.reshape(2, 128), output_weight.T,
        query_gain.reshape(2, 128), key_gain.reshape(2, 128),
    )
    later, table = call(
        pack_later, (jax.ShapeDtypeStruct((64, 128), BF), jax.ShapeDtypeStruct((6, 128), F32)),
        0, 7, any_from=0,
        scratch=[VMEM(a.shape, a.dtype) for a in sources] + [pltpu.SemaphoreType.DMA((7,))],
    )(*(pltpu.with_memory_space_constraint(a, pltpu.HBM) for a in sources))
    later = [later] + [lax.ppermute(later, "x", ring(j)) for j in range(1, NX)]
    later = jnp.broadcast_to(jnp.stack(later)[None], (NZ, NX, 64, 128))

    q_part, k_part = call(
        project,
        (jax.ShapeDtypeStruct((64, 128), BF), jax.ShapeDtypeStruct((NZ, 72, 128), BF)),
        1, 8, scratch=[VMEM((128, 1024), BF), VMEM((NX, NZ, 40, 128), BF)],
    )(here, *rows, *gathered)

    stage1 = lax.all_to_all(k_part, "z", 0, 0)
    stage2 = [lax.ppermute(stage1, AXES, shift_pairs(2, j)) for j in range(1, 4)]
    held = jnp.stack([stage1] + stage2)
    stage3 = [lax.ppermute(held, AXES, shift_pairs(3, j)) for j in range(1, 4)]

    up_own = lax.all_to_all(later, "z", 0, 0)
    up_other = lax.ppermute(up_own, "c", swap)
    q_pair = jnp.stack([q_part, lax.ppermute(q_part, "c", swap)])
    q_all = [q_pair] + [lax.ppermute(q_pair, "y", ring(j)) for j in range(1, NY)]
    queries, uk, uv, key_docs, gains, query_docs = call(
        make_queries,
        (
            jax.ShapeDtypeStruct((4, 256, 256), BF),
            jax.ShapeDtypeStruct((256, 256), BF),
            jax.ShapeDtypeStruct((256, 256), BF),
            jax.ShapeDtypeStruct((NS, 128), F32),
            jax.ShapeDtypeStruct((256, 128), F32),
            jax.ShapeDtypeStruct((2, 128), F32),
        ),
        1, 7, scratch=[VMEM((256, 256), F32), VMEM((2, NZ, NX, 32, 128), BF)],
    )(
        here, *q_all, up_own, up_other, table
    )

    keep, send, ml = call(
        attend,
        (
            jax.ShapeDtypeStruct((256, 128), F32),
            jax.ShapeDtypeStruct((256, 128), BF),
            jax.ShapeDtypeStruct((8, 256), F32),
        ),
        1, 10, room=34,
        scratch=[
            VMEM((4, 4, NZ, 72, 128), BF),
            VMEM((16, 4, 256, 256), F32),
            VMEM((16, 256, 256), BF),
            VMEM((4, 8, 256), F32),
            VMEM((4, 8, 256), F32),
            VMEM((256, 256), F32),
        ],
    )(here, queries, uk, uv, key_docs, gains, query_docs, held, *stage3)

    got = lax.ppermute(send, "c", swap)
    ml_got = lax.ppermute(ml, "c", swap)
    *parts, log_sums = call(
        combine,
        (jax.ShapeDtypeStruct((32, 1024), BF),) * NY + (jax.ShapeDtypeStruct((2, 256), F32),),
        1, 6, scratch=[VMEM((128, 1024), F32), VMEM((2, NZ, NX, 32, 128), BF)],
    )(here, keep, got, ml, ml_got, up_own, up_other)
    parts[1:] = [lax.ppermute(parts[j], "y", ring(j)) for j in range(1, NY)]
    mixed = call(finish, jax.ShapeDtypeStruct((32, 1024), BF), 0, 5)(
        *parts, out_gain.reshape(1, 1024)
    )
    log_sums = log_sums.reshape(2, 2, 4, 32).transpose(2, 1, 3, 0).reshape(256, 2)
    return mixed, log_sums


def solution(mesh):
    finer = Mesh(mesh.devices.reshape(NZ, NX, NY, NC), AXES)
    return jax.shard_map(
        layer,
        mesh=finer,
        in_specs=(
            P(AXES, None), P(SP), P(SP, None), P(SP, None), P(SP, None), P(), P(),
            P(SP, TP), P(SP, TP), P(SP, TP), P(TP, SP), P(),
        ),
        out_specs=(P(AXES, None), P(SP, TP)),
        check_vma=False,
    )
```

```python
import math

import jax
import jax.numpy as jnp
from jax import lax
from jax.experimental import pallas as pl
from jax.experimental.pallas import tpu as pltpu
from jax.sharding import Mesh
from jax.sharding import PartitionSpec as P


NOPE = 64
ROPE = 32
NZ, NX, NY, NC = 8, 4, 4, 2
NS = NZ * NX
AXES = ("z", "x", "y", "c")
SP = ("z", "x")
TP = ("y", "c")
NEG_BIG = -1e30
FLOOR = -1e20
THETA = 10000.0
EPS = 1e-06
LN2 = math.log(2.0)
SCALE2 = 1.0 / math.sqrt(NOPE + ROPE) / LN2
BF = jnp.bfloat16
F32 = jnp.float32


VMEM = pltpu.VMEM
SMEM_SPEC = pl.BlockSpec(memory_space=pltpu.SMEM)
VMEM_SPEC = pl.BlockSpec(memory_space=pltpu.VMEM)
ANY_SPEC = pl.BlockSpec(memory_space=pltpu.HBM)


def call(body, outs, n_smem, n_in, scratch=(), any_from=None, cost=None, room=16):
    specs = [SMEM_SPEC] * n_smem
    for i in range(n_in):
        specs.append(ANY_SPEC if any_from is not None and i >= any_from else VMEM_SPEC)
    single = not isinstance(outs, tuple)
    return pl.pallas_call(
        body,
        out_shape=outs,
        in_specs=specs,
        out_specs=VMEM_SPEC if single else tuple(VMEM_SPEC for _ in outs),
        scratch_shapes=list(scratch),
        compiler_params=pltpu.CompilerParams(vmem_limit_bytes=room * 1024 * 1024),
        cost_estimate=cost,
    )


def lanes(shape):
    return lax.broadcasted_iota(jnp.int32, shape, len(shape) - 1)


def column(row):
    return jnp.transpose(jnp.broadcast_to(row, (128, 128)))


def by_eights(step, count):
    def eight(i, carry):
        for k in range(8):
            step(8 * i + k)
        return carry

    lax.fori_loop(0, count // 8, eight, 0)
    most = count // 8 * 8

    @pl.when(lax.rem(count, 8) >= 4)
    def _():
        for k in range(4):
            step(most + k)

    done = count // 4 * 4

    @pl.when(lax.rem(count, 4) >= 2)
    def _():
        step(done)
        step(done + 1)

    @pl.when(lax.rem(count, 2) == 1)
    def _():
        step(count - 1)


def frequency(index):
    value = jnp.ones(index.shape, F32)
    for bit in range(4):
        factor = THETA ** (-(1 << bit) / 16)
        value = value * jnp.where((index // (1 << bit)) % 2 == 1, factor, 1.0)
    return value


def pack(where, dq_in, dk_in, dr_in, out, flipped, dq, dk, dr, sems):
    copies = [
        pltpu.make_async_copy(source, place, sems.at[i])
        for i, (source, place) in enumerate(((dq_in, dq), (dk_in, dk), (dr_in, dr)))
    ]
    for copy in copies:
        copy.start()
    for copy in copies:
        copy.wait()
    y = where[2]

    def chosen(ref):
        block = ref[:, 0:64]
        for k in range(1, NY):
            block = jnp.where(y == k, ref[:, 64 * k : 64 * (k + 1)], block)
        return block

    block = jnp.concatenate([chosen(dq), chosen(dk)], axis=1)
    rope = dr[...].astype(F32)
    rope = jnp.concatenate([rope, jnp.zeros((32, 96), F32)], axis=1)
    flipped[...] = jnp.transpose(jnp.concatenate([rope] * 4, axis=0))
    turned = jnp.concatenate([flipped[pl.ds(4 * y, 4), :], flipped[pl.ds(16 + 4 * y, 4), :]], axis=0)
    turned = turned.astype(BF)
    for z in range(NZ):
        out[z, 0:32, :] = block
        out[z, 32:40, :] = turned


def pack_later(*refs):
    inputs, out, table, places, sems = refs[:7], refs[7], refs[8], refs[9:16], refs[16]
    copies = [
        pltpu.make_async_copy(source, place, sems.at[i])
        for i, (source, place) in enumerate(zip(inputs, places))
    ]
    for copy in copies:
        copy.start()
    for copy in copies:
        copy.wait()
    up_query, up_key, up_value, docs_ref, out_t, query_gain, key_gain = places
    table[0:2, :] = query_gain[...]
    table[2:4, :] = key_gain[...]
    table[4:6, :] = docs_ref[...].astype(F32)
    src = lax.broadcasted_iota(jnp.int32, (192, 256), 0)
    lane = lanes((192, 256))
    plain = 96 * (lane // 64) + lane % 64
    turn = lane - 128
    rope = 64 + 96 * (turn // 32) + 16 * ((turn // 4) % 2) + 4 * ((turn % 32) // 8) + turn % 4
    chosen = jnp.where(lane < 128, plain, jnp.where(lane < 192, rope, -1))
    pick = jnp.where(src == chosen, 1.0, 0.0).astype(BF)
    sorted_query = jnp.dot(up_query[...], pick, preferred_element_type=F32)
    out[0:8, :] = sorted_query[:, 0:128].astype(BF)
    out[8:16, :] = up_key[...]
    out[16:24, :] = up_value[...]
    mixed = sorted_query[:, 128:256]
    docs = docs_ref[...].astype(F32)
    row = lax.broadcasted_iota(jnp.int32, (8, 128), 0)
    at = lanes((8, 128))
    for r in range(8):
        line = docs[r // 4 : r // 4 + 1, :]
        moved = pltpu.roll(jnp.broadcast_to(line, (8, 128)), (64 - 32 * (r % 4)) % 128, 1)
        mixed = jnp.where((row == r) & (at // 32 == 2), moved, mixed)
    out[24:32, :] = mixed.astype(BF)
    out[32:64, :] = out_t[...]


def project(where, t0, t1, t2, t3, g0, g1, g2, g3, q_ref, k_ref, tok, gathered):
    x = where[1]
    y = where[2]
    for j, part in enumerate((t0, t1, t2, t3)):
        at = lax.rem(y - j + NY, NY)
        tok[pl.ds(pl.multiple_of(at * 32, 32), 32), :] = part[...]
    for j, part in enumerate((g0, g1, g2, g3)):
        gathered[lax.rem(x - j + NX, NX)] = part[...]
    rows = tok[...]
    weights = jnp.concatenate(
        [gathered[k, z, 0:32, :] for z in range(NZ) for k in range(NX)], axis=0
    )
    both = jnp.dot(rows, weights, preferred_element_type=F32)
    turned = jnp.transpose(both).astype(BF)
    q_ref[...] = turned[0:64, :]
    for t in range(NZ):
        k_ref[t, 0:64, :] = turned[64:128, :]
    group = lanes((8, 128)) // 32
    pieces = []
    for z in range(NZ):
        piece = gathered[0, z, 32:40, :].astype(F32)
        for g in range(1, 4):
            piece = jnp.where(group == g, gathered[g, z, 32:40, :].astype(F32), piece)
        pieces.append(piece)
    rope = jnp.concatenate(pieces, axis=1)
    rope = jnp.concatenate([rope, jnp.zeros_like(rope)], axis=0).astype(BF)
    raw = lax.dot_general(rope, rows, (((1,), (1,)), ((), ())), preferred_element_type=F32)
    raw = raw[0:8, :].astype(BF).astype(F32)
    at = lanes((8, 128))
    row = lax.broadcasted_iota(jnp.int32, (8, 128), 0)
    pos = where[4] + 64 * (at // 32) + 32 * where[3] + at % 32
    angle = pos.astype(F32) * frequency(4 * y + row % 4)
    sine = jnp.sin(angle)
    rotated = raw * jnp.cos(angle) + pltpu.roll(raw, 4, 0) * jnp.where(row < 4, -sine, sine)
    rotated = rotated.astype(BF)
    for t in range(NZ):
        k_ref[t, 64:72, :] = rotated


def make_queries(
    where, q0, q1, q2, q3, up_own, up_other, table,
    out, uk_ref, uv_ref, docs_ref, col_ref, row_ref, latents, ups,
):
    x, y, c = where[1], where[2], where[3]
    for j, part in enumerate((q0, q1, q2, q3)):
        own, other = part[0].astype(F32), part[1].astype(F32)
        rows = pl.ds(pl.multiple_of(lax.rem(y - j + NY, NY) * 64, 64), 64)
        latents[rows, 0:128] = jnp.where(c == 0, own, other)
        latents[rows, 128:256] = jnp.where(c == 0, other, own)
    raw = latents[...]
    mean = jnp.sum(raw * raw, axis=0, keepdims=True) * (1.0 / 256.0)
    inverse = lax.rsqrt(mean + EPS)
    gains = jnp.concatenate([column(table[0:1, :]), column(table[1:2, :])], axis=0)
    gains = jnp.concatenate([gains, gains], axis=1)
    tokens_docs = table[4:6, :]
    at = lanes((1, 128))
    for i in range(2):
        col_ref[128 * i : 128 * (i + 1), :] = column(table[2 + i : 3 + i, :])
        ordered = jnp.zeros((1, 128), F32)
        for k in range(NY):
            line = tokens_docs[k // 2 : k // 2 + 1, :]
            moved = pltpu.roll(line, (32 * k - 64 * (k % 2) - 32 * i) % 128, 1)
            ordered = jnp.where(at // 32 == k, moved, ordered)
        row_ref[i : i + 1, :] = ordered
    latent = (raw * inverse * gains).astype(BF)
    tok = lanes((64, 256))
    row = lax.broadcasted_iota(jnp.int32, (64, 256), 0)
    pos = where[4] + 64 * ((tok % 128) // 32) + 32 * (tok // 128) + tok % 32
    angle = pos.astype(F32) * frequency(4 * ((row % 32) // 8) + row % 4)
    is_low = (row // 4) % 2 == 0
    cos = jnp.cos(angle)
    sine = jnp.sin(angle)
    low_sin = jnp.where(is_low, -sine, 0.0)
    high_sin = jnp.where(is_low, 0.0, sine)
    for p, up in enumerate((up_own, up_other)):
        for j in range(NX):
            ups[p, :, lax.rem(x - j + NX, NX)] = up[:, j, 0:32, :]
        wide = ups[p].reshape(NS, 32, 128).astype(F32)
        own = slice(128 * p, 128 * (p + 1))
        plain_w = jnp.transpose(wide[:, 0:8, :].reshape(256, 128)).astype(BF)
        rope_w = jnp.transpose(wide[:, 24:32, :].reshape(256, 128))[0:64, :].astype(BF)
        uk_ref[:, own] = wide[:, 8:16, :].reshape(256, 128).astype(BF)
        uv_ref[own, :] = jnp.transpose(wide[:, 16:24, :].reshape(256, 128)).astype(BF)
        plain = (jnp.dot(plain_w, latent, preferred_element_type=F32) * SCALE2).astype(BF)
        raw = jnp.dot(rope_w, latent, preferred_element_type=F32) * SCALE2
        rope = raw * cos + pltpu.roll(raw, 60, 0) * low_sin + pltpu.roll(raw, 4, 0) * high_sin
        rope = rope.astype(BF)
        for i in range(2):
            h = 2 * p + i
            out[h] = jnp.zeros((256, 256), BF)
            out[h, 64 * i : 64 * (i + 1), :] = plain[64 * i : 64 * (i + 1), :]
            out[h, 128:160, :] = rope[32 * i : 32 * (i + 1), :]
    docs = ups[0].reshape(NS, 32, 128)[:, 24:32, :].astype(F32)
    at = lanes((NS, 128))
    spread = jnp.zeros((NS, 128), F32)
    for k in range(NY):
        piece = jnp.where(c == 0, docs[:, 2 * k, :], docs[:, 2 * k + 1, :])
        spread = jnp.where(at // 32 == k, pltpu.roll(piece, (32 * k + 64) % 128, 1), spread)
    docs_ref[...] = spread


def attend(
    where, q_ref, uk, uv, key_docs, gains, query_docs, b0, b1, b2, b3,
    keep_ref, send_ref, ml_ref, kb, s_buf, v_buf, mx, total, acc,
):
    x0, y0, c = where[1], where[2], where[3]
    docs = key_docs[...]
    at = lanes((NS, 128))
    before = (at == 127) & (docs < query_docs[0:1, 0:1])
    behind = (at == 0) & (docs > query_docs[1:2, 127:128])
    low = jnp.sum(before.astype(jnp.int32))
    high = NS - 1 - jnp.sum(behind.astype(jnp.int32))
    count = (high - low) // 2 + 1
    begin = jnp.minimum(low, NS - 2 * count)

    def fetch(z, carry):
        for j, part in enumerate((b0, b1, b2, b3)):
            for k in range(4):
                kb[j, k, z] = part[k, z]
        return carry

    lax.fori_loop(begin // 4, (begin + 2 * count - 1) // 4 + 1, fetch, 0)
    mx[...] = jnp.full(mx.shape, NEG_BIG, F32)
    total[...] = jnp.zeros(total.shape, F32)
    acc[...] = jnp.zeros(acc.shape, F32)
    wanted = jnp.concatenate([query_docs[0:1, :], query_docs[1:2, :]], axis=1)

    def scores(tile):
        latents, ropes, same = [], [], []
        for half in range(2):
            block = begin + 2 * tile + half
            z, x = block // NX, lax.rem(block, NX)
            jx = lax.rem(x0 - x + NX, NX)
            parts, turned = [], []
            for y in range(NY):
                jy = lax.rem(y0 - y + NY, NY)
                third = jnp.where(c == 0, jy, jx)
                second = jnp.where(c == 0, jx, jy)
                slab = kb[third, second, z].astype(F32)
                parts.append(slab[0:64, :])
                turned.append(slab[64:72, :])
            squares = parts[0] * parts[0]
            for part in parts[1:]:
                squares = squares + part * part
            mean = jnp.sum(squares, axis=0, keepdims=True) * (1.0 / 256.0)
            inverse = lax.rsqrt(mean + EPS)
            latents.append(jnp.concatenate(parts, axis=0) * inverse * gains[...])
            ropes.append(jnp.concatenate(turned, axis=0))
            docs_col = column(key_docs[pl.ds(block, 1), :])
            same.append(jnp.concatenate([docs_col, docs_col], axis=1) == wanted)
        latent = jnp.concatenate(latents, axis=1)
        v_buf[tile] = jnp.dot(uv[...], latent.astype(BF), preferred_element_type=F32).astype(BF)
        turned = jnp.transpose(latent).astype(BF)
        rope = jnp.concatenate(ropes, axis=1)
        rope = jnp.concatenate([rope, jnp.zeros((96, 256), F32)], axis=0)
        rope = jnp.transpose(rope).astype(BF)
        keys = jnp.dot(turned, uk[...], preferred_element_type=F32).astype(BF)
        for h in range(4):
            p = h // 2
            stack = jnp.concatenate([keys[:, 128 * p : 128 * (p + 1)], rope], axis=1)
            got = jnp.dot(stack, q_ref[h], preferred_element_type=F32)
            got = jnp.concatenate(
                [
                    jnp.where(same[0], got[0:128, :], NEG_BIG),
                    jnp.where(same[1], got[128:256, :], NEG_BIG),
                ],
                axis=0,
            )
            s_buf[tile, h] = got
            mx[h] = jnp.maximum(mx[h], jnp.max(got.reshape(32, 8, 256), axis=0))

    by_eights(scores, count)
    tops = []
    for h in range(4):
        top = jnp.maximum(jnp.max(mx[h], axis=0, keepdims=True), FLOOR)
        mx[h] = jnp.broadcast_to(top, (8, 256))
        tops.append(top)

    def weigh(tile):
        for h in range(4):
            own = slice(64 * h, 64 * (h + 1))
            weights = jnp.exp2(s_buf[tile, h].reshape(32, 8, 256) - mx[h][None])
            total[h] = total[h] + jnp.sum(weights, axis=0)
            weights = weights.reshape(256, 256).astype(BF)
            acc[own, :] = acc[own, :] + jnp.dot(
                v_buf[tile, own, :], weights, preferred_element_type=F32
            )

    by_eights(weigh, count)
    for h in range(4):
        ml_ref[h : h + 1, :] = tops[h]
        ml_ref[4 + h : 5 + h, :] = jnp.sum(total[h], axis=0, keepdims=True)
    left, right = acc[:, 0:128], acc[:, 128:256]
    keep_ref[...] = jnp.where(c == 0, left, right)
    send_ref[...] = jnp.where(c == 0, right, left).astype(BF)


def combine(
    where, keep, got, ml_own, ml_got, w_own, w_other, part_ref, p1_ref, p2_ref, p3_ref, lse_ref,
    scratch, outs,
):
    x, c = where[1], where[3]
    m0, l0 = ml_own[0:4, :], ml_own[4:8, :]
    m1 = jnp.concatenate([ml_got[2:4, :], ml_got[0:2, :]], axis=0)
    l1 = jnp.concatenate([ml_got[6:8, :], ml_got[4:6, :]], axis=0)
    top = jnp.maximum(m0, m1)
    e0 = jnp.exp2(m0 - top)
    e1 = jnp.exp2(m1 - top)
    weight_sum = l0 * e0 + l1 * e1
    lse_ref[...] = ((top + jnp.log2(weight_sum)) * LN2)[0:2, :]
    f0 = e0 / weight_sum
    f1 = e1 / weight_sum
    f0 = jnp.where(c == 0, f0[:, 0:128], f0[:, 128:256])
    f1 = jnp.where(c == 0, f1[:, 0:128], f1[:, 128:256])
    result = jnp.zeros((128, 1024), F32)
    for p, w in enumerate((w_own, w_other)):
        pieces = []
        for i in range(2):
            h, k = 2 * p + i, (2 * p + i + 2) % 4
            mine = keep[64 * h : 64 * (h + 1), :]
            theirs = got[64 * k : 64 * (k + 1), :].astype(F32)
            pieces.append(mine * f0[h : h + 1, :] + theirs * f1[h : h + 1, :])
        attended = jnp.transpose(jnp.concatenate(pieces, axis=0)).astype(BF)
        for j in range(NX):
            outs[p, :, lax.rem(x - j + NX, NX)] = w[:, j, 32:64, :]
        result = result + lax.dot_general(
            attended, outs[p].reshape(1024, 128), (((1,), (1,)), ((), ())),
            preferred_element_type=F32,
        )
    scratch[...] = result
    y = where[2]
    for j, out in enumerate((part_ref, p1_ref, p2_ref, p3_ref)):
        to = lax.rem(y + j, NY)
        out[...] = scratch[pl.ds(pl.multiple_of(to * 32, 32), 32), :].astype(BF)


def finish(part, p1, p2, p3, gain, out):
    summed = part[...].astype(F32)
    for other in (p1, p2, p3):
        summed = summed + other[...].astype(F32)
    wide = summed.astype(BF).astype(F32)
    mean = jnp.mean(wide * wide, axis=1, keepdims=True)
    out[...] = (wide * lax.rsqrt(mean + EPS) * gain[...]).astype(BF)


def flat(z, x, y, c):
    return ((z * NX + x) * NY + y) * NC + c


def ring(j):
    return [(i, (i + j) % NY) for i in range(NY)]


def shift_pairs(stage, j):
    pairs = []
    for z in range(NZ):
        for x in range(NX):
            for y in range(NY):
                for c in range(NC):
                    along_x = (c == 0) == (stage == 2)
                    to = flat(z, (x + j) % NX, y, c) if along_x else flat(z, x, (y + j) % NY, c)
                    pairs.append((flat(z, x, y, c), to))
    return pairs


def layer(
    tokens, doc_ids, down_query, down_key, down_rotary, query_gain, key_gain,
    up_query, up_key, up_value, output_weight, out_gain,
):
    z = lax.axis_index("z")
    x = lax.axis_index("x")
    y = lax.axis_index("y")
    c = lax.axis_index("c")
    sp = z * NX + x
    here = jnp.stack([z, x, y, c, sp * 256]).astype(jnp.int32)
    swap = [(0, 1), (1, 0)]

    sources = (down_query, down_key, down_rotary)
    message = call(
        pack, jax.ShapeDtypeStruct((NZ, 40, 128), BF), 1, 3, any_from=0,
        scratch=[VMEM((128, 128), F32)]
        + [VMEM(a.shape, a.dtype) for a in sources]
        + [pltpu.SemaphoreType.DMA((3,))],
    )(here, *(pltpu.with_memory_space_constraint(a, pltpu.HBM) for a in sources))
    gathered = lax.all_to_all(message, "z", 0, 0)
    gathered = [gathered] + [lax.ppermute(gathered, "x", ring(j)) for j in range(1, NX)]

    rows = [tokens] + [lax.ppermute(tokens, "y", ring(j)) for j in range(1, NY)]

    sources = (
        up_query, up_key, up_value, doc_ids.reshape(2, 128), output_weight.T,
        query_gain.reshape(2, 128), key_gain.reshape(2, 128),
    )
    later, table = call(
        pack_later, (jax.ShapeDtypeStruct((64, 128), BF), jax.ShapeDtypeStruct((6, 128), F32)),
        0, 7, any_from=0,
        scratch=[VMEM(a.shape, a.dtype) for a in sources] + [pltpu.SemaphoreType.DMA((7,))],
    )(*(pltpu.with_memory_space_constraint(a, pltpu.HBM) for a in sources))
    later = [later] + [lax.ppermute(later, "x", ring(j)) for j in range(1, NX)]
    later = jnp.broadcast_to(jnp.stack(later)[None], (NZ, NX, 64, 128))

    q_part, k_part = call(
        project,
        (jax.ShapeDtypeStruct((64, 128), BF), jax.ShapeDtypeStruct((NZ, 72, 128), BF)),
        1, 8, scratch=[VMEM((128, 1024), BF), VMEM((NX, NZ, 40, 128), BF)],
    )(here, *rows, *gathered)

    stage1 = lax.all_to_all(k_part, "z", 0, 0)
    stage2 = [lax.ppermute(stage1, AXES, shift_pairs(2, j)) for j in range(1, 4)]
    held = jnp.stack([stage1] + stage2)
    stage3 = [lax.ppermute(held, AXES, shift_pairs(3, j)) for j in range(1, 4)]

    up_own = lax.all_to_all(later, "z", 0, 0)
    up_other = lax.ppermute(up_own, "c", swap)
    q_pair = jnp.stack([q_part, lax.ppermute(q_part, "c", swap)])
    q_all = [q_pair] + [lax.ppermute(q_pair, "y", ring(j)) for j in range(1, NY)]
    queries, uk, uv, key_docs, gains, query_docs = call(
        make_queries,
        (
            jax.ShapeDtypeStruct((4, 256, 256), BF),
            jax.ShapeDtypeStruct((256, 256), BF),
            jax.ShapeDtypeStruct((256, 256), BF),
            jax.ShapeDtypeStruct((NS, 128), F32),
            jax.ShapeDtypeStruct((256, 128), F32),
            jax.ShapeDtypeStruct((2, 128), F32),
        ),
        1, 7, scratch=[VMEM((256, 256), F32), VMEM((2, NZ, NX, 32, 128), BF)],
    )(
        here, *q_all, up_own, up_other, table
    )

    keep, send, ml = call(
        attend,
        (
            jax.ShapeDtypeStruct((256, 128), F32),
            jax.ShapeDtypeStruct((256, 128), BF),
            jax.ShapeDtypeStruct((8, 256), F32),
        ),
        1, 10, room=34,
        scratch=[
            VMEM((4, 4, NZ, 72, 128), BF),
            VMEM((16, 4, 256, 256), F32),
            VMEM((16, 256, 256), BF),
            VMEM((4, 8, 256), F32),
            VMEM((4, 8, 256), F32),
            VMEM((256, 256), F32),
        ],
    )(here, queries, uk, uv, key_docs, gains, query_docs, held, *stage3)

    got = lax.ppermute(send, "c", swap)
    ml_got = lax.ppermute(ml, "c", swap)
    *parts, log_sums = call(
        combine,
        (jax.ShapeDtypeStruct((32, 1024), BF),) * NY + (jax.ShapeDtypeStruct((2, 256), F32),),
        1, 6, scratch=[VMEM((128, 1024), F32), VMEM((2, NZ, NX, 32, 128), BF)],
    )(here, keep, got, ml, ml_got, up_own, up_other)
    parts[1:] = [lax.ppermute(parts[j], "y", ring(j)) for j in range(1, NY)]
    mixed = call(finish, jax.ShapeDtypeStruct((32, 1024), BF), 0, 5)(
        *parts, out_gain.reshape(1, 1024)
    )
    log_sums = log_sums.reshape(2, 2, 4, 32).transpose(2, 1, 3, 0).reshape(256, 2)
    return mixed, log_sums


def solution(mesh):
    finer = Mesh(mesh.devices.reshape(NZ, NX, NY, NC), AXES)
    return jax.shard_map(
        layer,
        mesh=finer,
        in_specs=(
            P(AXES, None), P(SP), P(SP, None), P(SP, None), P(SP, None), P(), P(),
            P(SP, TP), P(SP, TP), P(SP, TP), P(TP, SP), P(),
        ),
        out_specs=(P(AXES, None), P(SP, TP)),
        check_vma=False,
    )
```
